32 devices in a mesh: ep: 8 (over z, x), tp: 4 (over y, core).
Axes of the slice: x: 2, y: 2, z: 4, core: 2. Of those that a mesh axis runs over, the one named last changes fastest.
Arguments:
- receptance: bfloat16 [4096, 2048], P('ep', 'tp'), may hold values from -6 to 6
- key_rows: bfloat16 [4096, 2048], P('ep', 'tp'), may hold values from -6 to 6
- value_rows: bfloat16 [4096, 2048], P('ep', 'tp'), may hold values from -6 to 6
- decay_input: bfloat16 [4096, 2048], P('ep', 'tp'), may hold values from -2.796875 to 2.796875
- learn_input: bfloat16 [4096, 2048], P('ep', 'tp'), may hold values from -12 to 4
- decay_base: float32 [2048], P('tp'), may hold values from -20 to -2
- decay_shift: float32 [4096, 32], P('ep', 'tp'), may hold values from -1 to 20
- channel_gain: float32 [2048], P('tp'), may hold values from 0.1 to 1.9
- out_weight: bfloat16 [2048, 2048], P('tp'), may hold values from -0.125 to 0.125
- expert_input: bfloat16 [4096, 2048], P(('ep', 'tp')), may hold values from -6 to 6
- expert_gain: float32 [2048], replicated, may hold values from 0.1 to 1.9
- routes: int32 [4096, 2], P(('ep', 'tp')), may hold values from 0 to 7, all different within a row; in each aligned block of 128 rows (0 to 127, 128 to 255, ...) at most 64 rows name the same one
- route_weight: float32 [4096, 2], P(('ep', 'tp')), may hold values from 0.1 to 1
- gate_weight: bfloat16 [8, 2048, 1024], P('ep', None, 'tp'), may hold values from -0.125 to 0.125
- up_weight: bfloat16 [8, 2048, 1024], P('ep', None, 'tp'), may hold values from -0.125 to 0.125
- down_weight: bfloat16 [8, 1024, 2048], P('ep', 'tp'), may hold values from -0.1875 to 0.1875
Outputs:
- mixer_out: bfloat16 [4096, 2048], P(('ep', 'tp'))
- expert_out: bfloat16 [4096, 2048], P(('ep', 'tp'))
The draws below stay inside these ranges and needn't reach their ends.
Inputs may be any that keep to these rules, and one draw needn't show every extreme that they name: `routes`: within the rows of one device (aligned blocks of 128 rows) no expert is named by more than 64 rows, and in every draw some block names some expert exactly 64 times. Each row names 2 different experts.
All inputs are finite; a program needn't handle non-finite values.
Results may differ from the reference program's by a relative error of at most 0.024.
Values may be sent and summed in bfloat16 or wider, within the bound.
A program may use at most 128 MiB of HBM per device.

```python
import math
import jax
import jax.numpy as jnp
import numpy as np
from jax import lax

D = 2048
HEADS = 32
HEAD = 64
CHANNELS = 2048
FF = 1024
EXPERTS = 8
TOPK = 2
TOK_DEV = 128
MIX_ROWS = 512
MICRO_TOKENS = 4096
CAP = 64
N_TP = 4


def fast_heads(key):
    ranking = jax.random.permutation(jax.random.fold_in(key, 101), HEADS)
    quick_count = HEADS // 2
    return jnp.repeat(ranking < quick_count, HEAD)


def draw_decay_base(key, part):
    quick = fast_heads(key)
    spread = jax.random.uniform(jax.random.fold_in(key, 102), (CHANNELS,), jnp.float32)
    slow_rates = -jnp.log(jnp.float32(MICRO_TOKENS)) - 2.0 - spread
    quick_rates = -3.9 + 1.3 * spread
    return jnp.where(quick, quick_rates, slow_rates).astype(jnp.float32)


def draw_decay_shift(key, part):
    blocks = MICRO_TOKENS // MIX_ROWS
    reach = 0.5
    levels = jax.random.uniform(jax.random.fold_in(key, 103), (blocks, HEADS), jnp.float32, -reach, reach)
    each_row_amount = jnp.repeat(levels, MIX_ROWS, axis=0)
    surge_locations = jax.random.randint(jax.random.fold_in(key, 104), (3,), 0, MICRO_TOKENS)
    surge_groups = jnp.any(jnp.arange(MICRO_TOKENS, dtype=jnp.int32)[:, None] == surge_locations[None, :], axis=1)
    table_height = jnp.log(jnp.float32(MICRO_TOKENS)) + 3.0
    return (each_row_amount + jnp.where(surge_groups, table_height, 0.0)[:, None]).astype(jnp.float32)


def draw_learn_input(key, part):
    quick = fast_heads(key)
    slow_mean = -jnp.log(jnp.float32(MICRO_TOKENS) / HEAD) - 1.0
    centre = jnp.where(quick, 0.0, slow_mean)
    jitter = jnp.clip(jax.random.normal(jax.random.fold_in(key, 105), (MICRO_TOKENS, CHANNELS), jnp.float32), -3.0, 3.0)
    return (centre[None, :] + jitter).astype(jnp.bfloat16)


def block_scale(own_key, shape, cuts, smallest, top_value):
    factor_of = 1.0
    for dim, shards_of in cuts:
        draws = jax.random.uniform(jax.random.fold_in(jax.random.fold_in(own_key, 6), dim), (shards_of,), jnp.float32, smallest / len(cuts), top_value / len(cuts))
        factor_of = factor_of * jnp.repeat(jnp.exp(draws), shape[dim] // shards_of).reshape((-1,) + (1,) * (len(shape) - 1 - dim))
    return factor_of


def assign_block(own_key, own, number, rows, count, top, most, lean):
    sequence = jax.random.permutation(own_key, count)
    packed, ordinary = load_shares(count, rows * top, most, lean, True), load_shares(count, rows * top, most, lean, False)
    places = jnp.arange(count)

    def named(lengths, turn):
        used = int((lengths > 0).sum())
        fixed = max(1, used // 4)
        shifted = fixed + (places - fixed + turn * (used - fixed)) % max(1, count - fixed)
        return jnp.zeros((count,), jnp.int32).at[sequence[jnp.where(places < fixed, places, shifted)]].set(jnp.asarray(lengths, jnp.int32))

    lengths = jnp.where(number % 4 == 0, named(packed, number // 4), named(ordinary, number - number // 4 - 1))
    mixed = jax.random.permutation(jax.random.fold_in(own, 3), count)
    giver, sink = mixed[0:count // 2 * 2:2], mixed[1:count // 2 * 2:2]
    slack = jnp.minimum(lengths[giver] - 1, most - lengths[sink]) // 2
    slack = jnp.where((giver == sequence[0]) | (sink == sequence[0]) | (lengths[sink] == 0), 0, jnp.maximum(slack, 0))
    shifted = jax.random.randint(jax.random.fold_in(own, 4), (count // 2,), 0, 1 << 20) % (slack + 1)
    lengths = lengths.at[giver].add(-shifted).at[sink].add(shifted)
    items = jnp.searchsorted(jnp.cumsum(lengths), jnp.arange(rows * top), side="right").astype(jnp.int32)
    listing = items.reshape(top, rows).T
    listing = listing[jax.random.permutation(jax.random.fold_in(own, 1), rows)]
    turn = jax.random.randint(jax.random.fold_in(own, 2), (rows, 1), 0, top)
    return jnp.take_along_axis(listing, (jnp.arange(top)[None, :] + turn) % top, axis=1)


def load_shares(number_of, total, most, lean, full):
    loads = [(1 << 20) // math.isqrt(grade ** lean) + 1 for grade in range(1, number_of + 1)]
    largest = most if full else min(most, max(-(-total // number_of), total * loads[0] // sum(loads)))
    least = 1 if total - largest >= number_of - 1 else 0
    given, rest = [largest] + [least] * (number_of - 1), total - largest - least * (number_of - 1)
    while rest > 0:
        free = [i for i in range(1, number_of) if given[i] < largest] or [i for i in range(1, number_of) if given[i] < most]
        mass, left = sum([loads[i] for i in free]), rest
        for i in free:
            addition = min(most - given[i], max(1, left * loads[i] // mass), rest)
            given[i] = given[i] + addition
            rest = rest - addition
    return np.array(given)


def noise(own_key, dims, deviation, limit, pieces=(), held_as=jnp.bfloat16):
    entries = deviation * jax.random.normal(own_key, dims, jnp.float32)
    if pieces:
        entries = entries * block_scale(own_key, dims, pieces, -0.22, 0.18)
    return jnp.clip(entries, -limit, limit).astype(held_as)


def setup_inputs(seed: int = 0) -> dict:
    key_list = jax.random.split(jax.random.key(seed), 17)
    receptance = noise(key_list[0], (MICRO_TOKENS, CHANNELS), 1.0, 6.0, ((0, 8), (1, 4)))
    key_rows = noise(key_list[1], (MICRO_TOKENS, CHANNELS), 1.0, 6.0, ((0, 8), (1, 4)))
    value_rows = noise(key_list[2], (MICRO_TOKENS, CHANNELS), 1.0, 6.0, ((0, 8), (1, 4)))
    decay_input = noise(key_list[3], (MICRO_TOKENS, CHANNELS), 0.7, 2.796875, ((0, 8), (1, 4)))
    learn_input = draw_learn_input(jax.random.fold_in(key_list[16], 71), 0)
    decay_base = draw_decay_base(jax.random.fold_in(key_list[16], 71), 0)
    decay_shift = draw_decay_shift(jax.random.fold_in(key_list[16], 71), 0)
    channel_gain = jnp.clip(1.0 + 0.18 * jax.random.normal(key_list[7], (CHANNELS,), jnp.float32), 0.1, 1.9)
    out_weight = noise(key_list[8], (CHANNELS, D), CHANNELS ** -0.5, 0.125, ((0, 4),))
    expert_input = noise(key_list[9], (MICRO_TOKENS, D), 1.0, 6.0, ((0, 32),))
    expert_gain = jnp.clip(1.0 + 0.18 * jax.random.normal(key_list[10], (D,), jnp.float32), 0.1, 1.9)
    routes_keys = jax.random.split(jax.random.fold_in(key_list[11], 1), MICRO_TOKENS // TOK_DEV)
    routes_turns = jax.random.permutation(jax.random.fold_in(key_list[11], 3), MICRO_TOKENS // TOK_DEV)
    routes = jax.vmap(lambda own, number: assign_block(jax.random.fold_in(key_list[11], 2), own, number, TOK_DEV, EXPERTS, TOPK, CAP, 1))(routes_keys, routes_turns).reshape((MICRO_TOKENS, TOPK))
    route_weight = jnp.clip(jnp.exp(math.log(1.0) - 2.3025851 * jax.random.uniform(key_list[12], (MICRO_TOKENS, TOPK), jnp.float32) ** block_scale(key_list[12], (MICRO_TOKENS, TOPK), ((0, 32),), -0.2, 0.2)), 0.1, 1.0)
    gate_weight = noise(key_list[13], (EXPERTS, D, FF), D ** -0.5, 0.125, ((0, 8), (2, 4)))
    up_weight = noise(key_list[14], (EXPERTS, D, FF), D ** -0.5, 0.125, ((0, 8), (2, 4)))
    down_weight = noise(key_list[15], (EXPERTS, FF, D), FF ** -0.5, 0.1875, ((0, 8), (1, 4)))
    return {"receptance": receptance, "key_rows": key_rows, "value_rows": value_rows, "decay_input": decay_input, "learn_input": learn_input, "decay_base": decay_base, "decay_shift": decay_shift, "channel_gain": channel_gain, "out_weight": out_weight, "expert_input": expert_input, "expert_gain": expert_gain, "routes": routes, "route_weight": route_weight, "gate_weight": gate_weight, "up_weight": up_weight, "down_weight": down_weight}


NORM_EPS = 1e-06
GROUP_EPS = 0.00064
KEY_EPS = 1e-06
PRECISE = lax.Precision.HIGHEST

def rounded_sum(inputs, weight, groups):
    group_size = inputs.shape[1] // groups
    result = jnp.zeros((inputs.shape[0], weight.shape[1]), jnp.float32)
    for part_index in range(groups):
        lower = part_index * group_size
        partial_value = jnp.dot(inputs[:, lower:lower + group_size], weight[lower:lower + group_size], preferred_element_type=jnp.float32)
        result = result + lax.optimization_barrier(partial_value.astype(jnp.bfloat16)).astype(jnp.float32)
    return result.astype(jnp.bfloat16)

def slot_targets(block_routes, experts, capacity):
    flat_routes = block_routes.reshape(-1)
    matches = (flat_routes[:, None] == jnp.arange(experts, dtype=jnp.int32)[None, :]).astype(jnp.int32)
    earlier = jnp.cumsum(matches, axis=0) - matches
    slots = lax.optimization_barrier(jnp.sum(earlier * matches, axis=1)).reshape(block_routes.shape)
    return (block_routes * capacity + slots).astype(jnp.int32)

def token_mixer(receptance, key_rows, value_rows, decay_input, learn_input, decay_base, decay_shift, channel_gain, out_weight):
    head_shape = (MICRO_TOKENS, HEADS, HEAD)
    recept = receptance.astype(jnp.float32).reshape(head_shape)
    key_data = key_rows.astype(jnp.float32).reshape(head_shape)
    value_data = value_rows.astype(jnp.float32).reshape(head_shape)
    pre_decay = decay_input.astype(jnp.float32).reshape(head_shape) + decay_base.reshape(1, HEADS, HEAD) + decay_shift[:, :, None]
    decays = jnp.exp(-jnp.exp(-jax.nn.softplus(-pre_decay) - 0.5))
    rates = jax.nn.sigmoid(learn_input.astype(jnp.float32)).reshape(head_shape)
    unit_keys = key_data / jnp.sqrt(lax.optimization_barrier(jnp.sum(key_data * key_data, axis=2, keepdims=True)) + KEY_EPS)
    removal = unit_keys * rates

    def advance(state, inputs):
        recept_now, decay_now, key_now, value_now, unit_now, removal_now = inputs
        probes = jnp.einsum('hij,hj->hi', state, unit_now, precision=PRECISE)
        state = state * decay_now[:, None, :] - probes[:, :, None] * removal_now[:, None, :] + value_now[:, :, None] * key_now[:, None, :]
        return (state, jnp.einsum('hij,hj->hi', state, recept_now, precision=PRECISE))
    start_state = jnp.zeros((HEADS, HEAD, HEAD), jnp.float32)
    _, readout = lax.scan(advance, start_state, (recept, decays, key_data, value_data, unit_keys, removal))
    centred = readout - lax.optimization_barrier(jnp.mean(readout, axis=2, keepdims=True))
    variance = lax.optimization_barrier(jnp.mean(centred * centred, axis=2, keepdims=True))
    normed = (centred * lax.rsqrt(variance + GROUP_EPS)).reshape(MICRO_TOKENS, CHANNELS) * channel_gain
    return rounded_sum(normed.astype(jnp.bfloat16), out_weight, N_TP)

def expert_layer(expert_input, expert_gain, routes, route_weight, gate_weight, up_weight, down_weight):
    inputs = expert_input.astype(jnp.float32)
    normed = (inputs * lax.rsqrt(lax.optimization_barrier(jnp.mean(inputs * inputs, axis=1, keepdims=True)) + NORM_EPS) * expert_gain).astype(jnp.bfloat16)
    blocks = MICRO_TOKENS // TOK_DEV
    block_routes = routes.reshape(blocks, TOK_DEV, TOPK)
    targets = jax.vmap(lambda member: slot_targets(member, EXPERTS, CAP))(block_routes)
    slots = targets - block_routes * CAP
    block_index = jnp.arange(blocks, dtype=jnp.int32)[:, None, None]
    places = ((block_routes * blocks + block_index) * CAP + slots).astype(jnp.int32)
    token_index = jnp.broadcast_to(jnp.arange(MICRO_TOKENS, dtype=jnp.int32).reshape(blocks, TOK_DEV, 1), places.shape)
    owners = jnp.full((EXPERTS * blocks * CAP,), MICRO_TOKENS, jnp.int32).at[places.reshape(-1)].set(token_index.reshape(-1))
    padded = jnp.concatenate([normed, jnp.zeros((1, D), jnp.bfloat16)], axis=0)

    def run_expert(operands):
        owner_rows, w_gate, w_up, w_down = operands
        gathered = padded[owner_rows]
        gates = jnp.dot(gathered, w_gate, preferred_element_type=jnp.float32)
        uppers = jnp.dot(gathered, w_up, preferred_element_type=jnp.float32)
        hidden = (jax.nn.silu(gates) * uppers).astype(jnp.bfloat16)
        return rounded_sum(hidden, w_down, N_TP)
    outputs = lax.map(run_expert, (owners.reshape(EXPERTS, blocks * CAP), gate_weight, up_weight, down_weight))
    flat_rows = outputs.reshape(EXPERTS * blocks * CAP, D)
    picks = places.reshape(MICRO_TOKENS, TOPK)
    combined = jnp.zeros((MICRO_TOKENS, D), jnp.float32)
    for picked in range(TOPK):
        combined = combined + flat_rows[picks[:, picked]].astype(jnp.float32) * route_weight[:, picked:picked + 1]
    return combined.astype(jnp.bfloat16)

def reference(receptance, key_rows, value_rows, decay_input, learn_input, decay_base, decay_shift, channel_gain, out_weight, expert_input, expert_gain, routes, route_weight, gate_weight, up_weight, down_weight):
    mixer_out = token_mixer(receptance, key_rows, value_rows, decay_input, learn_input, decay_base, decay_shift, channel_gain, out_weight)
    expert_out = expert_layer(expert_input, expert_gain, routes, route_weight, gate_weight, up_weight, down_weight)
    return (mixer_out, expert_out)
```

```python
import functools

import jax
import jax.numpy as jnp
from jax import lax
from jax.experimental import pallas as pl
from jax.experimental.pallas import tpu as pltpu
from jax.sharding import PartitionSpec as P


SPAN = 128
STACK = 2
LANES = 128

NORM_EPS = 1e-06
GROUP_EPS = 0.00064
KEY_EPS = 1e-06
F32 = jnp.float32
BF16 = jnp.bfloat16


def mm(a, b):
    return lax.dot_general(
        a.astype(BF16), b.astype(BF16), (((1,), (0,)), ((), ())), preferred_element_type=F32
    )


def mm_nt(a, b):
    return lax.dot_general(
        a.astype(BF16), b.astype(BF16), (((1,), (1,)), ((), ())), preferred_element_type=F32
    )


def mm_tn(a, b):
    return lax.dot_general(
        a.astype(BF16), b.astype(BF16), (((0,), (0,)), ((), ())), preferred_element_type=F32
    )


def split_two(x):
    high = x.astype(BF16)
    return high, (x - high.astype(F32)).astype(BF16)


def grid_index(shape, axis):
    return lax.broadcasted_iota(jnp.int32, shape, axis)


def same_head(head_size):
    rows = grid_index((LANES, LANES), 0) // head_size
    cols = grid_index((LANES, LANES), 1) // head_size
    return rows == cols


def head_sums(x, block):
    high, low = split_two(x)
    return mm(
        jnp.concatenate([high, low], axis=1), jnp.concatenate([block, block], axis=0)
    )


def lower_inverses(strict_parts, rows, cols):
    eye = jnp.where(rows == cols, 1.0, 0.0)
    size = 1
    inverses = None
    while size < SPAN:
        off = (rows // (2 * size) == cols // (2 * size)) & (rows // size != cols // size)
        parts = [jnp.where(off, part, 0.0) for part in strict_parts]
        if inverses is None:
            inverses = [eye - part for part in parts]
        else:
            firsts = [mm(part, inv) for part, inv in zip(parts, inverses)]
            inverses = [inv - mm(inv, first) for inv, first in zip(inverses, firsts)]
        size *= 2
    return inverses


def local_kernel(
    head_size,
    r_ref,
    k_ref,
    v_ref,
    d_ref,
    l_ref,
    base_ref,
    shift_ref,
    reader_ref,
    local_ref,
    summary_ref,
    state,
):
    pair = pl.program_id(0)
    half = LANES // 2

    rows = grid_index((SPAN, SPAN), 0)
    cols = grid_index((SPAN, SPAN), 1)
    strict = rows > cols
    inclusive = rows >= cols
    first = grid_index((SPAN, LANES), 1) < half
    matched = same_head(head_size)
    block = matched.astype(BF16)
    diagonal = grid_index((LANES, LANES), 0) == grid_index((LANES, LANES), 1)
    tri = inclusive.astype(BF16)
    tri_two = jnp.concatenate([tri, tri], axis=1)

    state[:LANES] = jnp.zeros((LANES, LANES), F32)
    state[LANES:] = jnp.where(diagonal, 1.0, 0.0)

    heads = shift_ref.shape[1]
    chosen = grid_index((heads, LANES), 0) == 2 * pair + grid_index((heads, LANES), 1) // half

    def advance(step, nothing):
        start = pl.multiple_of(step * (STACK * SPAN), STACK * SPAN)
        rows_here = pl.ds(start, STACK * SPAN)
        shift = lax.dot_general(
            shift_ref[rows_here],
            chosen.astype(F32),
            (((1,), (0,)), ((), ())),
            precision=lax.Precision.HIGHEST,
            preferred_element_type=F32,
        )
        pre = d_ref[rows_here].astype(F32) + base_ref[0] + shift
        log_all = -0.6065306597126334 / (1.0 + jnp.exp(-pre))
        rates = 1.0 / (1.0 + jnp.exp(-l_ref[rows_here].astype(F32)))
        key_all = k_ref[rows_here].astype(F32)
        unit_all = key_all * lax.rsqrt(head_sums(key_all * key_all, block) + KEY_EPS)
        removal_all = unit_all * rates

        spans = STACK
        items = []
        strict_parts = []
        for j in range(spans):
            here = slice(j * SPAN, (j + 1) * SPAN)
            log_decay = log_all[here]
            high, low = split_two(log_decay)
            cum = mm(tri_two, jnp.concatenate([high, low], axis=0))
            middle = cum[SPAN // 2 - 1 : SPAN // 2]
            ending = cum[SPAN - 1 :]
            e_cm = jnp.exp(cum - middle)
            e_pm = jnp.exp(cum - log_decay - middle)
            shrink = jnp.exp(middle - cum)
            e_mid = jnp.exp(middle)
            e_tail = jnp.exp(ending - middle)
            unit, key = unit_all[here], key_all[here]
            value = v_ref[pl.ds(start + j * SPAN, SPAN)]
            turned = jnp.concatenate([value[:, half:], value[:, :half]], axis=1)
            recept = r_ref[pl.ds(start + j * SPAN, SPAN)].astype(F32)
            probes = unit * e_pm
            queries = recept * e_cm
            back_removal = removal_all[here] * shrink
            back_keys = key * shrink
            left = jnp.concatenate(
                [
                    jnp.where(first, probes, 0.0),
                    jnp.where(first, 0.0, probes),
                    jnp.where(first, queries, 0.0),
                    jnp.where(first, 0.0, queries),
                ],
                axis=0,
            )
            products = mm_nt(left, jnp.concatenate([back_removal, back_keys], axis=0))
            for h in range(2):
                strict_parts.append(
                    jnp.where(strict, products[h * SPAN : (h + 1) * SPAN, :SPAN], 0.0)
                )
            items.append(
                dict(
                    products=products,
                    turned=turned,
                    carrying=probes * e_mid,
                    reading=queries * e_mid,
                    removal_tail=back_removal * e_tail,
                    key_tail=back_keys * e_tail,
                    fade=jnp.exp(ending),
                )
            )
        inverses = lower_inverses(strict_parts, rows, cols)
        for j in range(spans):
            item = items[j]
            products, turned = item["products"], item["turned"]
            solved, removed, kept = [], [], []
            for h in range(2):
                top = slice(h * SPAN, (h + 1) * SPAN)
                bottom = slice((2 + h) * SPAN, (3 + h) * SPAN)
                pair_keys = jnp.where(strict, products[top, SPAN:], 0.0)
                read_removal = jnp.where(inclusive, products[bottom, :SPAN], 0.0)
                read_keys = jnp.where(inclusive, products[bottom, SPAN:], 0.0)
                both = mm(jnp.concatenate([pair_keys, read_keys], axis=0), turned)
                own = first if h == 0 else jnp.logical_not(first)
                right = jnp.where(own, item["carrying"], both[:SPAN])
                answer = mm(inverses[2 * j + h], right)
                solved.append(answer)
                removed.append(mm(read_removal, answer))
                kept.append(both[SPAN:])
            carried = jnp.where(first, solved[0], solved[1])
            local_turned = jnp.where(first, solved[1], solved[0])
            reader = item["reading"] - jnp.where(first, removed[0], removed[1])
            read_turned = jnp.where(first, kept[1] - removed[1], kept[0] - removed[0])
            local_read = jnp.concatenate([read_turned[:, half:], read_turned[:, :half]], axis=1)
            taken = mm_tn(
                jnp.concatenate([carried, local_turned], axis=1), item["removal_tail"]
            )
            offset_turned = mm_tn(turned, item["key_tail"]) - taken[LANES:]
            offset = jnp.concatenate([offset_turned[half:], offset_turned[:half]], axis=0)
            offset = jnp.where(matched, offset, 0.0)
            transition = jnp.where(diagonal, item["fade"], 0.0) - jnp.where(
                matched, taken[:LANES], 0.0
            )
            now = state[...]
            reads = mm_nt(reader, now)
            here = pl.ds(start + j * SPAN, SPAN)
            local_ref[here] = local_read + reads[:, :LANES]
            reader_ref[pl.ds(start + j * SPAN, SPAN)] = reads[:, LANES:].astype(BF16)
            now_high, now_low = split_two(now)
            step_high, step_low = split_two(transition)
            moved = mm(now_high, step_high) + mm(now_low, step_high) + mm(now_high, step_low)
            state[:LANES] = moved[:LANES] + offset
            state[LANES:] = moved[LANES:]
        return nothing

    lax.fori_loop(0, r_ref.shape[0] // (STACK * SPAN), advance, 0)
    summary_ref[1] = (state[:half] + state[half:LANES]).astype(BF16)
    summary_ref[0] = (state[LANES : LANES + half] + state[LANES + half :]).astype(BF16)


def mixer_local(receptance, keys, values, decay, learn, base, shift, head_size):
    rows, channels = receptance.shape
    pairs = channels // LANES
    heads = shift.shape[1]
    half = LANES // 2
    tile = pl.BlockSpec((rows, LANES), lambda p: (0, p))
    small = pl.BlockSpec((2, half, LANES), lambda p: (0, p, 0))
    return pl.pallas_call(
        functools.partial(local_kernel, head_size),
        grid=(pairs,),
        in_specs=[tile] * 5
        + [
            pl.BlockSpec((1, 1, LANES), lambda p: (p, 0, 0)),
            pl.BlockSpec((rows, heads), lambda p: (0, 0)),
        ],
        out_specs=[tile, tile, small],
        out_shape=[
            jax.ShapeDtypeStruct((rows, channels), BF16),
            jax.ShapeDtypeStruct((rows, channels), F32),
            jax.ShapeDtypeStruct((2, pairs * half, LANES), BF16),
        ],
        scratch_shapes=[pltpu.VMEM((2 * LANES, LANES), F32)],
        compiler_params=pltpu.CompilerParams(
            dimension_semantics=("arbitrary",), vmem_limit_bytes=24 * 2**20
        ),
        cost_estimate=pl.CostEstimate(
            flops=20 * 10**9, bytes_accessed=6 * 2**20, transcendentals=10**6
        ),
        name="mixer_local",
    )(receptance, keys, values, decay, learn, base.reshape(pairs, 1, LANES), shift)


def finish_kernel(
    head_size,
    summary_ref,
    reader_ref,
    local_ref,
    gain_ref,
    out_ref,
    landed,
    send_sems,
    recv_sems,
):
    here = lax.axis_index("ep")
    count = lax.axis_size("ep")
    half = LANES // 2
    _, channels = reader_ref.shape
    pairs = channels // LANES
    matched = same_head(head_size)
    block = matched.astype(BF16)

    def transfer(distance, target):
        return pltpu.make_async_remote_copy(
            src_ref=summary_ref,
            dst_ref=landed.at[distance - 1],
            send_sem=send_sems.at[distance - 1],
            recv_sem=recv_sems.at[distance - 1],
            device_id={"ep": target},
            device_id_type=pl.DeviceIdType.MESH,
        )

    barrier = pltpu.get_barrier_semaphore()

    def greet(distance, nothing):
        pl.semaphore_signal(
            barrier,
            inc=1,
            device_id={"ep": lax.rem(here + distance, count)},
            device_id_type=pl.DeviceIdType.MESH,
        )
        return nothing

    lax.fori_loop(1, count, greet, 0)
    pl.semaphore_wait(barrier, count - 1)

    def launch(distance, nothing):
        transfer(distance, here + distance).start()
        return nothing

    lax.fori_loop(1, count - here, launch, 0)

    def wide(place, kind, p):
        part = landed[place, kind, p * half : (p + 1) * half].astype(F32)
        return jnp.where(matched, jnp.concatenate([part, part], axis=0), 0.0)

    def turn(k, states):
        distance = here - k
        transfer(distance, k).wait_recv()
        after = []
        for p in range(pairs):
            high, low = split_two(states[p])
            moved = mm(jnp.concatenate([high, low], axis=0), wide(distance - 1, 0, p))
            after.append(moved[:LANES] + moved[LANES:] + wide(distance - 1, 1, p))
        return tuple(after)

    nothing = tuple(jnp.zeros((LANES, LANES), F32) for _ in range(pairs))
    entering = lax.fori_loop(0, here, turn, nothing)
    for p in range(pairs):
        lanes = slice(p * LANES, (p + 1) * LANES)
        read = mm_nt(reader_ref[:, lanes], entering[p]) + local_ref[:, lanes]
        centred = read - head_sums(read, block) * (1.0 / head_size)
        variance = head_sums(centred * centred, block) * (1.0 / head_size)
        scaled = centred * lax.rsqrt(variance + GROUP_EPS) * gain_ref[:, lanes]
        out_ref[:, lanes] = scaled.astype(BF16)

    def settle(distance, nothing):
        transfer(distance, here + distance).wait_send()
        return nothing

    lax.fori_loop(1, count - here, settle, 0)


def mixer_finish(summary, reader, local_read, gain, head_size):
    rows, channels = reader.shape
    count = lax.axis_size("ep")
    return pl.pallas_call(
        functools.partial(finish_kernel, head_size),
        in_specs=[pl.BlockSpec(memory_space=pltpu.VMEM)] * 4,
        out_specs=pl.BlockSpec(memory_space=pltpu.VMEM),
        out_shape=jax.ShapeDtypeStruct((rows, channels), BF16),
        scratch_shapes=[
            pltpu.VMEM((count - 1,) + summary.shape, BF16),
            pltpu.SemaphoreType.DMA((count - 1,)),
            pltpu.SemaphoreType.DMA((count - 1,)),
        ],
        compiler_params=pltpu.CompilerParams(
            vmem_limit_bytes=32 * 2**20, collective_id=0, has_side_effects=True
        ),
        cost_estimate=pl.CostEstimate(
            flops=10 * 10**9, bytes_accessed=4 * 2**20, transcendentals=10**5
        ),
        name="mixer_finish",
    )(summary, reader, local_read, gain.reshape(1, channels))


def part_kernel(shards, started, *refs):
    x_ref = refs[0]
    weights = refs[1 : 1 + 3 * shards]
    total_ref = refs[1 + 3 * shards] if started else None
    out_ref = refs[-1]
    rows = x_ref.shape[0]
    piece = min(rows, 256)

    def block(step, nothing):
        here = pl.ds(pl.multiple_of(step * piece, piece), piece)
        x = x_ref[here]
        total = total_ref[here] if started else None
        for s in range(shards):
            gate, up, down = weights[3 * s : 3 * s + 3]
            gates = mm(x, gate[...])
            uppers = mm(x, up[...])
            hidden = (gates / (1.0 + jnp.exp(-gates)) * uppers).astype(BF16)
            term = mm(hidden, down[...])
            total = term if total is None else total + term
        out_ref[here] = total.astype(out_ref.dtype)
        return nothing

    lax.fori_loop(0, rows // piece, block, 0)


def expert_part(incoming, weights, total, out_type):
    rows, width = incoming.shape
    shards = len(weights)
    units = weights[0][0].shape[1]
    started = total is not None
    flat = [array for shard in weights for array in shard]
    operands = [incoming] + flat + ([total] if started else [])
    return pl.pallas_call(
        functools.partial(part_kernel, shards, started),
        in_specs=[pl.BlockSpec(memory_space=pltpu.VMEM)] * len(operands),
        out_specs=pl.BlockSpec(memory_space=pltpu.VMEM),
        out_shape=jax.ShapeDtypeStruct((rows, width), out_type),
        compiler_params=pltpu.CompilerParams(vmem_limit_bytes=32 * 2**20),
        cost_estimate=pl.CostEstimate(
            flops=6 * rows * width * units * shards,
            bytes_accessed=2 * (rows * width + 3 * shards * units * width),
            transcendentals=rows * units * shards,
        ),
        name="expert_part",
    )(*operands)


def swap(x, distance):
    count = lax.axis_size("tp")
    return lax.ppermute(x, "tp", [(i, i ^ distance) for i in range(count)])


def spread_sum(term):
    rows, width = term.shape
    count = lax.axis_size("tp")
    place = lax.axis_index("tp")
    block = rows // count
    parts = term.reshape(count // 2, 2, block, width)
    low = place % 2
    kept = lax.dynamic_index_in_dim(parts, low, 1, keepdims=False)
    sent = lax.dynamic_index_in_dim(parts, 1 - low, 1, keepdims=False)
    pair = (kept.astype(F32) + swap(sent, 1).astype(F32)).astype(BF16)
    high = place // 2
    kept = lax.dynamic_index_in_dim(pair, high, 0, keepdims=False)
    sent = lax.dynamic_index_in_dim(pair, 1 - high, 0, keepdims=False)
    return (kept.astype(F32) + swap(sent, 2).astype(F32)).astype(BF16)


def slot_targets(block_routes, capacity):
    flat_routes = block_routes.reshape(-1)
    count = flat_routes.shape[0]
    order = jnp.arange(count, dtype=jnp.int32)
    before = (order[:, None] > order[None, :]) & (flat_routes[:, None] == flat_routes[None, :])
    slots = jnp.sum(before.astype(jnp.int32), axis=1).reshape(block_routes.shape)
    return block_routes * capacity + slots


def dispersal_table(targets, places):
    marks = (jnp.arange(places, dtype=jnp.int32)[:, None, None] == targets[None, :, :]).astype(
        jnp.int32
    )
    return jnp.sum(marks, axis=2).astype(jnp.bfloat16)


def one_device(
    receptance,
    key_rows,
    value_rows,
    decay_input,
    learn_input,
    decay_base,
    decay_shift,
    channel_gain,
    out_weight,
    expert_input,
    expert_gain,
    routes,
    route_weight,
    gate_weight,
    up_weight,
    down_weight,
):
    ep_count = lax.axis_size("ep")
    channels = receptance.shape[1]
    head_size = channels // decay_shift.shape[1]
    token_rows, model_width = expert_input.shape
    top_count = routes.shape[1]
    experts = gate_weight.shape[0] * ep_count
    capacity = max(2, 2 * token_rows * top_count // experts)
    slab_rows = ep_count * capacity

    own = (gate_weight[0], up_weight[0], down_weight[0])
    far = tuple(swap(array, 2) for array in own)
    near = tuple(swap(array, 1) for array in own)

    inputs = expert_input.astype(F32)
    expert_normed = (
        inputs
        * lax.rsqrt(jnp.mean(inputs * inputs, axis=1, keepdims=True) + NORM_EPS)
        * expert_gain
    ).astype(BF16)
    own_targets = slot_targets(routes, capacity)
    outgoing = jnp.dot(
        dispersal_table(own_targets, experts * capacity),
        expert_normed,
        preferred_element_type=F32,
    ).astype(BF16)
    arrived = lax.all_to_all(
        outgoing.reshape(experts, capacity, model_width),
        "ep",
        split_axis=0,
        concat_axis=0,
        tiled=True,
    ).reshape(slab_rows, model_width)

    reader, local_read, summary = mixer_local(
        receptance,
        key_rows,
        value_rows,
        decay_input,
        learn_input,
        decay_base,
        decay_shift,
        head_size,
    )
    mixed = mixer_finish(summary, reader, local_read, channel_gain, head_size)
    far_gate, far_up, arrived, mixed = lax.optimization_barrier(
        (far[0], far[1], arrived, mixed)
    )
    cross_gate, cross_up = swap(far_gate, 1), swap(far_up, 1)
    mixer_term = jnp.dot(mixed, out_weight, preferred_element_type=F32)
    first = expert_part(arrived, (own, near), None, F32)
    far_down, first, mixer_term = lax.optimization_barrier((far[2], first, mixer_term))
    cross_down = swap(far_down, 1)
    total = expert_part(
        arrived,
        ((far_gate, far_up, far_down), (cross_gate, cross_up, cross_down)),
        first,
        BF16,
    )
    total, mixer_term = lax.optimization_barrier((total, mixer_term))
    mixer_out = spread_sum(mixer_term.astype(BF16))
    returned = lax.all_to_all(
        total.reshape(ep_count, capacity, model_width),
        "ep",
        split_axis=0,
        concat_axis=0,
        tiled=True,
    )
    flat_rows = returned.reshape(experts * capacity, model_width)
    places = jnp.arange(experts * capacity, dtype=jnp.int32)
    combined = jnp.zeros((token_rows, model_width), F32)
    for picked in range(top_count):
        table = (own_targets[:, picked : picked + 1] == places[None, :]).astype(BF16)
        chosen = jnp.dot(table, flat_rows, preferred_element_type=F32)
        combined = combined + chosen * route_weight[:, picked : picked + 1]
    return (mixer_out, combined.astype(BF16))


def solution(mesh):
    return jax.shard_map(
        one_device,
        mesh=mesh,
        in_specs=(
            P("ep", "tp"),
            P("ep", "tp"),
            P("ep", "tp"),
            P("ep", "tp"),
            P("ep", "tp"),
            P("tp"),
            P("ep", "tp"),
            P("tp"),
            P("tp", None),
            P(("ep", "tp"), None),
            P(),
            P(("ep", "tp"), None),
            P(("ep", "tp"), None),
            P("ep", None, "tp"),
            P("ep", None, "tp"),
            P("ep", "tp", None),
        ),
        out_specs=(P(("ep", "tp"), None), P(("ep", "tp"), None)),
        check_vma=False,
    )
```

```python
import functools

import jax
import jax.numpy as jnp
from jax import lax
from jax.experimental import pallas as pl
from jax.experimental.pallas import tpu as pltpu
from jax.sharding import PartitionSpec as P


SPAN = 128
STACK = 2
LANES = 128

NORM_EPS = 1e-06
GROUP_EPS = 0.00064
KEY_EPS = 1e-06
F32 = jnp.float32
BF16 = jnp.bfloat16


def mm(a, b):
    return lax.dot_general(
        a.astype(BF16), b.astype(BF16), (((1,), (0,)), ((), ())), preferred_element_type=F32
    )


def mm_nt(a, b):
    return lax.dot_general(
        a.astype(BF16), b.astype(BF16), (((1,), (1,)), ((), ())), preferred_element_type=F32
    )


def mm_tn(a, b):
    return lax.dot_general(
        a.astype(BF16), b.astype(BF16), (((0,), (0,)), ((), ())), preferred_element_type=F32
    )


def split_two(x):
    high = x.astype(BF16)
    return high, (x - high.astype(F32)).astype(BF16)


def grid_index(shape, axis):
    return lax.broadcasted_iota(jnp.int32, shape, axis)


def same_head(head_size):
    rows = grid_index((LANES, LANES), 0) // head_size
    cols = grid_index((LANES, LANES), 1) // head_size
    return rows == cols


def head_sums(x, block):
    high, low = split_two(x)
    return mm(
        jnp.concatenate([high, low], axis=1), jnp.concatenate([block, block], axis=0)
    )


def lower_inverses(strict_parts, rows, cols):
    eye = jnp.where(rows == cols, 1.0, 0.0)
    size = 1
    inverses = None
    while size < SPAN:
        off = (rows // (2 * size) == cols // (2 * size)) & (rows // size != cols // size)
        parts = [jnp.where(off, part, 0.0) for part in strict_parts]
        if inverses is None:
            inverses = [eye - part for part in parts]
        else:
            firsts = [mm(part, inv) for part, inv in zip(parts, inverses)]
            inverses = [inv - mm(inv, first) for inv, first in zip(inverses, firsts)]
        size *= 2
    return inverses


def local_kernel(
    head_size,
    r_ref,
    k_ref,
    v_ref,
    d_ref,
    l_ref,
    base_ref,
    shift_ref,
    reader_ref,
    local_ref,
    summary_ref,
    state,
):
    pair = pl.program_id(0)
    half = LANES // 2

    rows = grid_index((SPAN, SPAN), 0)
    cols = grid_index((SPAN, SPAN), 1)
    strict = rows > cols
    inclusive = rows >= cols
    first = grid_index((SPAN, LANES), 1) < half
    matched = same_head(head_size)
    block = matched.astype(BF16)
    diagonal = grid_index((LANES, LANES), 0) == grid_index((LANES, LANES), 1)
    tri = inclusive.astype(BF16)
    tri_two = jnp.concatenate([tri, tri], axis=1)

    state[:LANES] = jnp.zeros((LANES, LANES), F32)
    state[LANES:] = jnp.where(diagonal, 1.0, 0.0)

    heads = shift_ref.shape[1]
    chosen = grid_index((heads, LANES), 0) == 2 * pair + grid_index((heads, LANES), 1) // half

    def advance(step, nothing):
        start = pl.multiple_of(step * (STACK * SPAN), STACK * SPAN)
        rows_here = pl.ds(start, STACK * SPAN)
        shift = lax.dot_general(
            shift_ref[rows_here],
            chosen.astype(F32),
            (((1,), (0,)), ((), ())),
            precision=lax.Precision.HIGHEST,
            preferred_element_type=F32,
        )
        pre = d_ref[rows_here].astype(F32) + base_ref[0] + shift
        log_all = -0.6065306597126334 / (1.0 + jnp.exp(-pre))
        rates = 1.0 / (1.0 + jnp.exp(-l_ref[rows_here].astype(F32)))
        key_all = k_ref[rows_here].astype(F32)
        unit_all = key_all * lax.rsqrt(head_sums(key_all * key_all, block) + KEY_EPS)
        removal_all = unit_all * rates

        spans = STACK
        items = []
        strict_parts = []
        for j in range(spans):
            here = slice(j * SPAN, (j + 1) * SPAN)
            log_decay = log_all[here]
            high, low = split_two(log_decay)
            cum = mm(tri_two, jnp.concatenate([high, low], axis=0))
            middle = cum[SPAN // 2 - 1 : SPAN // 2]
            ending = cum[SPAN - 1 :]
            e_cm = jnp.exp(cum - middle)
            e_pm = jnp.exp(cum - log_decay - middle)
            shrink = jnp.exp(middle - cum)
            e_mid = jnp.exp(middle)
            e_tail = jnp.exp(ending - middle)
            unit, key = unit_all[here], key_all[here]
            value = v_ref[pl.ds(start + j * SPAN, SPAN)]
            turned = jnp.concatenate([value[:, half:], value[:, :half]], axis=1)
            recept = r_ref[pl.ds(start + j * SPAN, SPAN)].astype(F32)
            probes = unit * e_pm
            queries = recept * e_cm
            back_removal = removal_all[here] * shrink
            back_keys = key * shrink
            left = jnp.concatenate(
                [
                    jnp.where(first, probes, 0.0),
                    jnp.where(first, 0.0, probes),
                    jnp.where(first, queries, 0.0),
                    jnp.where(first, 0.0, queries),
                ],
                axis=0,
            )
            products = mm_nt(left, jnp.concatenate([back_removal, back_keys], axis=0))
            for h in range(2):
                strict_parts.append(
                    jnp.where(strict, products[h * SPAN : (h + 1) * SPAN, :SPAN], 0.0)
                )
            items.append(
                dict(
                    products=products,
                    turned=turned,
                    carrying=probes * e_mid,
                    reading=queries * e_mid,
                    removal_tail=back_removal * e_tail,
                    key_tail=back_keys * e_tail,
                    fade=jnp.exp(ending),
                )
            )
        inverses = lower_inverses(strict_parts, rows, cols)
        for j in range(spans):
            item = items[j]
            products, turned = item["products"], item["turned"]
            solved, removed, kept = [], [], []
            for h in range(2):
                top = slice(h * SPAN, (h + 1) * SPAN)
                bottom = slice((2 + h) * SPAN, (3 + h) * SPAN)
                pair_keys = jnp.where(strict, products[top, SPAN:], 0.0)
                read_removal = jnp.where(inclusive, products[bottom, :SPAN], 0.0)
                read_keys = jnp.where(inclusive, products[bottom, SPAN:], 0.0)
                both = mm(jnp.concatenate([pair_keys, read_keys], axis=0), turned)
                own = first if h == 0 else jnp.logical_not(first)
                right = jnp.where(own, item["carrying"], both[:SPAN])
                answer = mm(inverses[2 * j + h], right)
                solved.append(answer)
                removed.append(mm(read_removal, answer))
                kept.append(both[SPAN:])
            carried = jnp.where(first, solved[0], solved[1])
            local_turned = jnp.where(first, solved[1], solved[0])
            reader = item["reading"] - jnp.where(first, removed[0], removed[1])
            read_turned = jnp.where(first, kept[1] - removed[1], kept[0] - removed[0])
            local_read = jnp.concatenate([read_turned[:, half:], read_turned[:, :half]], axis=1)
            taken = mm_tn(
                jnp.concatenate([carried, local_turned], axis=1), item["removal_tail"]
            )
            offset_turned = mm_tn(turned, item["key_tail"]) - taken[LANES:]
            offset = jnp.concatenate([offset_turned[half:], offset_turned[:half]], axis=0)
            offset = jnp.where(matched, offset, 0.0)
            transition = jnp.where(diagonal, item["fade"], 0.0) - jnp.where(
                matched, taken[:LANES], 0.0
            )
            now = state[...]
            reads = mm_nt(reader, now)
            here = pl.ds(start + j * SPAN, SPAN)
            local_ref[here] = local_read + reads[:, :LANES]
            reader_ref[pl.ds(start + j * SPAN, SPAN)] = reads[:, LANES:].astype(BF16)
            now_high, now_low = split_two(now)
            step_high, step_low = split_two(transition)
            moved = mm(now_high, step_high) + mm(now_low, step_high) + mm(now_high, step_low)
            state[:LANES] = moved[:LANES] + offset
            state[LANES:] = moved[LANES:]
        return nothing

    lax.fori_loop(0, r_ref.shape[0] // (STACK * SPAN), advance, 0)
    summary_ref[1] = (state[:half] + state[half:LANES]).astype(BF16)
    summary_ref[0] = (state[LANES : LANES + half] + state[LANES + half :]).astype(BF16)


def mixer_local(receptance, keys, values, decay, learn, base, shift, head_size):
    rows, channels = receptance.shape
    pairs = channels // LANES
    heads = shift.shape[1]
    half = LANES // 2
    tile = pl.BlockSpec((rows, LANES), lambda p: (0, p))
    small = pl.BlockSpec((2, half, LANES), lambda p: (0, p, 0))
    streams = [
        pltpu.with_memory_space_constraint(array, pltpu.HBM)
        for array in (receptance, keys, values, decay, learn)
    ]
    return pl.pallas_call(
        functools.partial(local_kernel, head_size),
        grid=(pairs,),
        in_specs=[tile] * 5
        + [
            pl.BlockSpec((1, 1, LANES), lambda p: (p, 0, 0)),
            pl.BlockSpec((rows, heads), lambda p: (0, 0)),
        ],
        out_specs=[tile, tile, small],
        out_shape=[
            jax.ShapeDtypeStruct((rows, channels), BF16),
            jax.ShapeDtypeStruct((rows, channels), F32),
            jax.ShapeDtypeStruct((2, pairs * half, LANES), BF16),
        ],
        scratch_shapes=[pltpu.VMEM((2 * LANES, LANES), F32)],
        compiler_params=pltpu.CompilerParams(
            dimension_semantics=("arbitrary",), vmem_limit_bytes=24 * 2**20
        ),
        cost_estimate=pl.CostEstimate(
            flops=20 * 10**9, bytes_accessed=6 * 2**20, transcendentals=10**6
        ),
        name="mixer_local",
    )(*streams, base.reshape(pairs, 1, LANES), shift)


def finish_kernel(
    head_size,
    summary_ref,
    reader_ref,
    local_ref,
    gain_ref,
    out_ref,
    before,
    sending,
    landed,
    send_sems,
    recv_sems,
):
    here = lax.axis_index("ep")
    count = lax.axis_size("ep")
    rounds = landed.shape[0]
    half = LANES // 2
    _, channels = reader_ref.shape
    pairs = channels // LANES
    matched = same_head(head_size)
    block = matched.astype(BF16)
    diagonal = grid_index((LANES, LANES), 0) == grid_index((LANES, LANES), 1)

    def transfer(level, distance, target):
        return pltpu.make_async_remote_copy(
            src_ref=sending,
            dst_ref=landed.at[level],
            send_sem=send_sems.at[distance - 1],
            recv_sem=recv_sems.at[level],
            device_id={"ep": target},
            device_id_type=pl.DeviceIdType.MESH,
        )

    barrier = pltpu.get_barrier_semaphore()

    def greet(distance, nothing):
        pl.semaphore_signal(
            barrier,
            inc=1,
            device_id={"ep": lax.rem(here + distance, count)},
            device_id_type=pl.DeviceIdType.MESH,
        )
        return nothing

    lax.fori_loop(1, count, greet, 0)

    def wide(part):
        part = part.astype(F32)
        return jnp.where(matched, jnp.concatenate([part, part], axis=0), 0.0)

    def spot(p):
        return slice(p * half, (p + 1) * half)

    for p in range(pairs):
        before[0, p] = jnp.where(diagonal, 1.0, 0.0)
        before[1, p] = jnp.zeros((LANES, LANES), F32)
    pl.semaphore_wait(barrier, count - 1)

    for level in range(rounds):
        reach = 2**level

        @pl.when(lax.rem(here, 2 * reach) == reach - 1)
        def _(level=level, reach=reach):
            for p in range(pairs):
                both = jnp.concatenate([before[0, p], before[1, p]], axis=0)
                high, low = split_two(both)
                step = wide(summary_ref[0, spot(p)])
                moved = mm(high, step) + mm(low, step)
                after = moved[LANES:] + wide(summary_ref[1, spot(p)])
                sending[0, spot(p)] = (moved[:half] + moved[half:LANES]).astype(BF16)
                sending[1, spot(p)] = (after[:half] + after[half:]).astype(BF16)

            def launch(distance, nothing):
                transfer(level, distance, here + distance).start()
                return nothing

            lax.fori_loop(1, reach + 1, launch, 0)

        @pl.when(lax.rem(here // reach, 2) == 1)
        def _(level=level, reach=reach):
            transfer(level, 1, here).wait_recv()
            for p in range(pairs):
                both = jnp.concatenate(
                    [wide(landed[level, 0, spot(p)]), wide(landed[level, 1, spot(p)])], axis=0
                )
                high, low = split_two(before[0, p])
                moved = mm(both, high) + mm(both, low)
                before[0, p] = moved[:LANES]
                before[1, p] = moved[LANES:] + before[1, p]

    for p in range(pairs):
        lanes = slice(p * LANES, (p + 1) * LANES)
        read = mm_nt(reader_ref[:, lanes], before[1, p]) + local_ref[:, lanes]
        centred = read - head_sums(read, block) * (1.0 / head_size)
        variance = head_sums(centred * centred, block) * (1.0 / head_size)
        scaled = centred * lax.rsqrt(variance + GROUP_EPS) * gain_ref[:, lanes]
        out_ref[:, lanes] = scaled.astype(BF16)

    for level in range(rounds):
        reach = 2**level

        @pl.when(lax.rem(here, 2 * reach) == reach - 1)
        def _(level=level, reach=reach):
            def settle(distance, nothing):
                transfer(level, distance, here + distance).wait_send()
                return nothing

            lax.fori_loop(1, reach + 1, settle, 0)


def mixer_finish(summary, reader, local_read, gain, head_size):
    rows, channels = reader.shape
    pairs = channels // LANES
    count = lax.axis_size("ep")
    rounds = (count - 1).bit_length()
    return pl.pallas_call(
        functools.partial(finish_kernel, head_size),
        in_specs=[pl.BlockSpec(memory_space=pltpu.VMEM)] * 4,
        out_specs=pl.BlockSpec(memory_space=pltpu.VMEM),
        out_shape=jax.ShapeDtypeStruct((rows, channels), BF16),
        scratch_shapes=[
            pltpu.VMEM((2, pairs, LANES, LANES), F32),
            pltpu.VMEM(summary.shape, BF16),
            pltpu.VMEM((rounds,) + summary.shape, BF16),
            pltpu.SemaphoreType.DMA((count // 2,)),
            pltpu.SemaphoreType.DMA((rounds,)),
        ],
        compiler_params=pltpu.CompilerParams(
            vmem_limit_bytes=32 * 2**20, collective_id=0, has_side_effects=True
        ),
        cost_estimate=pl.CostEstimate(
            flops=10 * 10**9, bytes_accessed=4 * 2**20, transcendentals=10**5
        ),
        name="mixer_finish",
    )(summary, reader, local_read, gain.reshape(1, channels))


def gated(x, gate, up):
    gates = mm(x, gate)
    uppers = mm(x, up)
    return (gates / (1.0 + jnp.exp(-gates)) * uppers).astype(BF16)


def part_kernel(x_ref, *refs):
    weights, (total_ref, hidden_ref) = refs[:-2], refs[-2:]
    rows = x_ref.shape[0]
    units = weights[0].shape[1]
    piece = min(rows, 256)

    def block(step, nothing):
        here = pl.ds(pl.multiple_of(step * piece, piece), piece)
        x = x_ref[here]
        total = None
        for s in range(2):
            gate, up, down = weights[3 * s : 3 * s + 3]
            term = mm(gated(x, gate[...], up[...]), down[...])
            total = term if total is None else total + term
        total_ref[here] = total
        for s in range(2):
            gate, up = weights[6 + 2 * s : 8 + 2 * s]
            hidden_ref[here, s * units : (s + 1) * units] = gated(x, gate[...], up[...])
        return nothing

    lax.fori_loop(0, rows // piece, block, 0)


def expert_part(incoming, full, partial):
    rows, width = incoming.shape
    units = full[0][0].shape[1]
    flat = [array for shard in full + partial for array in shard]
    operands = [incoming] + flat
    return pl.pallas_call(
        part_kernel,
        in_specs=[pl.BlockSpec(memory_space=pltpu.VMEM)] * len(operands),
        out_specs=[pl.BlockSpec(memory_space=pltpu.VMEM)] * 2,
        out_shape=[
            jax.ShapeDtypeStruct((rows, width), F32),
            jax.ShapeDtypeStruct((rows, 2 * units), BF16),
        ],
        compiler_params=pltpu.CompilerParams(vmem_limit_bytes=32 * 2**20),
        cost_estimate=pl.CostEstimate(
            flops=20 * rows * width * units,
            bytes_accessed=2 * (rows * width + 10 * units * width),
            transcendentals=4 * rows * units,
        ),
        name="expert_part",
    )(*operands)


def return_kernel(
    capacity,
    mixed_ref,
    project_ref,
    total_ref,
    hidden_ref,
    far_ref,
    target_ref,
    weight_ref,
    mixer_ref,
    expert_ref,
    cross,
    staged,
    landed,
    term,
    near_in,
    pair_out,
    far_in,
    combined,
    send_sems,
    recv_sems,
    side_send,
    side_recv,
):
    here = lax.axis_index("ep")
    count = lax.axis_size("ep")
    place = lax.axis_index("tp")
    low, high = lax.rem(place, 2), place // 2
    beside = place + 1 - 2 * low
    across = place + 2 - 4 * high
    units = far_ref.shape[0]
    tokens = expert_ref.shape[0]

    def side(src, dst, index, target):
        return pltpu.make_async_remote_copy(
            src_ref=src,
            dst_ref=dst,
            send_sem=side_send.at[index],
            recv_sem=side_recv.at[index],
            device_id={"tp": target},
            device_id_type=pl.DeviceIdType.MESH,
        )

    def rows_of(member):
        return pl.ds(pl.multiple_of(member * capacity, capacity), capacity)

    def back(distance, member):
        return pltpu.make_async_remote_copy(
            src_ref=staged.at[rows_of(member)],
            dst_ref=landed.at[rows_of(here)],
            send_sem=send_sems.at[distance - 1],
            recv_sem=recv_sems.at[distance - 1],
            device_id={"ep": member},
            device_id_type=pl.DeviceIdType.MESH,
        )

    barrier = pltpu.get_barrier_semaphore()

    def greet(distance, nothing):
        pl.semaphore_signal(
            barrier,
            inc=1,
            device_id={"ep": lax.rem(here + distance, count)},
            device_id_type=pl.DeviceIdType.MESH,
        )
        return nothing

    lax.fori_loop(1, count, greet, 0)
    for target in (beside, across):
        pl.semaphore_signal(
            barrier,
            inc=1,
            device_id={"tp": target},
            device_id_type=pl.DeviceIdType.MESH,
        )
    pl.semaphore_wait(barrier, count + 1)

    forward = side(far_ref, cross, 0, beside)
    forward.start()
    forward.wait_recv()

    def finished(member):
        rows = rows_of(member)
        hidden = hidden_ref[rows]
        row = total_ref[rows] + mm(hidden[:, :units], far_ref[...])
        return (row + mm(hidden[:, units:], cross[...])).astype(BF16)

    def far_first(k):
        return count // 2 + ((k + 1) // 2) * (2 * lax.rem(k, 2) - 1)

    def send_block(k, nothing):
        distance = far_first(k)
        member = lax.rem(here + distance, count)
        staged[rows_of(member)] = finished(member)
        back(distance, member).start()
        return nothing

    lax.fori_loop(0, count - 1, send_block, 0)
    landed[rows_of(here)] = finished(here)

    def project(b, nothing):
        rows = pl.ds(pl.multiple_of(b * tokens, tokens), tokens)
        term[rows] = mm(mixed_ref[rows], project_ref[...]).astype(BF16)
        return nothing

    def block_rows(b):
        return pl.ds(pl.multiple_of(b * tokens, tokens), tokens)

    lax.fori_loop(0, 4, project, 0)
    nears = [
        side(term.at[block_rows(2 * y + 1 - low)], near_in.at[y], 1 + y, beside)
        for y in range(2)
    ]
    for copy in nears:
        copy.start()

    target = target_ref[...]
    weight = weight_ref[...]
    slot = grid_index((tokens, capacity), 1)

    def taken(member):
        table = jnp.zeros((tokens, capacity), F32)
        scale = jnp.zeros((tokens, 1), F32)
        for picked in range(target.shape[1]):
            own = target[:, picked : picked + 1] - member * capacity
            table = jnp.where(own == slot, 1.0, table)
            inside = (own >= 0) & (own < capacity)
            scale = jnp.where(inside, weight[:, picked : picked + 1], scale)
        return mm(table, landed[rows_of(member)]) * scale

    combined[...] = taken(here)

    for copy in nears:
        copy.wait_recv()
    other = 1 - high
    pair_out[...] = (
        term[block_rows(2 * other + low)].astype(F32) + near_in[other].astype(F32)
    ).astype(BF16)
    cross_send = side(pair_out, far_in, 3, across)
    cross_send.start()

    def gather_block(k, nothing):
        distance = far_first(count - 2 - k)
        member = lax.rem(here + count - distance, count)
        back(distance, member).wait_recv()
        combined[...] += taken(member)
        return nothing

    lax.fori_loop(0, count // 2, gather_block, 0)
    cross_send.wait_recv()
    kept = term[block_rows(2 * high + low)].astype(F32) + near_in[high].astype(F32)
    mixer_ref[...] = (kept + far_in[...].astype(F32)).astype(BF16)
    lax.fori_loop(count // 2, count - 1, gather_block, 0)
    expert_ref[...] = combined[...].astype(BF16)

    def settle(k, nothing):
        distance = far_first(k)
        back(distance, lax.rem(here + distance, count)).wait_send()
        return nothing

    lax.fori_loop(0, count - 1, settle, 0)
    for copy in [forward] + nears + [cross_send]:
        copy.wait_send()


def return_rows(mixed, out_weight, total, hidden, far_down, targets, route_weight, capacity):
    count = lax.axis_size("ep")
    rows, width = total.shape
    tokens = targets.shape[0]
    operands = (mixed, out_weight, total, hidden, far_down, targets, route_weight)
    return pl.pallas_call(
        functools.partial(return_kernel, capacity),
        in_specs=[pl.BlockSpec(memory_space=pltpu.VMEM)] * len(operands),
        out_specs=[pl.BlockSpec(memory_space=pltpu.VMEM)] * 2,
        out_shape=[jax.ShapeDtypeStruct((tokens, width), BF16)] * 2,
        scratch_shapes=[
            pltpu.VMEM(far_down.shape, BF16),
            pltpu.VMEM((rows, width), BF16),
            pltpu.VMEM((rows, width), BF16),
            pltpu.VMEM((mixed.shape[0], width), BF16),
            pltpu.VMEM((2, tokens, width), BF16),
            pltpu.VMEM((tokens, width), BF16),
            pltpu.VMEM((tokens, width), BF16),
            pltpu.VMEM((tokens, width), F32),
            pltpu.SemaphoreType.DMA((count - 1,)),
            pltpu.SemaphoreType.DMA((count - 1,)),
            pltpu.SemaphoreType.DMA((4,)),
            pltpu.SemaphoreType.DMA((4,)),
        ],
        compiler_params=pltpu.CompilerParams(
            vmem_limit_bytes=40 * 2**20, collective_id=1, has_side_effects=True
        ),
        cost_estimate=pl.CostEstimate(
            flops=6 * 10**9, bytes_accessed=12 * 2**20, transcendentals=0
        ),
        name="return_rows",
    )(*operands)


def swap(x, distance):
    count = lax.axis_size("tp")
    return lax.ppermute(x, "tp", [(i, i ^ distance) for i in range(count)])


def slot_targets(block_routes, capacity):
    flat_routes = block_routes.reshape(-1)
    count = flat_routes.shape[0]
    order = jnp.arange(count, dtype=jnp.int32)
    before = (order[:, None] > order[None, :]) & (flat_routes[:, None] == flat_routes[None, :])
    slots = jnp.sum(before.astype(jnp.int32), axis=1).reshape(block_routes.shape)
    return block_routes * capacity + slots


def dispersal_table(targets, places):
    marks = (jnp.arange(places, dtype=jnp.int32)[:, None, None] == targets[None, :, :]).astype(
        jnp.int32
    )
    return jnp.sum(marks, axis=2).astype(jnp.bfloat16)


def one_device(
    receptance,
    key_rows,
    value_rows,
    decay_input,
    learn_input,
    decay_base,
    decay_shift,
    channel_gain,
    out_weight,
    expert_input,
    expert_gain,
    routes,
    route_weight,
    gate_weight,
    up_weight,
    down_weight,
):
    ep_count = lax.axis_size("ep")
    channels = receptance.shape[1]
    head_size = channels // decay_shift.shape[1]
    token_rows, model_width = expert_input.shape
    top_count = routes.shape[1]
    experts = gate_weight.shape[0] * ep_count
    capacity = max(2, 2 * token_rows * top_count // experts)
    slab_rows = ep_count * capacity

    own = (gate_weight[0], up_weight[0], down_weight[0])
    far = tuple(swap(array, 2) for array in own)
    near = tuple(swap(array, 1) for array in own)

    inputs = expert_input.astype(F32)
    expert_normed = (
        inputs
        * lax.rsqrt(jnp.mean(inputs * inputs, axis=1, keepdims=True) + NORM_EPS)
        * expert_gain
    ).astype(BF16)
    own_targets = slot_targets(routes, capacity)
    outgoing = jnp.dot(
        dispersal_table(own_targets, experts * capacity),
        expert_normed,
        preferred_element_type=F32,
    ).astype(BF16)
    arrived = lax.all_to_all(
        outgoing.reshape(experts, capacity, model_width),
        "ep",
        split_axis=0,
        concat_axis=0,
        tiled=True,
    ).reshape(slab_rows, model_width)

    reader, local_read, summary = mixer_local(
        receptance,
        key_rows,
        value_rows,
        decay_input,
        learn_input,
        decay_base,
        decay_shift,
        head_size,
    )
    cross = tuple(swap(array, 1) for array in far[:2])
    mixed = mixer_finish(summary, reader, local_read, channel_gain, head_size)
    total, hidden = expert_part(arrived, (own, near), (far[:2], cross))
    return tuple(
        return_rows(
            mixed, out_weight, total, hidden, far[2], own_targets, route_weight, capacity
        )
    )


def solution(mesh):
    return jax.shard_map(
        one_device,
        mesh=mesh,
        in_specs=(
            P("ep", "tp"),
            P("ep", "tp"),
            P("ep", "tp"),
            P("ep", "tp"),
            P("ep", "tp"),
            P("tp"),
            P("ep", "tp"),
            P("tp"),
            P("tp", None),
            P(("ep", "tp"), None),
            P(),
            P(("ep", "tp"), None),
            P(("ep", "tp"), None),
            P("ep", None, "tp"),
            P("ep", None, "tp"),
            P("ep", "tp", None),
        ),
        out_specs=(P(("ep", "tp"), None), P(("ep", "tp"), None)),
        check_vma=False,
    )
```

```python
import functools

import jax
import jax.numpy as jnp
from jax import lax
from jax.experimental import pallas as pl
from jax.experimental.pallas import tpu as pltpu
from jax.sharding import PartitionSpec as P


SPAN = 128
STACK = 2
LANES = 128

NORM_EPS = 1e-06
GROUP_EPS = 0.00064
KEY_EPS = 1e-06
F32 = jnp.float32
BF16 = jnp.bfloat16


def mm(a, b):
    return lax.dot_general(
        a.astype(BF16), b.astype(BF16), (((1,), (0,)), ((), ())), preferred_element_type=F32
    )


def mm_nt(a, b):
    return lax.dot_general(
        a.astype(BF16), b.astype(BF16), (((1,), (1,)), ((), ())), preferred_element_type=F32
    )


def mm_tn(a, b):
    return lax.dot_general(
        a.astype(BF16), b.astype(BF16), (((0,), (0,)), ((), ())), preferred_element_type=F32
    )


def split_two(x):
    high = x.astype(BF16)
    return high, (x - high.astype(F32)).astype(BF16)


def grid_index(shape, axis):
    return lax.broadcasted_iota(jnp.int32, shape, axis)


def same_head(head_size):
    rows = grid_index((LANES, LANES), 0) // head_size
    cols = grid_index((LANES, LANES), 1) // head_size
    return rows == cols


def head_sums(x, block):
    high, low = split_two(x)
    return mm(
        jnp.concatenate([high, low], axis=1), jnp.concatenate([block, block], axis=0)
    )


def lower_inverses(strict_parts, rows, cols):
    eye = jnp.where(rows == cols, 1.0, 0.0)
    size = 1
    inverses = None
    while size < SPAN:
        off = (rows // (2 * size) == cols // (2 * size)) & (rows // size != cols // size)
        parts = [jnp.where(off, part, 0.0) for part in strict_parts]
        if inverses is None:
            inverses = [eye - part for part in parts]
        else:
            firsts = [mm(part, inv) for part, inv in zip(parts, inverses)]
            inverses = [inv - mm(inv, first) for inv, first in zip(inverses, firsts)]
        size *= 2
    return inverses


def local_kernel(
    head_size,
    r_ref,
    k_ref,
    v_ref,
    d_ref,
    l_ref,
    base_ref,
    shift_ref,
    reader_ref,
    local_ref,
    summary_ref,
    state,
):
    pair = pl.program_id(0)
    half = LANES // 2

    rows = grid_index((SPAN, SPAN), 0)
    cols = grid_index((SPAN, SPAN), 1)
    strict = rows > cols
    inclusive = rows >= cols
    first = grid_index((SPAN, LANES), 1) < half
    matched = same_head(head_size)
    block = matched.astype(BF16)
    diagonal = grid_index((LANES, LANES), 0) == grid_index((LANES, LANES), 1)
    tri = inclusive.astype(BF16)
    tri_two = jnp.concatenate([tri, tri], axis=1)

    state[:LANES] = jnp.zeros((LANES, LANES), F32)
    state[LANES:] = jnp.where(diagonal, 1.0, 0.0)

    heads = shift_ref.shape[1]
    chosen = grid_index((heads, LANES), 0) == 2 * pair + grid_index((heads, LANES), 1) // half

    def advance(step, nothing):
        start = pl.multiple_of(step * (STACK * SPAN), STACK * SPAN)
        rows_here = pl.ds(start, STACK * SPAN)
        shift = lax.dot_general(
            shift_ref[rows_here],
            chosen.astype(F32),
            (((1,), (0,)), ((), ())),
            precision=lax.Precision.HIGHEST,
            preferred_element_type=F32,
        )
        pre = d_ref[rows_here].astype(F32) + base_ref[0] + shift
        log_all = -0.6065306597126334 / (1.0 + jnp.exp(-pre))
        rates = 1.0 / (1.0 + jnp.exp(-l_ref[rows_here].astype(F32)))
        key_all = k_ref[rows_here].astype(F32)
        unit_all = key_all * lax.rsqrt(head_sums(key_all * key_all, block) + KEY_EPS)
        removal_all = unit_all * rates

        spans = STACK
        items = []
        strict_parts = []
        for j in range(spans):
            here = slice(j * SPAN, (j + 1) * SPAN)
            log_decay = log_all[here]
            high, low = split_two(log_decay)
            cum = mm(tri_two, jnp.concatenate([high, low], axis=0))
            middle = cum[SPAN // 2 - 1 : SPAN // 2]
            ending = cum[SPAN - 1 :]
            e_cm = jnp.exp(cum - middle)
            e_pm = jnp.exp(cum - log_decay - middle)
            shrink = jnp.exp(middle - cum)
            e_mid = jnp.exp(middle)
            e_tail = jnp.exp(ending - middle)
            unit, key = unit_all[here], key_all[here]
            value = v_ref[pl.ds(start + j * SPAN, SPAN)]
            turned = jnp.concatenate([value[:, half:], value[:, :half]], axis=1)
            recept = r_ref[pl.ds(start + j * SPAN, SPAN)].astype(F32)
            probes = unit * e_pm
            queries = recept * e_cm
            back_removal = removal_all[here] * shrink
            back_keys = key * shrink
            left = jnp.concatenate(
                [
                    jnp.where(first, probes, 0.0),
                    jnp.where(first, 0.0, probes),
                    jnp.where(first, queries, 0.0),
                    jnp.where(first, 0.0, queries),
                ],
                axis=0,
            )
            products = mm_nt(left, jnp.concatenate([back_removal, back_keys], axis=0))
            for h in range(2):
                strict_parts.append(
                    jnp.where(strict, products[h * SPAN : (h + 1) * SPAN, :SPAN], 0.0)
                )
            items.append(
                dict(
                    products=products,
                    turned=turned,
                    carrying=probes * e_mid,
                    reading=queries * e_mid,
                    removal_tail=back_removal * e_tail,
                    key_tail=back_keys * e_tail,
                    fade=jnp.exp(ending),
                )
            )
        inverses = lower_inverses(strict_parts, rows, cols)
        for j in range(spans):
            item = items[j]
            products, turned = item["products"], item["turned"]
            solved, removed, kept = [], [], []
            for h in range(2):
                top = slice(h * SPAN, (h + 1) * SPAN)
                bottom = slice((2 + h) * SPAN, (3 + h) * SPAN)
                pair_keys = jnp.where(strict, products[top, SPAN:], 0.0)
                read_removal = jnp.where(inclusive, products[bottom, :SPAN], 0.0)
                read_keys = jnp.where(inclusive, products[bottom, SPAN:], 0.0)
                both = mm(jnp.concatenate([pair_keys, read_keys], axis=0), turned)
                own = first if h == 0 else jnp.logical_not(first)
                right = jnp.where(own, item["carrying"], both[:SPAN])
                answer = mm(inverses[2 * j + h], right)
                solved.append(answer)
                removed.append(mm(read_removal, answer))
                kept.append(both[SPAN:])
            carried = jnp.where(first, solved[0], solved[1])
            local_turned = jnp.where(first, solved[1], solved[0])
            reader = item["reading"] - jnp.where(first, removed[0], removed[1])
            read_turned = jnp.where(first, kept[1] - removed[1], kept[0] - removed[0])
            local_read = jnp.concatenate([read_turned[:, half:], read_turned[:, :half]], axis=1)
            taken = mm_tn(
                jnp.concatenate([carried, local_turned], axis=1), item["removal_tail"]
            )
            offset_turned = mm_tn(turned, item["key_tail"]) - taken[LANES:]
            offset = jnp.concatenate([offset_turned[half:], offset_turned[:half]], axis=0)
            offset = jnp.where(matched, offset, 0.0)
            transition = jnp.where(diagonal, item["fade"], 0.0) - jnp.where(
                matched, taken[:LANES], 0.0
            )
            now = state[...]
            reads = mm_nt(reader, now)
            here = pl.ds(start + j * SPAN, SPAN)
            local_ref[here] = local_read + reads[:, :LANES]
            reader_ref[pl.ds(start + j * SPAN, SPAN)] = reads[:, LANES:].astype(BF16)
            now_high, now_low = split_two(now)
            step_high, step_low = split_two(transition)
            moved = mm(now_high, step_high) + mm(now_low, step_high) + mm(now_high, step_low)
            state[:LANES] = moved[:LANES] + offset
            state[LANES:] = moved[LANES:]
        return nothing

    lax.fori_loop(0, r_ref.shape[0] // (STACK * SPAN), advance, 0)
    summary_ref[1] = (state[:half] + state[half:LANES]).astype(BF16)
    summary_ref[0] = (state[LANES : LANES + half] + state[LANES + half :]).astype(BF16)


def mixer_local(receptance, keys, values, decay, learn, base, shift, head_size):
    rows, channels = receptance.shape
    pairs = channels // LANES
    heads = shift.shape[1]
    half = LANES // 2
    tile = pl.BlockSpec((rows, LANES), lambda p: (0, p))
    small = pl.BlockSpec((2, half, LANES), lambda p: (0, p, 0))
    streams = [in_hbm(array) for array in (receptance, keys, values, decay, learn)]
    return pl.pallas_call(
        functools.partial(local_kernel, head_size),
        grid=(pairs,),
        in_specs=[tile] * 5
        + [
            pl.BlockSpec((1, 1, LANES), lambda p: (p, 0, 0)),
            pl.BlockSpec((rows, heads), lambda p: (0, 0)),
        ],
        out_specs=[tile, tile, small],
        out_shape=[
            jax.ShapeDtypeStruct((rows, channels), BF16),
            jax.ShapeDtypeStruct((rows, channels), F32),
            jax.ShapeDtypeStruct((2, pairs * half, LANES), BF16),
        ],
        scratch_shapes=[pltpu.VMEM((2 * LANES, LANES), F32)],
        compiler_params=pltpu.CompilerParams(
            dimension_semantics=("arbitrary",), vmem_limit_bytes=24 * 2**20
        ),
        cost_estimate=pl.CostEstimate(
            flops=20 * 10**9, bytes_accessed=6 * 2**20, transcendentals=10**6
        ),
        name="mixer_local",
    )(*streams, base.reshape(pairs, 1, LANES), shift)


def gated(x, gate, up):
    gates = mm(x, gate)
    uppers = mm(x, up)
    return (gates / (1.0 + jnp.exp(-gates)) * uppers).astype(BF16)


def send_to(src, dst, send_sem, recv_sem, target):
    return pltpu.make_async_remote_copy(
        src_ref=src,
        dst_ref=dst,
        send_sem=send_sem,
        recv_sem=recv_sem,
        device_id=target,
        device_id_type=pl.DeviceIdType.MESH,
    )


def greet_all(barrier, here, count, others):
    def greet(distance, nothing):
        pl.semaphore_signal(
            barrier,
            inc=1,
            device_id={"ep": lax.rem(here + distance, count)},
            device_id_type=pl.DeviceIdType.MESH,
        )
        return nothing

    lax.fori_loop(1, count, greet, 0)
    for target in others:
        pl.semaphore_signal(
            barrier, inc=1, device_id={"tp": target}, device_id_type=pl.DeviceIdType.MESH
        )


def part_kernel(
    head_size,
    x_ref,
    summary_ref,
    own_gate,
    own_up,
    own_down,
    near_gate,
    near_up,
    near_down,
    far_gate,
    far_up,
    total_ref,
    hidden_ref,
    entering_ref,
    held,
    held_down,
    cross,
    before,
    sending,
    landed,
    load_sems,
    send_sems,
    recv_sems,
    side_send,
    side_recv,
):
    here = lax.axis_index("ep")
    count = lax.axis_size("ep")
    place = lax.axis_index("tp")
    beside = place + 1 - 2 * lax.rem(place, 2)
    rounds = landed.shape[0]
    half = LANES // 2
    pairs = before.shape[1]
    rows = x_ref.shape[0]
    units = own_gate.shape[1]
    piece = min(rows, 256)
    matched = same_head(head_size)
    diagonal = grid_index((LANES, LANES), 0) == grid_index((LANES, LANES), 1)

    loads = [
        pltpu.make_async_copy(src, dst, load_sems.at[i])
        for i, (src, dst) in enumerate(
            [
                (own_gate, held.at[0]),
                (own_up, held.at[1]),
                (own_down, held_down.at[0]),
                (near_gate, held.at[2]),
                (near_up, held.at[3]),
                (near_down, held_down.at[1]),
                (far_gate, held.at[4]),
                (far_up, held.at[5]),
            ]
        )
    ]
    for load in loads:
        load.start()
    barrier = pltpu.get_barrier_semaphore()
    greet_all(barrier, here, count, (beside,))

    def transfer(level, distance, target):
        return send_to(
            sending,
            landed.at[level],
            send_sems.at[distance - 1],
            recv_sems.at[level],
            {"ep": target},
        )

    def wide(part):
        part = part.astype(F32)
        return jnp.where(matched, jnp.concatenate([part, part], axis=0), 0.0)

    def spot(p):
        return slice(p * half, (p + 1) * half)

    for p in range(pairs):
        before[0, p] = jnp.where(diagonal, 1.0, 0.0)
        before[1, p] = jnp.zeros((LANES, LANES), F32)
    pl.semaphore_wait(barrier, count)
    forwards = [
        send_to(src, cross.at[i], side_send.at[i], side_recv.at[i], {"tp": beside})
        for i, src in enumerate((far_gate, far_up))
    ]
    for forward in forwards:
        forward.start()

    def send_round(level):
        reach = 2**level

        @pl.when(lax.rem(here, 2 * reach) == reach - 1)
        def _():
            for p in range(pairs):
                both = jnp.concatenate([before[0, p], before[1, p]], axis=0)
                high, low = split_two(both)
                step = wide(summary_ref[0, spot(p)])
                moved = mm(high, step) + mm(low, step)
                after = moved[LANES:] + wide(summary_ref[1, spot(p)])
                sending[0, spot(p)] = (moved[:half] + moved[half:LANES]).astype(BF16)
                sending[1, spot(p)] = (after[:half] + after[half:]).astype(BF16)

            def launch(distance, nothing):
                transfer(level, distance, here + distance).start()
                return nothing

            lax.fori_loop(1, reach + 1, launch, 0)

    def take_round(level):
        reach = 2**level

        @pl.when(lax.rem(here // reach, 2) == 1)
        def _():
            transfer(level, 1, here).wait_recv()
            for p in range(pairs):
                both = jnp.concatenate(
                    [wide(landed[level, 0, spot(p)]), wide(landed[level, 1, spot(p)])], axis=0
                )
                high, low = split_two(before[0, p])
                moved = mm(both, high) + mm(both, low)
                before[0, p] = moved[:LANES]
                before[1, p] = moved[LANES:] + before[1, p]

    def over_rows(body):
        def step(i, nothing):
            body(pl.ds(pl.multiple_of(i * piece, piece), piece))
            return nothing

        lax.fori_loop(0, rows // piece, step, 0)

    def first_part(at):
        hidden = gated(x_ref[at], held[0], held[1])
        total_ref[at] = mm(hidden, held_down[0])

    def second_part(at):
        hidden = gated(x_ref[at], held[2], held[3])
        total_ref[at] += mm(hidden, held_down[1])

    def third_part(at):
        hidden_ref[at, :units] = gated(x_ref[at], held[4], held[5])

    def fourth_part(at):
        hidden_ref[at, units:] = gated(x_ref[at], cross[0], cross[1])

    send_round(0)
    bodies = (first_part, second_part, third_part, fourth_part)
    needs = (loads[:3], loads[3:6], loads[6:], ())
    for turn in range(max(len(bodies), rounds)):
        if turn < len(bodies):
            for load in needs[turn]:
                load.wait()
            if turn == len(bodies) - 1:
                for forward in forwards:
                    forward.wait_recv()
            over_rows(bodies[turn])
        if turn < rounds:
            take_round(turn)
            if turn + 1 < rounds:
                send_round(turn + 1)
    for p in range(pairs):
        entering_ref[p * LANES : (p + 1) * LANES] = before[1, p]

    for level in range(rounds):
        reach = 2**level

        @pl.when(lax.rem(here, 2 * reach) == reach - 1)
        def _(level=level, reach=reach):
            def settle(distance, nothing):
                transfer(level, distance, here + distance).wait_send()
                return nothing

            lax.fori_loop(1, reach + 1, settle, 0)

    for forward in forwards:
        forward.wait_send()


def in_hbm(array):
    return pltpu.with_memory_space_constraint(array, pltpu.HBM)


def expert_part(incoming, summary, own, near, far, head_size):
    rows, width = incoming.shape
    units = own[0].shape[1]
    pairs = summary.shape[1] * 2 // LANES
    count = lax.axis_size("ep")
    rounds = (count - 1).bit_length()
    weights = [in_hbm(array) for array in own + near + far]
    return pl.pallas_call(
        functools.partial(part_kernel, head_size),
        in_specs=[pl.BlockSpec(memory_space=pltpu.VMEM)] * 2
        + [pl.BlockSpec(memory_space=pl.ANY)] * len(weights),
        out_specs=[pl.BlockSpec(memory_space=pltpu.VMEM)] * 3,
        out_shape=[
            jax.ShapeDtypeStruct((rows, width), F32),
            jax.ShapeDtypeStruct((rows, 2 * units), BF16),
            jax.ShapeDtypeStruct((pairs * LANES, LANES), F32),
        ],
        scratch_shapes=[
            pltpu.VMEM((6, width, units), BF16),
            pltpu.VMEM((2, units, width), BF16),
            pltpu.VMEM((2, width, units), BF16),
            pltpu.VMEM((2, pairs, LANES, LANES), F32),
            pltpu.VMEM(summary.shape, BF16),
            pltpu.VMEM((rounds,) + summary.shape, BF16),
            pltpu.SemaphoreType.DMA((8,)),
            pltpu.SemaphoreType.DMA((count // 2,)),
            pltpu.SemaphoreType.DMA((rounds,)),
            pltpu.SemaphoreType.DMA((2,)),
            pltpu.SemaphoreType.DMA((2,)),
        ],
        compiler_params=pltpu.CompilerParams(
            vmem_limit_bytes=32 * 2**20, collective_id=0, has_side_effects=True
        ),
        cost_estimate=pl.CostEstimate(
            flops=20 * rows * width * units,
            bytes_accessed=2 * (rows * width + 10 * units * width),
            transcendentals=4 * rows * units,
        ),
        name="expert_part",
    )(incoming, summary, *weights)


def return_kernel(
    capacity,
    head_size,
    reader_ref,
    local_ref,
    project_ref,
    gain_ref,
    entering_ref,
    total_ref,
    hidden_ref,
    far_ref,
    target_ref,
    weight_ref,
    mixer_ref,
    expert_ref,
    reader,
    local,
    project,
    mixed,
    cross,
    staged,
    landed,
    term,
    near_in,
    pair_out,
    far_in,
    combined,
    load_sems,
    send_sems,
    recv_sems,
    side_send,
    side_recv,
):
    here = lax.axis_index("ep")
    count = lax.axis_size("ep")
    place = lax.axis_index("tp")
    low, high = lax.rem(place, 2), place // 2
    beside = place + 1 - 2 * low
    across = place + 2 - 4 * high
    units = far_ref.shape[0]
    tokens = expert_ref.shape[0]
    pairs = reader.shape[1] // LANES
    block = same_head(head_size).astype(BF16)

    def side(src, dst, index, target):
        return send_to(src, dst, side_send.at[index], side_recv.at[index], {"tp": target})

    def rows_of(member):
        return pl.ds(pl.multiple_of(member * capacity, capacity), capacity)

    def back(distance, member):
        return send_to(
            staged.at[rows_of(member)],
            landed.at[rows_of(here)],
            send_sems.at[distance - 1],
            recv_sems.at[distance - 1],
            {"ep": member},
        )

    barrier = pltpu.get_barrier_semaphore()
    greet_all(barrier, here, count, (beside, across))
    pl.semaphore_wait(barrier, count + 1)

    forward = side(far_ref, cross, 0, beside)
    forward.start()
    loads = [
        pltpu.make_async_copy(src, dst, load_sems.at[i])
        for i, (src, dst) in enumerate(
            [(reader_ref, reader), (local_ref, local), (project_ref, project)]
        )
    ]
    for load in loads:
        load.start()
    forward.wait_recv()

    def finished(member):
        rows = rows_of(member)
        hidden = hidden_ref[rows]
        row = total_ref[rows] + mm(hidden[:, :units], far_ref[...])
        return (row + mm(hidden[:, units:], cross[...])).astype(BF16)

    def far_first(k):
        return count // 2 + ((k + 1) // 2) * (2 * lax.rem(k, 2) - 1)

    def send_block(k, nothing):
        distance = far_first(k)
        member = lax.rem(here + distance, count)
        staged[rows_of(member)] = finished(member)
        back(distance, member).start()
        return nothing

    lax.fori_loop(0, count - 1, send_block, 0)
    landed[rows_of(here)] = finished(here)

    for load in loads:
        load.wait()
    for p in range(pairs):
        lanes = slice(p * LANES, (p + 1) * LANES)
        entering = entering_ref[p * LANES : (p + 1) * LANES]
        read = mm_nt(reader[:, lanes], entering) + local[:, lanes]
        centred = read - head_sums(read, block) * (1.0 / head_size)
        variance = head_sums(centred * centred, block) * (1.0 / head_size)
        scaled = centred * lax.rsqrt(variance + GROUP_EPS) * gain_ref[:, lanes]
        mixed[:, lanes] = scaled.astype(BF16)

    def block_rows(b):
        return pl.ds(pl.multiple_of(b * tokens, tokens), tokens)

    def project_block(b, nothing):
        rows = block_rows(b)
        term[rows] = mm(mixed[rows], project[...]).astype(BF16)
        return nothing

    lax.fori_loop(0, 4, project_block, 0)
    nears = [
        side(term.at[block_rows(2 * y + 1 - low)], near_in.at[y], 1 + y, beside)
        for y in range(2)
    ]
    for copy in nears:
        copy.start()

    target = target_ref[...]
    weight = weight_ref[...]
    slot = grid_index((tokens, capacity), 1)

    def taken(member):
        table = jnp.zeros((tokens, capacity), F32)
        scale = jnp.zeros((tokens, 1), F32)
        for picked in range(target.shape[1]):
            own = target[:, picked : picked + 1] - member * capacity
            table = jnp.where(own == slot, 1.0, table)
            inside = (own >= 0) & (own < capacity)
            scale = jnp.where(inside, weight[:, picked : picked + 1], scale)
        return mm(table, landed[rows_of(member)]) * scale

    combined[...] = taken(here)

    for copy in nears:
        copy.wait_recv()
    other = 1 - high
    pair_out[...] = (
        term[block_rows(2 * other + low)].astype(F32) + near_in[other].astype(F32)
    ).astype(BF16)
    cross_send = side(pair_out, far_in, 3, across)
    cross_send.start()

    def gather_block(k, nothing):
        distance = far_first(count - 2 - k)
        member = lax.rem(here + count - distance, count)
        back(distance, member).wait_recv()
        combined[...] += taken(member)
        return nothing

    lax.fori_loop(0, count // 2, gather_block, 0)
    cross_send.wait_recv()
    kept = term[block_rows(2 * high + low)].astype(F32) + near_in[high].astype(F32)
    mixer_ref[...] = (kept + far_in[...].astype(F32)).astype(BF16)
    lax.fori_loop(count // 2, count - 1, gather_block, 0)
    expert_ref[...] = combined[...].astype(BF16)

    def settle(k, nothing):
        distance = far_first(k)
        back(distance, lax.rem(here + distance, count)).wait_send()
        return nothing

    lax.fori_loop(0, count - 1, settle, 0)
    for copy in [forward] + nears + [cross_send]:
        copy.wait_send()


def return_rows(
    reader,
    local_read,
    out_weight,
    gain,
    entering,
    total,
    hidden,
    far_down,
    targets,
    route_weight,
    capacity,
    head_size,
):
    count = lax.axis_size("ep")
    rows, width = total.shape
    tokens = targets.shape[0]
    streamed = [in_hbm(array) for array in (reader, local_read, out_weight)]
    operands = (
        gain.reshape(1, gain.shape[0]),
        entering,
        total,
        hidden,
        far_down,
        targets,
        route_weight,
    )
    return pl.pallas_call(
        functools.partial(return_kernel, capacity, head_size),
        in_specs=[pl.BlockSpec(memory_space=pl.ANY)] * 3
        + [pl.BlockSpec(memory_space=pltpu.VMEM)] * len(operands),
        out_specs=[pl.BlockSpec(memory_space=pltpu.VMEM)] * 2,
        out_shape=[jax.ShapeDtypeStruct((tokens, width), BF16)] * 2,
        scratch_shapes=[
            pltpu.VMEM(reader.shape, BF16),
            pltpu.VMEM(local_read.shape, F32),
            pltpu.VMEM(out_weight.shape, BF16),
            pltpu.VMEM(reader.shape, BF16),
            pltpu.VMEM(far_down.shape, BF16),
            pltpu.VMEM((rows, width), BF16),
            pltpu.VMEM((rows, width), BF16),
            pltpu.VMEM((reader.shape[0], width), BF16),
            pltpu.VMEM((2, tokens, width), BF16),
            pltpu.VMEM((tokens, width), BF16),
            pltpu.VMEM((tokens, width), BF16),
            pltpu.VMEM((tokens, width), F32),
            pltpu.SemaphoreType.DMA((3,)),
            pltpu.SemaphoreType.DMA((count - 1,)),
            pltpu.SemaphoreType.DMA((count - 1,)),
            pltpu.SemaphoreType.DMA((4,)),
            pltpu.SemaphoreType.DMA((4,)),
        ],
        compiler_params=pltpu.CompilerParams(
            vmem_limit_bytes=40 * 2**20, collective_id=1, has_side_effects=True
        ),
        cost_estimate=pl.CostEstimate(
            flops=6 * 10**9, bytes_accessed=12 * 2**20, transcendentals=0
        ),
        name="return_rows",
    )(*streamed, *operands)


def swap(x, distance):
    count = lax.axis_size("tp")
    return lax.ppermute(x, "tp", [(i, i ^ distance) for i in range(count)])


def slot_targets(block_routes, capacity):
    flat_routes = block_routes.reshape(-1)
    count = flat_routes.shape[0]
    order = jnp.arange(count, dtype=jnp.int32)
    before = (order[:, None] > order[None, :]) & (flat_routes[:, None] == flat_routes[None, :])
    slots = jnp.sum(before.astype(jnp.int32), axis=1).reshape(block_routes.shape)
    return block_routes * capacity + slots


def dispersal_table(targets, places):
    marks = (jnp.arange(places, dtype=jnp.int32)[:, None, None] == targets[None, :, :]).astype(
        jnp.int32
    )
    return jnp.sum(marks, axis=2).astype(jnp.bfloat16)


def one_device(
    receptance,
    key_rows,
    value_rows,
    decay_input,
    learn_input,
    decay_base,
    decay_shift,
    channel_gain,
    out_weight,
    expert_input,
    expert_gain,
    routes,
    route_weight,
    gate_weight,
    up_weight,
    down_weight,
):
    ep_count = lax.axis_size("ep")
    channels = receptance.shape[1]
    head_size = channels // decay_shift.shape[1]
    token_rows, model_width = expert_input.shape
    top_count = routes.shape[1]
    experts = gate_weight.shape[0] * ep_count
    capacity = max(2, 2 * token_rows * top_count // experts)
    slab_rows = ep_count * capacity

    own = (gate_weight[0], up_weight[0], down_weight[0])
    far = tuple(swap(array, 2) for array in own)
    near = tuple(swap(array, 1) for array in own)

    inputs = expert_input.astype(F32)
    expert_normed = (
        inputs
        * lax.rsqrt(jnp.mean(inputs * inputs, axis=1, keepdims=True) + NORM_EPS)
        * expert_gain
    ).astype(BF16)
    own_targets = slot_targets(routes, capacity)
    outgoing = jnp.dot(
        dispersal_table(own_targets, experts * capacity),
        expert_normed,
        preferred_element_type=F32,
    ).astype(BF16)
    arrived = lax.all_to_all(
        outgoing.reshape(experts, capacity, model_width),
        "ep",
        split_axis=0,
        concat_axis=0,
        tiled=True,
    ).reshape(slab_rows, model_width)

    reader, local_read, summary = mixer_local(
        receptance,
        key_rows,
        value_rows,
        decay_input,
        learn_input,
        decay_base,
        decay_shift,
        head_size,
    )
    total, hidden, entering = expert_part(arrived, summary, own, near, far[:2], head_size)
    return tuple(
        return_rows(
            reader,
            local_read,
            out_weight,
            channel_gain,
            entering,
            total,
            hidden,
            far[2],
            own_targets,
            route_weight,
            capacity,
            head_size,
        )
    )


def solution(mesh):
    return jax.shard_map(
        one_device,
        mesh=mesh,
        in_specs=(
            P("ep", "tp"),
            P("ep", "tp"),
            P("ep", "tp"),
            P("ep", "tp"),
            P("ep", "tp"),
            P("tp"),
            P("ep", "tp"),
            P("tp"),
            P("tp", None),
            P(("ep", "tp"), None),
            P(),
            P(("ep", "tp"), None),
            P(("ep", "tp"), None),
            P("ep", None, "tp"),
            P("ep", None, "tp"),
            P("ep", "tp", None),
        ),
        out_specs=(P(("ep", "tp"), None), P(("ep", "tp"), None)),
        check_vma=False,
    )
```

```python
import functools

import jax
import jax.numpy as jnp
from jax import lax
from jax.experimental import pallas as pl
from jax.experimental.pallas import tpu as pltpu
from jax.sharding import PartitionSpec as P


SPAN = 128
STACK = 2
LANES = 128

NORM_EPS = 1e-06
GROUP_EPS = 0.00064
KEY_EPS = 1e-06
F32 = jnp.float32
BF16 = jnp.bfloat16


def mm(a, b):
    return lax.dot_general(
        a.astype(BF16), b.astype(BF16), (((1,), (0,)), ((), ())), preferred_element_type=F32
    )


def mm_nt(a, b):
    return lax.dot_general(
        a.astype(BF16), b.astype(BF16), (((1,), (1,)), ((), ())), preferred_element_type=F32
    )


def mm_tn(a, b):
    return lax.dot_general(
        a.astype(BF16), b.astype(BF16), (((0,), (0,)), ((), ())), preferred_element_type=F32
    )


def split_two(x):
    high = x.astype(BF16)
    return high, (x - high.astype(F32)).astype(BF16)


def grid_index(shape, axis):
    return lax.broadcasted_iota(jnp.int32, shape, axis)


def same_head(head_size):
    rows = grid_index((LANES, LANES), 0) // head_size
    cols = grid_index((LANES, LANES), 1) // head_size
    return rows == cols


def head_sums(x, block):
    high, low = split_two(x)
    return mm(
        jnp.concatenate([high, low], axis=1), jnp.concatenate([block, block], axis=0)
    )


def lower_inverses(strict_parts, rows, cols):
    eye = jnp.where(rows == cols, 1.0, 0.0)
    size = 1
    inverses = None
    while size < SPAN:
        off = (rows // (2 * size) == cols // (2 * size)) & (rows // size != cols // size)
        parts = [jnp.where(off, part, 0.0) for part in strict_parts]
        if inverses is None:
            inverses = [eye - part for part in parts]
        else:
            firsts = [mm(part, inv) for part, inv in zip(parts, inverses)]
            inverses = [inv - mm(inv, first) for inv, first in zip(inverses, firsts)]
        size *= 2
    return inverses


def send_to(src, dst, send_sem, recv_sem, target):
    return pltpu.make_async_remote_copy(
        src_ref=src,
        dst_ref=dst,
        send_sem=send_sem,
        recv_sem=recv_sem,
        device_id=target,
        device_id_type=pl.DeviceIdType.MESH,
    )


def greet_all(barrier, here, count, others):
    def greet(distance, nothing):
        pl.semaphore_signal(
            barrier,
            inc=1,
            device_id={"ep": lax.rem(here + distance, count)},
            device_id_type=pl.DeviceIdType.MESH,
        )
        return nothing

    lax.fori_loop(1, count, greet, 0)
    for target in others:
        pl.semaphore_signal(
            barrier, inc=1, device_id={"tp": target}, device_id_type=pl.DeviceIdType.MESH
        )


def in_hbm(array):
    return pltpu.with_memory_space_constraint(array, pltpu.HBM)


def far_first(k, count):
    return count // 2 + ((k + 1) // 2) * (2 * lax.rem(k, 2) - 1)


def pack_rows(tokens_ref, scale_ref, routes_ref, outgoing, count, capacity):
    inputs = tokens_ref[...].astype(F32)
    square = jnp.sum(inputs * inputs, axis=1, keepdims=True) * (1.0 / inputs.shape[1])
    normed = (inputs * lax.rsqrt(square + NORM_EPS) * scale_ref[...]).astype(BF16)
    rows = inputs.shape[0]
    members = grid_index((count, rows), 0)
    named = jnp.zeros((count, rows), F32)
    for picked in range(routes_ref.shape[0]):
        named = jnp.where(routes_ref[picked : picked + 1] == members, 1.0, named)
    earlier = grid_index((rows, rows), 0) < grid_index((rows, rows), 1)
    slots = mm(named, earlier.astype(F32))
    slots = jnp.where(named > 0.5, slots, -1.0).astype(jnp.int32)
    wanted = grid_index((capacity, rows), 0)
    group = max(1, min(count, 256 // capacity))
    for begin in range(0, count, group):
        table = jnp.concatenate(
            [
                jnp.where(slots[e : e + 1] == wanted, 1.0, 0.0)
                for e in range(begin, begin + group)
            ],
            axis=0,
        )
        outgoing[begin * capacity : (begin + group) * capacity] = mm(table, normed).astype(BF16)


def local_kernel(
    head_size,
    capacity,
    r_ref,
    k_ref,
    v_ref,
    d_ref,
    l_ref,
    base_ref,
    shift_ref,
    tokens_ref,
    scale_ref,
    routes_ref,
    own_gate,
    own_up,
    own_down,
    reader_ref,
    local_ref,
    summary_ref,
    arrived,
    near_gate,
    near_up,
    near_down,
    state,
    outgoing,
    keep_sem,
    send_sems,
    recv_sems,
    side_send,
    side_recv,
):
    pair = pl.program_id(0)
    half = LANES // 2
    here = lax.axis_index("ep")
    count = lax.axis_size("ep")
    place = lax.axis_index("tp")
    beside = place + 1 - 2 * lax.rem(place, 2)

    def rows_of(member):
        return pl.ds(pl.multiple_of(member * capacity, capacity), capacity)

    def post(distance, member):
        return send_to(
            outgoing.at[rows_of(member)],
            arrived.at[rows_of(here)],
            send_sems.at[distance - 1],
            recv_sems.at[distance - 1],
            {"ep": member},
        )

    keep = pltpu.make_async_copy(
        outgoing.at[rows_of(here)], arrived.at[rows_of(here)], keep_sem
    )
    nears = [
        send_to(src, dst, side_send.at[i], side_recv.at[i], {"tp": beside})
        for i, (src, dst) in enumerate(
            [(own_gate, near_gate), (own_up, near_up), (own_down, near_down)]
        )
    ]

    @pl.when(pair == 0)
    def _():
        barrier = pltpu.get_barrier_semaphore()
        greet_all(barrier, here, count, (beside,))
        pack_rows(tokens_ref, scale_ref, routes_ref, outgoing, count, capacity)
        pl.semaphore_wait(barrier, count)

        def launch(k, nothing):
            distance = far_first(k, count)
            post(distance, lax.rem(here + distance, count)).start()
            return nothing

        lax.fori_loop(0, count - 1, launch, 0)
        keep.start()
        for copy in nears:
            copy.start()

    rows = grid_index((SPAN, SPAN), 0)
    cols = grid_index((SPAN, SPAN), 1)
    strict = rows > cols
    inclusive = rows >= cols
    first = grid_index((SPAN, LANES), 1) < half
    matched = same_head(head_size)
    block = matched.astype(BF16)
    diagonal = grid_index((LANES, LANES), 0) == grid_index((LANES, LANES), 1)
    tri = inclusive.astype(BF16)
    tri_two = jnp.concatenate([tri, tri], axis=1)

    state[:LANES] = jnp.zeros((LANES, LANES), F32)
    state[LANES:] = jnp.where(diagonal, 1.0, 0.0)

    heads = shift_ref.shape[1]
    chosen = grid_index((heads, LANES), 0) == 2 * pair + grid_index((heads, LANES), 1) // half

    def advance(step, nothing):
        start = pl.multiple_of(step * (STACK * SPAN), STACK * SPAN)
        rows_here = pl.ds(start, STACK * SPAN)
        shift = lax.dot_general(
            shift_ref[rows_here],
            chosen.astype(F32),
            (((1,), (0,)), ((), ())),
            precision=lax.Precision.HIGHEST,
            preferred_element_type=F32,
        )
        pre = d_ref[rows_here].astype(F32) + base_ref[0] + shift
        log_all = -0.6065306597126334 / (1.0 + jnp.exp(-pre))
        rates = 1.0 / (1.0 + jnp.exp(-l_ref[rows_here].astype(F32)))
        key_all = k_ref[rows_here].astype(F32)
        unit_all = key_all * lax.rsqrt(head_sums(key_all * key_all, block) + KEY_EPS)
        removal_all = unit_all * rates

        spans = STACK
        items = []
        strict_parts = []
        for j in range(spans):
            here = slice(j * SPAN, (j + 1) * SPAN)
            log_decay = log_all[here]
            high, low = split_two(log_decay)
            cum = mm(tri_two, jnp.concatenate([high, low], axis=0))
            middle = cum[SPAN // 2 - 1 : SPAN // 2]
            ending = cum[SPAN - 1 :]
            e_cm = jnp.exp(cum - middle)
            e_pm = jnp.exp(cum - log_decay - middle)
            shrink = jnp.exp(middle - cum)
            e_mid = jnp.exp(middle)
            e_tail = jnp.exp(ending - middle)
            unit, key = unit_all[here], key_all[here]
            value = v_ref[pl.ds(start + j * SPAN, SPAN)]
            turned = jnp.concatenate([value[:, half:], value[:, :half]], axis=1)
            recept = r_ref[pl.ds(start + j * SPAN, SPAN)].astype(F32)
            probes = unit * e_pm
            queries = recept * e_cm
            back_removal = removal_all[here] * shrink
            back_keys = key * shrink
            left = jnp.concatenate(
                [
                    jnp.where(first, probes, 0.0),
                    jnp.where(first, 0.0, probes),
                    jnp.where(first, queries, 0.0),
                    jnp.where(first, 0.0, queries),
                ],
                axis=0,
            )
            products = mm_nt(left, jnp.concatenate([back_removal, back_keys], axis=0))
            for h in range(2):
                strict_parts.append(
                    jnp.where(strict, products[h * SPAN : (h + 1) * SPAN, :SPAN], 0.0)
                )
            items.append(
                dict(
                    products=products,
                    turned=turned,
                    carrying=probes * e_mid,
                    reading=queries * e_mid,
                    removal_tail=back_removal * e_tail,
                    key_tail=back_keys * e_tail,
                    fade=jnp.exp(ending),
                )
            )
        inverses = lower_inverses(strict_parts, rows, cols)
        for j in range(spans):
            item = items[j]
            products, turned = item["products"], item["turned"]
            solved, removed, kept = [], [], []
            for h in range(2):
                top = slice(h * SPAN, (h + 1) * SPAN)
                bottom = slice((2 + h) * SPAN, (3 + h) * SPAN)
                pair_keys = jnp.where(strict, products[top, SPAN:], 0.0)
                read_removal = jnp.where(inclusive, products[bottom, :SPAN], 0.0)
                read_keys = jnp.where(inclusive, products[bottom, SPAN:], 0.0)
                both = mm(jnp.concatenate([pair_keys, read_keys], axis=0), turned)
                own = first if h == 0 else jnp.logical_not(first)
                right = jnp.where(own, item["carrying"], both[:SPAN])
                answer = mm(inverses[2 * j + h], right)
                solved.append(answer)
                removed.append(mm(read_removal, answer))
                kept.append(both[SPAN:])
            carried = jnp.where(first, solved[0], solved[1])
            local_turned = jnp.where(first, solved[1], solved[0])
            reader = item["reading"] - jnp.where(first, removed[0], removed[1])
            read_turned = jnp.where(first, kept[1] - removed[1], kept[0] - removed[0])
            local_read = jnp.concatenate([read_turned[:, half:], read_turned[:, :half]], axis=1)
            taken = mm_tn(
                jnp.concatenate([carried, local_turned], axis=1), item["removal_tail"]
            )
            offset_turned = mm_tn(turned, item["key_tail"]) - taken[LANES:]
            offset = jnp.concatenate([offset_turned[half:], offset_turned[:half]], axis=0)
            offset = jnp.where(matched, offset, 0.0)
            transition = jnp.where(diagonal, item["fade"], 0.0) - jnp.where(
                matched, taken[:LANES], 0.0
            )
            now = state[...]
            reads = mm_nt(reader, now)
            here = pl.ds(start + j * SPAN, SPAN)
            local_ref[here] = local_read + reads[:, :LANES]
            reader_ref[pl.ds(start + j * SPAN, SPAN)] = reads[:, LANES:].astype(BF16)
            now_high, now_low = split_two(now)
            step_high, step_low = split_two(transition)
            moved = mm(now_high, step_high) + mm(now_low, step_high) + mm(now_high, step_low)
            state[:LANES] = moved[:LANES] + offset
            state[LANES:] = moved[LANES:]
        return nothing

    lax.fori_loop(0, r_ref.shape[0] // (STACK * SPAN), advance, 0)
    summary_ref[1] = (state[:half] + state[half:LANES]).astype(BF16)
    summary_ref[0] = (state[LANES : LANES + half] + state[LANES + half :]).astype(BF16)

    @pl.when(pair == pl.num_programs(0) - 1)
    def _():
        def collect(k, nothing):
            distance = far_first(k, count)
            copy = post(distance, lax.rem(here + distance, count))
            copy.wait_send()
            copy.wait_recv()
            return nothing

        lax.fori_loop(0, count - 1, collect, 0)
        keep.wait()
        for copy in nears:
            copy.wait()


def mixer_local(
    receptance,
    keys,
    values,
    decay,
    learn,
    base,
    shift,
    tokens,
    scale,
    routes,
    own,
    head_size,
    capacity,
):
    rows, channels = receptance.shape
    pairs = channels // LANES
    heads = shift.shape[1]
    half = LANES // 2
    count = lax.axis_size("ep")
    token_rows, width = tokens.shape
    picks = routes.shape[1]
    tile = pl.BlockSpec((rows, LANES), lambda p: (0, p))
    small = pl.BlockSpec((2, half, LANES), lambda p: (0, p, 0))
    anywhere = pl.BlockSpec(memory_space=pl.ANY)
    streams = [in_hbm(array) for array in (receptance, keys, values, decay, learn)]
    shards = [in_hbm(array) for array in own]
    return pl.pallas_call(
        functools.partial(local_kernel, head_size, capacity),
        grid=(pairs,),
        in_specs=[tile] * 5
        + [
            pl.BlockSpec((1, 1, LANES), lambda p: (p, 0, 0)),
            pl.BlockSpec((rows, heads), lambda p: (0, 0)),
            pl.BlockSpec((token_rows, width), lambda p: (0, 0)),
            pl.BlockSpec((1, width), lambda p: (0, 0)),
            pl.BlockSpec((picks, token_rows), lambda p: (0, 0)),
        ]
        + [anywhere] * 3,
        out_specs=[tile, tile, small] + [anywhere] * 4,
        out_shape=[
            jax.ShapeDtypeStruct((rows, channels), BF16),
            jax.ShapeDtypeStruct((rows, channels), F32),
            jax.ShapeDtypeStruct((2, pairs * half, LANES), BF16),
            jax.ShapeDtypeStruct((count * capacity, width), BF16),
        ]
        + [jax.ShapeDtypeStruct(array.shape, BF16) for array in own],
        scratch_shapes=[
            pltpu.VMEM((2 * LANES, LANES), F32),
            pltpu.VMEM((count * capacity, width), BF16),
            pltpu.SemaphoreType.DMA,
            pltpu.SemaphoreType.DMA((count - 1,)),
            pltpu.SemaphoreType.DMA((count - 1,)),
            pltpu.SemaphoreType.DMA((3,)),
            pltpu.SemaphoreType.DMA((3,)),
        ],
        compiler_params=pltpu.CompilerParams(
            dimension_semantics=("arbitrary",),
            vmem_limit_bytes=24 * 2**20,
            collective_id=2,
            has_side_effects=True,
        ),
        cost_estimate=pl.CostEstimate(
            flops=20 * 10**9, bytes_accessed=6 * 2**20, transcendentals=10**6
        ),
        name="mixer_local",
    )(
        *streams,
        base.reshape(pairs, 1, LANES),
        shift,
        tokens,
        scale.reshape(1, width),
        routes.T,
        *shards,
    )


def gated(x, gate, up):
    gates = mm(x, gate)
    uppers = mm(x, up)
    return (gates / (1.0 + jnp.exp(-gates)) * uppers).astype(BF16)


def part_kernel(
    head_size,
    own_gate,
    own_up,
    own_down,
    summary_ref,
    x_ref,
    near_gate,
    near_up,
    near_down,
    far_gate,
    far_up,
    total_ref,
    hidden_ref,
    entering_ref,
    held,
    held_down,
    cross,
    before,
    sending,
    landed,
    load_sems,
    send_sems,
    recv_sems,
    side_send,
    side_recv,
):
    here = lax.axis_index("ep")
    count = lax.axis_size("ep")
    place = lax.axis_index("tp")
    beside = place + 1 - 2 * lax.rem(place, 2)
    rounds = landed.shape[0]
    half = LANES // 2
    pairs = before.shape[1]
    rows = x_ref.shape[0]
    units = own_gate.shape[1]
    piece = min(rows, 256)
    matched = same_head(head_size)
    diagonal = grid_index((LANES, LANES), 0) == grid_index((LANES, LANES), 1)

    loads = [
        pltpu.make_async_copy(src, dst, load_sems.at[i])
        for i, (src, dst) in enumerate(
            [
                (own_gate, held.at[0]),
                (own_up, held.at[1]),
                (own_down, held_down),
            ]
        )
    ]
    for load in loads:
        load.start()
    barrier = pltpu.get_barrier_semaphore()
    greet_all(barrier, here, count, (beside,))

    def transfer(level, distance, target):
        return send_to(
            sending,
            landed.at[level],
            send_sems.at[distance - 1],
            recv_sems.at[level],
            {"ep": target},
        )

    def transfer_state(level, distance, target):
        return send_to(
            sending.at[1],
            landed.at[level, 1],
            send_sems.at[distance - 1],
            recv_sems.at[level],
            {"ep": target},
        )

    def sends_all(reach):
        return (lax.rem(here, 2 * reach) == reach - 1) & (here >= 2 * reach)

    def wide(part):
        part = part.astype(F32)
        return jnp.where(matched, jnp.concatenate([part, part], axis=0), 0.0)

    def spot(p):
        return slice(p * half, (p + 1) * half)

    for p in range(pairs):
        before[0, p] = jnp.where(diagonal, 1.0, 0.0)
        before[1, p] = jnp.zeros((LANES, LANES), F32)
    pl.semaphore_wait(barrier, count)
    forwards = [
        send_to(src, cross.at[i], side_send.at[i], side_recv.at[i], {"tp": beside})
        for i, src in enumerate((far_gate, far_up))
    ]
    for forward in forwards:
        forward.start()

    def send_round(level):
        reach = 2**level

        @pl.when(lax.rem(here, 2 * reach) == reach - 1)
        def _():
            for p in range(pairs):
                both = jnp.concatenate([before[0, p], before[1, p]], axis=0)
                high, low = split_two(both)
                step = wide(summary_ref[0, spot(p)])
                moved = mm(high, step) + mm(low, step)
                after = moved[LANES:] + wide(summary_ref[1, spot(p)])
                sending[0, spot(p)] = (moved[:half] + moved[half:LANES]).astype(BF16)
                sending[1, spot(p)] = (after[:half] + after[half:]).astype(BF16)

        def launch_with(transfer):
            def launch(distance, nothing):
                transfer(level, distance, here + distance).start()
                return nothing

            lax.fori_loop(1, reach + 1, launch, 0)

        pl.when(sends_all(reach))(lambda: launch_with(transfer))
        pl.when(here == reach - 1)(lambda: launch_with(transfer_state))

    def take_round(level):
        reach = 2**level

        @pl.when((lax.rem(here // reach, 2) == 1) & (here >= 2 * reach))
        def _():
            transfer(level, 1, here).wait_recv()
            for p in range(pairs):
                both = jnp.concatenate(
                    [wide(landed[level, 0, spot(p)]), wide(landed[level, 1, spot(p)])], axis=0
                )
                high, low = split_two(before[0, p])
                moved = mm(both, high) + mm(both, low)
                before[0, p] = moved[:LANES]
                before[1, p] = moved[LANES:] + before[1, p]

        @pl.when((here >= reach) & (here < 2 * reach))
        def _():
            transfer_state(level, 1, here).wait_recv()
            for p in range(pairs):
                state = wide(landed[level, 1, spot(p)])
                high, low = split_two(before[0, p])
                before[1, p] = mm(state, high) + mm(state, low) + before[1, p]

    def over_rows(body):
        def step(i, nothing):
            body(pl.ds(pl.multiple_of(i * piece, piece), piece))
            return nothing

        lax.fori_loop(0, rows // piece, step, 0)

    def first_part(at):
        hidden = gated(x_ref[at], held[0], held[1])
        total_ref[at] = mm(hidden, held_down[...])

    def second_part(at):
        hidden = gated(x_ref[at], near_gate[...], near_up[...])
        total_ref[at] += mm(hidden, near_down[...])

    def third_part(at):
        hidden_ref[at, :units] = gated(x_ref[at], far_gate[...], far_up[...])

    def fourth_part(at):
        hidden_ref[at, units:] = gated(x_ref[at], cross[0], cross[1])

    send_round(0)
    bodies = (first_part, second_part, third_part, fourth_part)
    needs = (loads, (), (), ())
    for turn in range(max(len(bodies), rounds)):
        if turn < len(bodies):
            for load in needs[turn]:
                load.wait()
            if turn == len(bodies) - 1:
                for forward in forwards:
                    forward.wait_recv()
            over_rows(bodies[turn])
        if turn < rounds:
            take_round(turn)
            if turn + 1 < rounds:
                send_round(turn + 1)
    for p in range(pairs):
        entering_ref[p * LANES : (p + 1) * LANES] = before[1, p]

    def settle_with(transfer, level, reach):
        def settle(distance, nothing):
            transfer(level, distance, here + distance).wait_send()
            return nothing

        lax.fori_loop(1, reach + 1, settle, 0)

    for level in range(rounds):
        reach = 2**level
        pl.when(sends_all(reach))(functools.partial(settle_with, transfer, level, reach))
        pl.when(here == reach - 1)(
            functools.partial(settle_with, transfer_state, level, reach)
        )

    for forward in forwards:
        forward.wait_send()


def expert_part(incoming, summary, own, near, far, head_size):
    rows, width = incoming.shape
    units = own[0].shape[1]
    pairs = summary.shape[1] * 2 // LANES
    count = lax.axis_size("ep")
    rounds = (count - 1).bit_length()
    shards = [in_hbm(array) for array in own]
    operands = (summary, incoming) + near + far
    return pl.pallas_call(
        functools.partial(part_kernel, head_size),
        in_specs=[pl.BlockSpec(memory_space=pl.ANY)] * 3
        + [pl.BlockSpec(memory_space=pltpu.VMEM)] * len(operands),
        out_specs=[pl.BlockSpec(memory_space=pltpu.VMEM)] * 3,
        out_shape=[
            jax.ShapeDtypeStruct((rows, width), F32),
            jax.ShapeDtypeStruct((rows, 2 * units), BF16),
            jax.ShapeDtypeStruct((pairs * LANES, LANES), F32),
        ],
        scratch_shapes=[
            pltpu.VMEM((2, width, units), BF16),
            pltpu.VMEM((units, width), BF16),
            pltpu.VMEM((2, width, units), BF16),
            pltpu.VMEM((2, pairs, LANES, LANES), F32),
            pltpu.VMEM(summary.shape, BF16),
            pltpu.VMEM((rounds,) + summary.shape, BF16),
            pltpu.SemaphoreType.DMA((3,)),
            pltpu.SemaphoreType.DMA((count // 2,)),
            pltpu.SemaphoreType.DMA((rounds,)),
            pltpu.SemaphoreType.DMA((2,)),
            pltpu.SemaphoreType.DMA((2,)),
        ],
        compiler_params=pltpu.CompilerParams(
            vmem_limit_bytes=32 * 2**20, collective_id=0, has_side_effects=True
        ),
        cost_estimate=pl.CostEstimate(
            flops=20 * rows * width * units,
            bytes_accessed=2 * (rows * width + 10 * units * width),
            transcendentals=4 * rows * units,
        ),
        name="expert_part",
    )(*shards, *operands)


def return_kernel(
    capacity,
    head_size,
    project_ref,
    reader,
    local,
    gain_ref,
    entering_ref,
    total_ref,
    hidden_ref,
    far_ref,
    routes_ref,
    weight_ref,
    mixer_ref,
    expert_ref,
    project,
    mixed,
    cross,
    staged,
    landed,
    term,
    near_in,
    pair_out,
    far_in,
    combined,
    load_sem,
    send_sems,
    recv_sems,
    side_send,
    side_recv,
):
    here = lax.axis_index("ep")
    count = lax.axis_size("ep")
    place = lax.axis_index("tp")
    low, high = lax.rem(place, 2), place // 2
    beside = place + 1 - 2 * low
    across = place + 2 - 4 * high
    units = far_ref.shape[0]
    tokens = expert_ref.shape[0]
    pairs = reader.shape[1] // LANES
    block = same_head(head_size).astype(BF16)

    def side(src, dst, index, target):
        return send_to(src, dst, side_send.at[index], side_recv.at[index], {"tp": target})

    def rows_of(member):
        return pl.ds(pl.multiple_of(member * capacity, capacity), capacity)

    def back(distance, member):
        return send_to(
            staged.at[rows_of(member)],
            landed.at[rows_of(here)],
            send_sems.at[distance - 1],
            recv_sems.at[distance - 1],
            {"ep": member},
        )

    barrier = pltpu.get_barrier_semaphore()
    greet_all(barrier, here, count, (beside, across))
    pl.semaphore_wait(barrier, count + 1)

    forward = side(far_ref, cross, 0, beside)
    forward.start()
    load = pltpu.make_async_copy(project_ref, project, load_sem)
    load.start()
    forward.wait_recv()

    def finished(member):
        rows = rows_of(member)
        hidden = hidden_ref[rows]
        row = total_ref[rows] + mm(hidden[:, :units], far_ref[...])
        return (row + mm(hidden[:, units:], cross[...])).astype(BF16)

    def send_block(k, nothing):
        distance = far_first(k, count)
        member = lax.rem(here + distance, count)
        staged[rows_of(member)] = finished(member)
        back(distance, member).start()
        return nothing

    lax.fori_loop(0, count - 1, send_block, 0)
    landed[rows_of(here)] = finished(here)

    load.wait()
    for p in range(pairs):
        lanes = slice(p * LANES, (p + 1) * LANES)
        entering = entering_ref[p * LANES : (p + 1) * LANES]
        read = mm_nt(reader[:, lanes], entering) + local[:, lanes]
        centred = read - head_sums(read, block) * (1.0 / head_size)
        variance = head_sums(centred * centred, block) * (1.0 / head_size)
        scaled = centred * lax.rsqrt(variance + GROUP_EPS) * gain_ref[:, lanes]
        mixed[:, lanes] = scaled.astype(BF16)

    def block_rows(b):
        return pl.ds(pl.multiple_of(b * tokens, tokens), tokens)

    def project_block(b, nothing):
        rows = block_rows(b)
        term[rows] = mm(mixed[rows], project[...]).astype(BF16)
        return nothing

    lax.fori_loop(0, 4, project_block, 0)
    nears = [
        side(term.at[block_rows(2 * y + 1 - low)], near_in.at[y], 1 + y, beside)
        for y in range(2)
    ]
    for copy in nears:
        copy.start()

    picks = routes_ref.shape[0]
    packed = jnp.concatenate(
        [routes_ref[...].astype(F32), weight_ref[...], jnp.zeros((8 - 2 * picks, tokens), F32)],
        axis=0,
    ).T
    lane = grid_index((tokens, LANES), 1)
    routes = [packed[:, i : i + 1].astype(jnp.int32) for i in range(picks)]
    weight = packed[:, picks : 2 * picks]
    named = jnp.zeros((tokens, LANES), F32)
    for route in routes:
        named = jnp.where(route == lane, 1.0, named)
    earlier = grid_index((tokens, tokens), 0) > grid_index((tokens, tokens), 1)
    slots = mm(earlier.astype(F32), named)
    target = jnp.concatenate(
        [
            route * capacity
            + jnp.sum(jnp.where(route == lane, slots, 0.0), axis=1, keepdims=True).astype(
                jnp.int32
            )
            for route in routes
        ],
        axis=1,
    )
    slot = grid_index((tokens, capacity), 1)

    def taken(member):
        table = jnp.zeros((tokens, capacity), F32)
        scale = jnp.zeros((tokens, 1), F32)
        for picked in range(target.shape[1]):
            own = target[:, picked : picked + 1] - member * capacity
            table = jnp.where(own == slot, 1.0, table)
            inside = (own >= 0) & (own < capacity)
            scale = jnp.where(inside, weight[:, picked : picked + 1], scale)
        return mm(table, landed[rows_of(member)]) * scale

    combined[...] = taken(here)

    for copy in nears:
        copy.wait_recv()
    other = 1 - high
    pair_out[...] = (
        term[block_rows(2 * other + low)].astype(F32) + near_in[other].astype(F32)
    ).astype(BF16)
    cross_send = side(pair_out, far_in, 3, across)
    cross_send.start()

    def gather_block(k, nothing):
        distance = far_first(count - 2 - k, count)
        member = lax.rem(here + count - distance, count)
        back(distance, member).wait_recv()
        combined[...] += taken(member)
        return nothing

    lax.fori_loop(0, count // 2, gather_block, 0)
    cross_send.wait_recv()
    kept = term[block_rows(2 * high + low)].astype(F32) + near_in[high].astype(F32)
    mixer_ref[...] = (kept + far_in[...].astype(F32)).astype(BF16)
    lax.fori_loop(count // 2, count - 1, gather_block, 0)
    expert_ref[...] = combined[...].astype(BF16)

    def settle(k, nothing):
        distance = far_first(k, count)
        back(distance, lax.rem(here + distance, count)).wait_send()
        return nothing

    lax.fori_loop(0, count - 1, settle, 0)
    for copy in [forward] + nears + [cross_send]:
        copy.wait_send()


def return_rows(
    reader,
    local_read,
    out_weight,
    gain,
    entering,
    total,
    hidden,
    far_down,
    routes,
    route_weight,
    capacity,
    head_size,
):
    count = lax.axis_size("ep")
    rows, width = total.shape
    tokens = routes.shape[0]
    operands = (
        reader,
        local_read,
        gain.reshape(1, gain.shape[0]),
        entering,
        total,
        hidden,
        far_down,
        routes.T,
        route_weight.T,
    )
    return pl.pallas_call(
        functools.partial(return_kernel, capacity, head_size),
        in_specs=[pl.BlockSpec(memory_space=pl.ANY)]
        + [pl.BlockSpec(memory_space=pltpu.VMEM)] * len(operands),
        out_specs=[pl.BlockSpec(memory_space=pltpu.VMEM)] * 2,
        out_shape=[jax.ShapeDtypeStruct((tokens, width), BF16)] * 2,
        scratch_shapes=[
            pltpu.VMEM(out_weight.shape, BF16),
            pltpu.VMEM(reader.shape, BF16),
            pltpu.VMEM(far_down.shape, BF16),
            pltpu.VMEM((rows, width), BF16),
            pltpu.VMEM((rows, width), BF16),
            pltpu.VMEM((reader.shape[0], width), BF16),
            pltpu.VMEM((2, tokens, width), BF16),
            pltpu.VMEM((tokens, width), BF16),
            pltpu.VMEM((tokens, width), BF16),
            pltpu.VMEM((tokens, width), F32),
            pltpu.SemaphoreType.DMA,
            pltpu.SemaphoreType.DMA((count - 1,)),
            pltpu.SemaphoreType.DMA((count - 1,)),
            pltpu.SemaphoreType.DMA((4,)),
            pltpu.SemaphoreType.DMA((4,)),
        ],
        compiler_params=pltpu.CompilerParams(
            vmem_limit_bytes=40 * 2**20, collective_id=1, has_side_effects=True
        ),
        cost_estimate=pl.CostEstimate(
            flops=6 * 10**9, bytes_accessed=12 * 2**20, transcendentals=0
        ),
        name="return_rows",
    )(in_hbm(out_weight), *operands)


def swap(x, distance):
    count = lax.axis_size("tp")
    return lax.ppermute(x, "tp", [(i, i ^ distance) for i in range(count)])


def one_device(
    receptance,
    key_rows,
    value_rows,
    decay_input,
    learn_input,
    decay_base,
    decay_shift,
    channel_gain,
    out_weight,
    expert_input,
    expert_gain,
    routes,
    route_weight,
    gate_weight,
    up_weight,
    down_weight,
):
    ep_count = lax.axis_size("ep")
    channels = receptance.shape[1]
    head_size = channels // decay_shift.shape[1]
    experts = gate_weight.shape[0] * ep_count
    capacity = max(2, 2 * expert_input.shape[0] * routes.shape[1] // experts)

    own = (gate_weight[0], up_weight[0], down_weight[0])
    far = tuple(swap(array, 2) for array in own)
    reader, local_read, summary, arrived, *near = mixer_local(
        receptance,
        key_rows,
        value_rows,
        decay_input,
        learn_input,
        decay_base,
        decay_shift,
        expert_input,
        expert_gain,
        routes,
        own,
        head_size,
        capacity,
    )
    near = tuple(near)
    total, hidden, entering = expert_part(arrived, summary, own, near, far[:2], head_size)
    return tuple(
        return_rows(
            reader,
            local_read,
            out_weight,
            channel_gain,
            entering,
            total,
            hidden,
            far[2],
            routes,
            route_weight,
            capacity,
            head_size,
        )
    )


def solution(mesh):
    return jax.shard_map(
        one_device,
        mesh=mesh,
        in_specs=(
            P("ep", "tp"),
            P("ep", "tp"),
            P("ep", "tp"),
            P("ep", "tp"),
            P("ep", "tp"),
            P("tp"),
            P("ep", "tp"),
            P("tp"),
            P("tp", None),
            P(("ep", "tp"), None),
            P(),
            P(("ep", "tp"), None),
            P(("ep", "tp"), None),
            P("ep", None, "tp"),
            P("ep", None, "tp"),
            P("ep", "tp", None),
        ),
        out_specs=(P(("ep", "tp"), None), P(("ep", "tp"), None)),
        check_vma=False,
    )
```

```python
import functools

import jax
import jax.numpy as jnp
from jax import lax
from jax.experimental import pallas as pl
from jax.experimental.pallas import tpu as pltpu
from jax.sharding import PartitionSpec as P

SPAN = 128
STACK = 2
LANES = 128

NORM_EPS = 1e-06
GROUP_EPS = 0.00064
KEY_EPS = 1e-06
F32 = jnp.float32
BF16 = jnp.bfloat16


def mm(a, b):
    return lax.dot_general(
        a.astype(BF16), b.astype(BF16), (((1,), (0,)), ((), ())), preferred_element_type=F32
    )


def mm_nt(a, b):
    return lax.dot_general(
        a.astype(BF16), b.astype(BF16), (((1,), (1,)), ((), ())), preferred_element_type=F32
    )


def mm_tn(a, b):
    return lax.dot_general(
        a.astype(BF16), b.astype(BF16), (((0,), (0,)), ((), ())), preferred_element_type=F32
    )


def split_two(x):
    high = x.astype(BF16)
    return high, (x - high.astype(F32)).astype(BF16)


def grid_index(shape, axis):
    return lax.broadcasted_iota(jnp.int32, shape, axis)


def same_head(head_size):
    rows = grid_index((LANES, LANES), 0) // head_size
    cols = grid_index((LANES, LANES), 1) // head_size
    return rows == cols


def head_sums(x, block):
    high, low = split_two(x)
    return mm(
        jnp.concatenate([high, low], axis=1), jnp.concatenate([block, block], axis=0)
    )


def lower_inverses(strict_parts, rows, cols):
    eye = jnp.where(rows == cols, 1.0, 0.0)
    size = 1
    inverses = None
    while size < SPAN:
        off = (rows // (2 * size) == cols // (2 * size)) & (rows // size != cols // size)
        parts = [jnp.where(off, part, 0.0) for part in strict_parts]
        if inverses is None:
            inverses = [eye - part for part in parts]
        else:
            firsts = [mm(part, inv) for part, inv in zip(parts, inverses)]
            inverses = [inv - mm(inv, first) for inv, first in zip(inverses, firsts)]
        size *= 2
    return inverses


def send_to(src, dst, send_sem, recv_sem, target):
    return pltpu.make_async_remote_copy(
        src_ref=src,
        dst_ref=dst,
        send_sem=send_sem,
        recv_sem=recv_sem,
        device_id=target,
        device_id_type=pl.DeviceIdType.MESH,
    )


def greet_all(barrier, here, count, others):
    def greet(distance, nothing):
        pl.semaphore_signal(
            barrier,
            inc=1,
            device_id={"ep": lax.rem(here + distance, count)},
            device_id_type=pl.DeviceIdType.MESH,
        )
        return nothing

    lax.fori_loop(1, count, greet, 0)
    for target in others:
        pl.semaphore_signal(
            barrier, inc=1, device_id={"tp": target}, device_id_type=pl.DeviceIdType.MESH
        )


def in_hbm(array):
    return pltpu.with_memory_space_constraint(array, pltpu.HBM)


def pack_rows(tokens_ref, scale_ref, routes_ref, outgoing, count, capacity):
    inputs = tokens_ref[...].astype(F32)
    square = jnp.sum(inputs * inputs, axis=1, keepdims=True) * (1.0 / inputs.shape[1])
    normed = (inputs * lax.rsqrt(square + NORM_EPS) * scale_ref[...]).astype(BF16)
    rows = inputs.shape[0]
    members = grid_index((count, rows), 0)
    named = jnp.zeros((count, rows), F32)
    for picked in range(routes_ref.shape[0]):
        named = jnp.where(routes_ref[picked : picked + 1] == members, 1.0, named)
    earlier = grid_index((rows, rows), 0) < grid_index((rows, rows), 1)
    slots = mm(named, earlier.astype(F32))
    slots = jnp.where(named > 0.5, slots, -1.0).astype(jnp.int32)
    wanted = grid_index((capacity, rows), 0)
    group = max(1, min(count, 256 // capacity))
    for begin in range(0, count, group):
        table = jnp.concatenate(
            [
                jnp.where(slots[e : e + 1] == wanted, 1.0, 0.0)
                for e in range(begin, begin + group)
            ],
            axis=0,
        )
        outgoing[begin * capacity : (begin + group) * capacity] = mm(table, normed).astype(BF16)


def scan_pair(
    pair,
    head_size,
    r_ref,
    k_ref,
    v_ref,
    d_ref,
    l_ref,
    base_ref,
    shift_ref,
    reader_ref,
    local_ref,
    summary_ref,
    state,
):
    half = LANES // 2
    lanes = pl.ds(pl.multiple_of(pair * LANES, LANES), LANES)
    spot = pl.ds(pl.multiple_of(pair * half, half), half)

    rows = grid_index((SPAN, SPAN), 0)
    cols = grid_index((SPAN, SPAN), 1)
    strict = rows > cols
    inclusive = rows >= cols
    first = grid_index((SPAN, LANES), 1) < half
    matched = same_head(head_size)
    block = matched.astype(BF16)
    diagonal = grid_index((LANES, LANES), 0) == grid_index((LANES, LANES), 1)
    tri = inclusive.astype(BF16)
    tri_two = jnp.concatenate([tri, tri], axis=1)

    state[:LANES] = jnp.zeros((LANES, LANES), F32)
    state[LANES:] = jnp.where(diagonal, 1.0, 0.0)

    heads = shift_ref.shape[1]
    chosen = grid_index((heads, LANES), 0) == 2 * pair + grid_index((heads, LANES), 1) // half
    def advance(step, nothing):
        start = pl.multiple_of(step * (STACK * SPAN), STACK * SPAN)
        rows_here = pl.ds(start, STACK * SPAN)
        shift = lax.dot_general(
            shift_ref[rows_here],
            chosen.astype(F32),
            (((1,), (0,)), ((), ())),
            precision=lax.Precision.HIGHEST,
            preferred_element_type=F32,
        )
        pre = d_ref[rows_here, lanes].astype(F32) + base_ref[:, lanes] + shift
        log_all = -0.6065306597126334 / (1.0 + jnp.exp(-pre))
        rates = 1.0 / (1.0 + jnp.exp(-l_ref[rows_here, lanes].astype(F32)))
        key_all = k_ref[rows_here, lanes].astype(F32)
        unit_all = key_all * lax.rsqrt(head_sums(key_all * key_all, block) + KEY_EPS)
        removal_all = unit_all * rates

        spans = STACK
        items = []
        strict_parts = []
        for j in range(spans):
            here = slice(j * SPAN, (j + 1) * SPAN)
            log_decay = log_all[here]
            high, low = split_two(log_decay)
            cum = mm(tri_two, jnp.concatenate([high, low], axis=0))
            middle = cum[SPAN // 2 - 1 : SPAN // 2]
            ending = cum[SPAN - 1 :]
            e_cm = jnp.exp(cum - middle)
            e_pm = jnp.exp(cum - log_decay - middle)
            shrink = jnp.exp(middle - cum)
            e_mid = jnp.exp(middle)
            e_tail = jnp.exp(ending - middle)
            unit, key = unit_all[here], key_all[here]
            value = v_ref[pl.ds(start + j * SPAN, SPAN), lanes]
            turned = jnp.concatenate([value[:, half:], value[:, :half]], axis=1)
            recept = r_ref[pl.ds(start + j * SPAN, SPAN), lanes].astype(F32)
            probes = unit * e_pm
            queries = recept * e_cm
            back_removal = removal_all[here] * shrink
            back_keys = key * shrink
            left = jnp.concatenate(
                [
                    jnp.where(first, probes, 0.0),
                    jnp.where(first, 0.0, probes),
                    jnp.where(first, queries, 0.0),
                    jnp.where(first, 0.0, queries),
                ],
                axis=0,
            )
            products = mm_nt(left, jnp.concatenate([back_removal, back_keys], axis=0))
            for h in range(2):
                strict_parts.append(
                    jnp.where(strict, products[h * SPAN : (h + 1) * SPAN, :SPAN], 0.0)
                )
            items.append(
                dict(
                    products=products,
                    turned=turned,
                    carrying=probes * e_mid,
                    reading=queries * e_mid,
                    removal_tail=back_removal * e_tail,
                    key_tail=back_keys * e_tail,
                    fade=jnp.exp(ending),
                )
            )
        inverses = lower_inverses(strict_parts, rows, cols)
        for j in range(spans):
            item = items[j]
            products, turned = item["products"], item["turned"]
            solved, removed, kept = [], [], []
            for h in range(2):
                top = slice(h * SPAN, (h + 1) * SPAN)
                bottom = slice((2 + h) * SPAN, (3 + h) * SPAN)
                pair_keys = jnp.where(strict, products[top, SPAN:], 0.0)
                read_removal = jnp.where(inclusive, products[bottom, :SPAN], 0.0)
                read_keys = jnp.where(inclusive, products[bottom, SPAN:], 0.0)
                both = mm(jnp.concatenate([pair_keys, read_keys], axis=0), turned)
                own = first if h == 0 else jnp.logical_not(first)
                right = jnp.where(own, item["carrying"], both[:SPAN])
                answer = mm(inverses[2 * j + h], right)
                solved.append(answer)
                removed.append(mm(read_removal, answer))
                kept.append(both[SPAN:])
            carried = jnp.where(first, solved[0], solved[1])
            local_turned = jnp.where(first, solved[1], solved[0])
            reader = item["reading"] - jnp.where(first, removed[0], removed[1])
            read_turned = jnp.where(first, kept[1] - removed[1], kept[0] - removed[0])
            local_read = jnp.concatenate([read_turned[:, half:], read_turned[:, :half]], axis=1)
            taken = mm_tn(
                jnp.concatenate([carried, local_turned], axis=1), item["removal_tail"]
            )
            offset_turned = mm_tn(turned, item["key_tail"]) - taken[LANES:]
            offset = jnp.concatenate([offset_turned[half:], offset_turned[:half]], axis=0)
            offset = jnp.where(matched, offset, 0.0)
            transition = jnp.where(diagonal, item["fade"], 0.0) - jnp.where(
                matched, taken[:LANES], 0.0
            )
            now = state[...]
            reads = mm_nt(reader, now)
            here = pl.ds(start + j * SPAN, SPAN)
            local_ref[here, lanes] = local_read + reads[:, :LANES]
            reader_ref[pl.ds(start + j * SPAN, SPAN), lanes] = reads[:, LANES:].astype(BF16)
            now_high, now_low = split_two(now)
            step_high, step_low = split_two(transition)
            moved = mm(now_high, step_high) + mm(now_low, step_high) + mm(now_high, step_low)
            state[:LANES] = moved[:LANES] + offset
            state[LANES:] = moved[LANES:]
        return nothing

    lax.fori_loop(0, r_ref.shape[0] // (STACK * SPAN), advance, 0)
    summary_ref[1, spot] = (state[:half] + state[half:LANES]).astype(BF16)
    summary_ref[0, spot] = (state[LANES : LANES + half] + state[LANES + half :]).astype(BF16)


def gated(x, gate, up):
    gates = mm(x, gate)
    uppers = mm(x, up)
    return (gates / (1.0 + jnp.exp(-gates)) * uppers).astype(BF16)


def layer_kernel(capacity, head_size, *refs):
    (
        r_hbm,
        k_hbm,
        v_hbm,
        d_hbm,
        l_hbm,
        base_hbm,
        shift_hbm,
        gain_hbm,
        project_hbm,
        tokens_hbm,
        scale_hbm,
        routes_hbm,
        weight_hbm,
        gate_hbm,
        up_hbm,
        down_hbm,
        mixer_ref,
        expert_ref,
        r_ref,
        k_ref,
        v_ref,
        d_ref,
        l_ref,
        base_ref,
        shift_in,
        gain_ref,
        project,
        tokens_ref,
        scale_ref,
        routes_ref,
        weight_ref,
        own_gate,
        own_up,
        own_down,
        near_gate,
        near_up,
        near_down,
        far_gate,
        far_up,
        far_down,
        cross_gate,
        cross_up,
        cross_down,
        shift_ref,
        reader,
        local,
        summary,
        state,
        outgoing,
        x_ref,
        total,
        hidden_ref,
        before,
        sending,
        passed,
        mixed,
        staged,
        landed,
        term,
        near_in,
        pair_out,
        far_in,
        combined,
        load_sems,
        post_send,
        post_recv,
        back_send,
        back_recv,
        round_send,
        round_recv,
        side_send,
        side_recv,
    ) = refs
    here = lax.axis_index("ep")
    count = lax.axis_size("ep")
    place = lax.axis_index("tp")
    low, high = lax.rem(place, 2), place // 2
    beside = place + 1 - 2 * low
    across = place + 2 - 4 * high
    reach_half = count // 2
    local_index, own_half = lax.rem(here, reach_half), here // reach_half
    rounds = passed.shape[0]
    half = LANES // 2
    pairs = before.shape[1]
    rows = x_ref.shape[0]
    units = own_gate.shape[1]
    tokens = expert_ref.shape[0]
    matched = same_head(head_size)
    block = matched.astype(BF16)
    diagonal = grid_index((LANES, LANES), 0) == grid_index((LANES, LANES), 1)

    pieces = [
        (tokens_hbm, tokens_ref),
        (scale_hbm, scale_ref),
        (routes_hbm, routes_ref),
        (weight_hbm, weight_ref),
        (base_hbm, base_ref),
        (shift_hbm, shift_in),
        (gain_hbm, gain_ref),
        (r_hbm, r_ref),
        (k_hbm, k_ref),
        (v_hbm, v_ref),
        (d_hbm, d_ref),
        (l_hbm, l_ref),
        (gate_hbm, own_gate),
        (up_hbm, own_up),
        (down_hbm, own_down),
        (project_hbm, project),
    ]
    loads = [
        pltpu.make_async_copy(src, dst, load_sems.at[i]) for i, (src, dst) in enumerate(pieces)
    ]
    keep_sem = load_sems.at[len(pieces)]
    barrier = pltpu.get_barrier_semaphore()
    greet_all(barrier, here, count, (beside, across))
    for load in loads:
        load.start()

    def side(src, dst, index, target):
        return send_to(src, dst, side_send.at[index], side_recv.at[index], {"tp": target})

    def rows_of(member):
        return pl.ds(pl.multiple_of(member * capacity, capacity), capacity)

    def partner(k, sign):
        crossing, shift = (k + 1) // reach_half, lax.rem(k + 1, reach_half)
        member = lax.rem(local_index + reach_half + sign * shift, reach_half)
        return member + reach_half * (own_half + crossing * (1 - 2 * own_half))

    def post(k, member):
        return send_to(
            outgoing.at[rows_of(member)],
            x_ref.at[rows_of(here)],
            post_send.at[k],
            post_recv.at[k],
            {"ep": member},
        )

    def back(k, member):
        return send_to(
            staged.at[rows_of(member)],
            landed.at[rows_of(here)],
            back_send.at[k],
            back_recv.at[k],
            {"ep": member},
        )

    cut = units // 2
    fars = [side(gate_hbm, far_gate, 0, across), side(up_hbm, far_up, 1, across)] + [
        side(down_hbm.at[i * cut : (i + 1) * cut], far_down.at[i * cut : (i + 1) * cut], 2 + i, across)
        for i in range(2)
    ]
    nears = [
        side(gate_hbm, near_gate, 4, beside),
        side(up_hbm, near_up, 5, beside),
        side(down_hbm, near_down, 6, beside),
    ]
    forwards = [side(far_gate, cross_gate, 7, beside), side(far_up, cross_up, 8, beside)] + [
        side(
            far_down.at[i * cut : (i + 1) * cut], cross_down.at[i * cut : (i + 1) * cut], 9 + i, beside
        )
        for i in range(2)
    ]

    pl.semaphore_wait(barrier, count + 1)
    for copy in fars + nears:
        copy.start()
    for load in loads[:3]:
        load.wait()
    pack_rows(tokens_ref, scale_ref, routes_ref, outgoing, count, capacity)

    def launch_post(k, nothing):
        post(k, partner(k, 1)).start()
        return nothing

    lax.fori_loop(0, count - 1, launch_post, 0)
    keep = pltpu.make_async_copy(outgoing.at[rows_of(here)], x_ref.at[rows_of(here)], keep_sem)
    keep.start()

    for load in loads[3:12]:
        load.wait()
    shift_ref[...] = shift_in[...].T

    def scan(p, nothing):
        scan_pair(
            p,
            head_size,
            r_ref,
            k_ref,
            v_ref,
            d_ref,
            l_ref,
            base_ref,
            shift_ref,
            reader,
            local,
            summary,
            state,
        )
        return nothing

    lax.fori_loop(0, pairs, scan, 0)

    def transfer(level, distance, target):
        return send_to(
            sending,
            passed.at[level],
            round_send.at[distance - 1],
            round_recv.at[level],
            {"ep": target},
        )

    def transfer_state(level, distance, target):
        return send_to(
            sending.at[1],
            passed.at[level, 1],
            round_send.at[distance - 1],
            round_recv.at[level],
            {"ep": target},
        )

    def sends_all(reach):
        return (lax.rem(here, 2 * reach) == reach - 1) & (here >= 2 * reach)

    def wide(part):
        part = part.astype(F32)
        return jnp.where(matched, jnp.concatenate([part, part], axis=0), 0.0)

    def spot(p):
        return slice(p * half, (p + 1) * half)

    for p in range(pairs):
        before[0, p] = jnp.where(diagonal, 1.0, 0.0)
        before[1, p] = jnp.zeros((LANES, LANES), F32)

    def send_round(level):
        reach = 2**level

        @pl.when(lax.rem(here, 2 * reach) == reach - 1)
        def _():
            for p in range(pairs):
                both = jnp.concatenate([before[0, p], before[1, p]], axis=0)
                upper, lower = split_two(both)
                step = wide(summary[0, spot(p)])
                moved = mm(upper, step) + mm(lower, step)
                after = moved[LANES:] + wide(summary[1, spot(p)])
                sending[0, spot(p)] = (moved[:half] + moved[half:LANES]).astype(BF16)
                sending[1, spot(p)] = (after[:half] + after[half:]).astype(BF16)

        def launch_with(transfer):
            def launch(distance, nothing):
                transfer(level, distance, here + distance).start()
                return nothing

            lax.fori_loop(1, reach + 1, launch, 0)

        pl.when(sends_all(reach))(lambda: launch_with(transfer))
        pl.when(here == reach - 1)(lambda: launch_with(transfer_state))

    def take_round(level):
        reach = 2**level

        @pl.when((lax.rem(here // reach, 2) == 1) & (here >= 2 * reach))
        def _():
            transfer(level, 1, here).wait_recv()
            for p in range(pairs):
                both = jnp.concatenate(
                    [wide(passed[level, 0, spot(p)]), wide(passed[level, 1, spot(p)])], axis=0
                )
                upper, lower = split_two(before[0, p])
                moved = mm(both, upper) + mm(both, lower)
                before[0, p] = moved[:LANES]
                before[1, p] = moved[LANES:] + before[1, p]

        @pl.when((here >= reach) & (here < 2 * reach))
        def _():
            transfer_state(level, 1, here).wait_recv()
            for p in range(pairs):
                entering = wide(passed[level, 1, spot(p)])
                upper, lower = split_two(before[0, p])
                before[1, p] = mm(entering, upper) + mm(entering, lower) + before[1, p]

    def settle_with(transfer, level, reach):
        def settle(distance, nothing):
            transfer(level, distance, here + distance).wait_send()
            return nothing

        lax.fori_loop(1, reach + 1, settle, 0)

    def at_half(which):
        return pl.ds(pl.multiple_of(which * (rows // 2), rows // 2), rows // 2)

    def full_parts(at):
        x = x_ref[at]
        total[at] = mm(gated(x, own_gate[...], own_up[...]), own_down[...])
        total[at] += mm(gated(x, near_gate[...], near_up[...]), near_down[...])

    def far_parts(at):
        x = x_ref[at]
        hidden_ref[at, :units] = gated(x, far_gate[...], far_up[...])
        hidden_ref[at, units:] = gated(x, cross_gate[...], cross_up[...])

    def take_post(k, nothing):
        post(k, partner(k, -1)).wait_recv()
        return nothing

    send_round(0)
    for load in loads[12:15]:
        load.wait()
    keep.wait()
    for copy in nears:
        copy.wait_recv()
    lax.fori_loop(0, reach_half - 1, take_post, 0)
    full_parts(at_half(own_half))
    fars[0].wait_recv()
    forwards[0].start()
    take_round(0)
    if rounds > 1:
        send_round(1)
    fars[1].wait_recv()
    forwards[1].start()
    lax.fori_loop(reach_half - 1, count - 1, take_post, 0)
    full_parts(at_half(1 - own_half))
    for level in range(1, min(rounds, 2)):
        take_round(level)
        if level + 1 < rounds:
            send_round(level + 1)
    for copy in forwards[:2]:
        copy.wait_recv()

    def far_step(i, nothing):
        far_parts(at_half(i))
        return nothing

    lax.fori_loop(0, 2, far_step, 0)
    for level in range(2, rounds):
        take_round(level)
        if level + 1 < rounds:
            send_round(level + 1)

    for i in range(2):
        fars[2 + i].wait_recv()
        forwards[2 + i].start()
    for copy in forwards[2:]:
        copy.wait_recv()

    def finished(member):
        at = rows_of(member)
        hidden = hidden_ref[at]
        row = total[at] + mm(hidden[:, :units], far_down[...])
        return (row + mm(hidden[:, units:], cross_down[...])).astype(BF16)

    def send_back(k, nothing):
        k = lax.rem(k + reach_half - 1, count - 1)
        member = partner(k, 1)
        staged[rows_of(member)] = finished(member)
        back(k, member).start()
        return nothing

    lax.fori_loop(0, count - 1, send_back, 0)
    landed[rows_of(here)] = finished(here)

    loads[15].wait()
    for p in range(pairs):
        lanes = slice(p * LANES, (p + 1) * LANES)
        read = mm_nt(reader[:, lanes], before[1, p]) + local[:, lanes]
        centred = read - head_sums(read, block) * (1.0 / head_size)
        variance = head_sums(centred * centred, block) * (1.0 / head_size)
        scaled = centred * lax.rsqrt(variance + GROUP_EPS) * gain_ref[:, lanes]
        mixed[:, lanes] = scaled.astype(BF16)

    def block_rows(b):
        return pl.ds(pl.multiple_of(b * tokens, tokens), tokens)

    def project_block(b, nothing):
        at = block_rows(b)
        term[at] = mm(mixed[at], project[...]).astype(BF16)
        return nothing

    lax.fori_loop(0, 4, project_block, 0)
    sums = [
        side(term.at[block_rows(2 * y + 1 - low)], near_in.at[y], 11 + y, beside)
        for y in range(2)
    ]
    for copy in sums:
        copy.start()

    picks = routes_ref.shape[0]
    packed = jnp.concatenate(
        [routes_ref[...].astype(F32), weight_ref[...], jnp.zeros((8 - 2 * picks, tokens), F32)],
        axis=0,
    ).T
    lane = grid_index((tokens, LANES), 1)
    routes = [packed[:, i : i + 1].astype(jnp.int32) for i in range(picks)]
    weight = packed[:, picks : 2 * picks]
    named = jnp.zeros((tokens, LANES), F32)
    for route in routes:
        named = jnp.where(route == lane, 1.0, named)
    earlier = grid_index((tokens, tokens), 0) > grid_index((tokens, tokens), 1)
    slots = mm(earlier.astype(F32), named)
    target = jnp.concatenate(
        [
            route * capacity
            + jnp.sum(jnp.where(route == lane, slots, 0.0), axis=1, keepdims=True).astype(
                jnp.int32
            )
            for route in routes
        ],
        axis=1,
    )
    slot = grid_index((tokens, capacity), 1)

    def taken(member):
        table = jnp.zeros((tokens, capacity), F32)
        scale = jnp.zeros((tokens, 1), F32)
        for picked in range(target.shape[1]):
            own = target[:, picked : picked + 1] - member * capacity
            table = jnp.where(own == slot, 1.0, table)
            inside = (own >= 0) & (own < capacity)
            scale = jnp.where(inside, weight[:, picked : picked + 1], scale)
        return mm(table, landed[rows_of(member)]) * scale

    combined[...] = taken(here)

    for copy in sums:
        copy.wait_recv()
    other = 1 - high
    pair_out[...] = (
        term[block_rows(2 * other + low)].astype(F32) + near_in[other].astype(F32)
    ).astype(BF16)
    last_sum = side(pair_out, far_in, 13, across)
    last_sum.start()

    def gather_block(k, nothing):
        member = partner(k, -1)
        back(k, member).wait_recv()
        combined[...] += taken(member)
        return nothing

    lax.fori_loop(0, reach_half - 1, gather_block, 0)
    last_sum.wait_recv()
    kept = term[block_rows(2 * high + low)].astype(F32) + near_in[high].astype(F32)
    mixer_ref[...] = (kept + far_in[...].astype(F32)).astype(BF16)
    lax.fori_loop(reach_half - 1, count - 1, gather_block, 0)
    expert_ref[...] = combined[...].astype(BF16)

    def settle_rows(k, nothing):
        post(k, partner(k, 1)).wait_send()
        back(k, partner(k, 1)).wait_send()
        return nothing

    lax.fori_loop(0, count - 1, settle_rows, 0)
    for level in range(rounds):
        reach = 2**level
        pl.when(sends_all(reach))(functools.partial(settle_with, transfer, level, reach))
        pl.when(here == reach - 1)(
            functools.partial(settle_with, transfer_state, level, reach)
        )
    for copy in fars + nears + forwards + sums + [last_sum]:
        copy.wait_send()


def whole_layer(streams, base, shift, gain, out_weight, tokens, scale, routes, weights, own, head_size, capacity):
    rows, channels = streams[0].shape
    pairs = channels // LANES
    half = LANES // 2
    count = lax.axis_size("ep")
    rounds = (count - 1).bit_length()
    token_rows, width = tokens.shape
    slots = count * capacity
    units = own[0].shape[1]
    inputs = list(streams) + [
        base.reshape(1, channels),
        shift.T,
        gain.reshape(1, channels),
        out_weight,
        tokens,
        scale.reshape(1, width),
        routes.T,
        weights.T,
    ]
    operands = [in_hbm(array) for array in inputs + list(own)]
    block = (token_rows, width)
    wide, tall = (width, units), (units, width)
    held = [pltpu.VMEM(array.shape, array.dtype) for array in inputs]
    shards = [pltpu.VMEM(shape, BF16) for shape in (wide, wide, tall) * 4]
    dma = pltpu.SemaphoreType.DMA
    return pl.pallas_call(
        functools.partial(layer_kernel, capacity, head_size),
        in_specs=[pl.BlockSpec(memory_space=pl.ANY)] * len(operands),
        out_specs=[pl.BlockSpec(memory_space=pltpu.VMEM)] * 2,
        out_shape=[jax.ShapeDtypeStruct(block, BF16)] * 2,
        scratch_shapes=held
        + shards
        + [
            pltpu.VMEM(shift.shape, F32),
            pltpu.VMEM((rows, channels), BF16),
            pltpu.VMEM((rows, channels), F32),
            pltpu.VMEM((2, pairs * half, LANES), BF16),
            pltpu.VMEM((2 * LANES, LANES), F32),
            pltpu.VMEM((slots, width), BF16),
            pltpu.VMEM((slots, width), BF16),
            pltpu.VMEM((slots, width), F32),
            pltpu.VMEM((slots, 2 * units), BF16),
            pltpu.VMEM((2, pairs, LANES, LANES), F32),
            pltpu.VMEM((2, pairs * half, LANES), BF16),
            pltpu.VMEM((rounds, 2, pairs * half, LANES), BF16),
            pltpu.VMEM((rows, channels), BF16),
            pltpu.VMEM((slots, width), BF16),
            pltpu.VMEM((slots, width), BF16),
            pltpu.VMEM((rows, width), BF16),
            pltpu.VMEM((2,) + block, BF16),
            pltpu.VMEM(block, BF16),
            pltpu.VMEM(block, BF16),
            pltpu.VMEM(block, F32),
            dma((len(operands) + 1,)),
            dma((count - 1,)),
            dma((count - 1,)),
            dma((count - 1,)),
            dma((count - 1,)),
            dma((count // 2,)),
            dma((rounds,)),
            dma((14,)),
            dma((14,)),
        ],
        compiler_params=pltpu.CompilerParams(
            vmem_limit_bytes=48 * 2**20, collective_id=0, has_side_effects=True
        ),
        cost_estimate=pl.CostEstimate(
            flops=40 * 10**9, bytes_accessed=20 * 2**20, transcendentals=2 * 10**6
        ),
        name="whole_layer",
    )(*operands)


def on_device(
    receptance,
    key_rows,
    value_rows,
    decay_input,
    learn_input,
    decay_base,
    decay_shift,
    channel_gain,
    out_weight,
    expert_input,
    expert_gain,
    routes,
    route_weight,
    gate_weight,
    up_weight,
    down_weight,
):
    head_size = receptance.shape[1] // decay_shift.shape[1]
    experts = gate_weight.shape[0] * lax.axis_size("ep")
    capacity = max(2, 2 * expert_input.shape[0] * routes.shape[1] // experts)
    return tuple(
        whole_layer(
            (receptance, key_rows, value_rows, decay_input, learn_input),
            decay_base,
            decay_shift,
            channel_gain,
            out_weight,
            expert_input,
            expert_gain,
            routes,
            route_weight,
            (gate_weight[0], up_weight[0], down_weight[0]),
            head_size,
            capacity,
        )
    )


def solution(mesh):
    return jax.shard_map(
        on_device,
        mesh=mesh,
        in_specs=(
            P("ep", "tp"),
            P("ep", "tp"),
            P("ep", "tp"),
            P("ep", "tp"),
            P("ep", "tp"),
            P("tp"),
            P("ep", "tp"),
            P("tp"),
            P("tp", None),
            P(("ep", "tp"), None),
            P(),
            P(("ep", "tp"), None),
            P(("ep", "tp"), None),
            P("ep", None, "tp"),
            P("ep", None, "tp"),
            P("ep", "tp", None),
        ),
        out_specs=(P(("ep", "tp"), None), P(("ep", "tp"), None)),
        check_vma=False,
    )
```

```python
import functools

import jax
import jax.numpy as jnp
from jax import lax
from jax.experimental import pallas as pl
from jax.experimental.pallas import tpu as pltpu
from jax.sharding import PartitionSpec as P

SPAN = 128
STACK = 2
LANES = 128
EARLY = 3

NORM_EPS = 1e-06
GROUP_EPS = 0.00064
KEY_EPS = 1e-06
F32 = jnp.float32
BF16 = jnp.bfloat16


def mm(a, b):
    return lax.dot_general(
        a.astype(BF16), b.astype(BF16), (((1,), (0,)), ((), ())), preferred_element_type=F32
    )


def mm_nt(a, b):
    return lax.dot_general(
        a.astype(BF16), b.astype(BF16), (((1,), (1,)), ((), ())), preferred_element_type=F32
    )


def mm_tn(a, b):
    return lax.dot_general(
        a.astype(BF16), b.astype(BF16), (((0,), (0,)), ((), ())), preferred_element_type=F32
    )


def split_two(x):
    high = x.astype(BF16)
    return high, (x - high.astype(F32)).astype(BF16)


def grid_index(shape, axis):
    return lax.broadcasted_iota(jnp.int32, shape, axis)


def same_head(head_size):
    rows = grid_index((LANES, LANES), 0) // head_size
    cols = grid_index((LANES, LANES), 1) // head_size
    return rows == cols


def head_sums(x, block):
    high, low = split_two(x)
    return mm(
        jnp.concatenate([high, low], axis=1), jnp.concatenate([block, block], axis=0)
    )


def lower_inverses(strict_parts, rows, cols):
    eye = jnp.where(rows == cols, 1.0, 0.0)
    size = 1
    inverses = None
    while size < SPAN:
        off = (rows // (2 * size) == cols // (2 * size)) & (rows // size != cols // size)
        parts = [jnp.where(off, part, 0.0) for part in strict_parts]
        if inverses is None:
            inverses = [eye - part for part in parts]
        else:
            firsts = [mm(part, inv) for part, inv in zip(parts, inverses)]
            inverses = [inv - mm(inv, first) for inv, first in zip(inverses, firsts)]
        size *= 2
    return inverses


def send_to(src, dst, send_sem, recv_sem, target):
    return pltpu.make_async_remote_copy(
        src_ref=src,
        dst_ref=dst,
        send_sem=send_sem,
        recv_sem=recv_sem,
        device_id=target,
        device_id_type=pl.DeviceIdType.MESH,
    )


def greet_all(barrier, here, count, others):
    def greet(distance, nothing):
        pl.semaphore_signal(
            barrier,
            inc=1,
            device_id={"ep": lax.rem(here + distance, count)},
            device_id_type=pl.DeviceIdType.MESH,
        )
        return nothing

    lax.fori_loop(1, count, greet, 0)
    for target in others:
        pl.semaphore_signal(
            barrier, inc=1, device_id={"tp": target}, device_id_type=pl.DeviceIdType.MESH
        )


def in_hbm(array):
    return pltpu.with_memory_space_constraint(array, pltpu.HBM)


def pack_rows(tokens_ref, scale_ref, routes_ref, outgoing, count, capacity):
    inputs = tokens_ref[...].astype(F32)
    square = jnp.sum(inputs * inputs, axis=1, keepdims=True) * (1.0 / inputs.shape[1])
    normed = (inputs * lax.rsqrt(square + NORM_EPS) * scale_ref[...]).astype(BF16)
    rows = inputs.shape[0]
    members = grid_index((count, rows), 0)
    named = jnp.zeros((count, rows), F32)
    for picked in range(routes_ref.shape[0]):
        named = jnp.where(routes_ref[picked : picked + 1] == members, 1.0, named)
    earlier = grid_index((rows, rows), 0) < grid_index((rows, rows), 1)
    slots = mm(named, earlier.astype(F32))
    slots = jnp.where(named > 0.5, slots, -1.0).astype(jnp.int32)
    wanted = grid_index((capacity, rows), 0)
    group = max(1, min(count, 256 // capacity))
    for begin in range(0, count, group):
        table = jnp.concatenate(
            [
                jnp.where(slots[e : e + 1] == wanted, 1.0, 0.0)
                for e in range(begin, begin + group)
            ],
            axis=0,
        )
        outgoing[begin * capacity : (begin + group) * capacity] = mm(table, normed).astype(BF16)


def scan_pair(
    pair,
    head_size,
    r_ref,
    k_ref,
    v_ref,
    d_ref,
    l_ref,
    base_ref,
    shift_ref,
    reader_ref,
    local_ref,
    summary_ref,
    state,
):
    half = LANES // 2
    lanes = pl.ds(pl.multiple_of(pair * LANES, LANES), LANES)
    spot = pl.ds(pl.multiple_of(pair * half, half), half)

    rows = grid_index((SPAN, SPAN), 0)
    cols = grid_index((SPAN, SPAN), 1)
    strict = rows > cols
    inclusive = rows >= cols
    first = grid_index((SPAN, LANES), 1) < half
    matched = same_head(head_size)
    block = matched.astype(BF16)
    diagonal = grid_index((LANES, LANES), 0) == grid_index((LANES, LANES), 1)
    tri = inclusive.astype(BF16)
    tri_two = jnp.concatenate([tri, tri], axis=1)

    state[:LANES] = jnp.zeros((LANES, LANES), F32)
    state[LANES:] = jnp.where(diagonal, 1.0, 0.0)

    heads = shift_ref.shape[1]
    chosen = grid_index((heads, LANES), 0) == 2 * pair + grid_index((heads, LANES), 1) // half
    def advance(step, nothing):
        start = pl.multiple_of(step * (STACK * SPAN), STACK * SPAN)
        rows_here = pl.ds(start, STACK * SPAN)
        shift = lax.dot_general(
            shift_ref[rows_here],
            chosen.astype(F32),
            (((1,), (0,)), ((), ())),
            precision=lax.Precision.HIGHEST,
            preferred_element_type=F32,
        )
        pre = d_ref[rows_here, lanes].astype(F32) + base_ref[:, lanes] + shift
        log_all = -0.6065306597126334 / (1.0 + jnp.exp(-pre))
        rates = 1.0 / (1.0 + jnp.exp(-l_ref[rows_here, lanes].astype(F32)))
        key_all = k_ref[rows_here, lanes].astype(F32)
        unit_all = key_all * lax.rsqrt(head_sums(key_all * key_all, block) + KEY_EPS)
        removal_all = unit_all * rates

        spans = STACK
        items = []
        strict_parts = []
        for j in range(spans):
            here = slice(j * SPAN, (j + 1) * SPAN)
            log_decay = log_all[here]
            high, low = split_two(log_decay)
            cum = mm(tri_two, jnp.concatenate([high, low], axis=0))
            middle = cum[SPAN // 2 - 1 : SPAN // 2]
            ending = cum[SPAN - 1 :]
            e_cm = jnp.exp(cum - middle)
            e_pm = jnp.exp(cum - log_decay - middle)
            shrink = jnp.exp(middle - cum)
            e_mid = jnp.exp(middle)
            e_tail = jnp.exp(ending - middle)
            unit, key = unit_all[here], key_all[here]
            value = v_ref[pl.ds(start + j * SPAN, SPAN), lanes]
            turned = jnp.concatenate([value[:, half:], value[:, :half]], axis=1)
            recept = r_ref[pl.ds(start + j * SPAN, SPAN), lanes].astype(F32)
            probes = unit * e_pm
            queries = recept * e_cm
            back_removal = removal_all[here] * shrink
            back_keys = key * shrink
            left = jnp.concatenate(
                [
                    jnp.where(first, probes, 0.0),
                    jnp.where(first, 0.0, probes),
                    jnp.where(first, queries, 0.0),
                    jnp.where(first, 0.0, queries),
                ],
                axis=0,
            )
            products = mm_nt(left, jnp.concatenate([back_removal, back_keys], axis=0))
            for h in range(2):
                strict_parts.append(
                    jnp.where(strict, products[h * SPAN : (h + 1) * SPAN, :SPAN], 0.0)
                )
            items.append(
                dict(
                    products=products,
                    turned=turned,
                    carrying=probes * e_mid,
                    reading=queries * e_mid,
                    removal_tail=back_removal * e_tail,
                    key_tail=back_keys * e_tail,
                    fade=jnp.exp(ending),
                )
            )
        inverses = lower_inverses(strict_parts, rows, cols)
        for j in range(spans):
            item = items[j]
            products, turned = item["products"], item["turned"]
            solved, removed, kept = [], [], []
            for h in range(2):
                top = slice(h * SPAN, (h + 1) * SPAN)
                bottom = slice((2 + h) * SPAN, (3 + h) * SPAN)
                pair_keys = jnp.where(strict, products[top, SPAN:], 0.0)
                read_removal = jnp.where(inclusive, products[bottom, :SPAN], 0.0)
                read_keys = jnp.where(inclusive, products[bottom, SPAN:], 0.0)
                both = mm(jnp.concatenate([pair_keys, read_keys], axis=0), turned)
                own = first if h == 0 else jnp.logical_not(first)
                right = jnp.where(own, item["carrying"], both[:SPAN])
                answer = mm(inverses[2 * j + h], right)
                solved.append(answer)
                removed.append(mm(read_removal, answer))
                kept.append(both[SPAN:])
            carried = jnp.where(first, solved[0], solved[1])
            local_turned = jnp.where(first, solved[1], solved[0])
            reader = item["reading"] - jnp.where(first, removed[0], removed[1])
            read_turned = jnp.where(first, kept[1] - removed[1], kept[0] - removed[0])
            local_read = jnp.concatenate([read_turned[:, half:], read_turned[:, :half]], axis=1)
            taken = mm_tn(
                jnp.concatenate([carried, local_turned], axis=1), item["removal_tail"]
            )
            offset_turned = mm_tn(turned, item["key_tail"]) - taken[LANES:]
            offset = jnp.concatenate([offset_turned[half:], offset_turned[:half]], axis=0)
            offset = jnp.where(matched, offset, 0.0)
            transition = jnp.where(diagonal, item["fade"], 0.0) - jnp.where(
                matched, taken[:LANES], 0.0
            )
            now = state[...]
            reads = mm_nt(reader, now)
            here = pl.ds(start + j * SPAN, SPAN)
            local_ref[here, lanes] = local_read + reads[:, :LANES]
            reader_ref[pl.ds(start + j * SPAN, SPAN), lanes] = reads[:, LANES:].astype(BF16)
            now_high, now_low = split_two(now)
            step_high, step_low = split_two(transition)
            moved = mm(now_high, step_high) + mm(now_low, step_high) + mm(now_high, step_low)
            state[:LANES] = moved[:LANES] + offset
            state[LANES:] = moved[LANES:]
        return nothing

    lax.fori_loop(0, r_ref.shape[0] // (STACK * SPAN), advance, 0)
    summary_ref[1, spot] = (state[:half] + state[half:LANES]).astype(BF16)
    summary_ref[0, spot] = (state[LANES : LANES + half] + state[LANES + half :]).astype(BF16)


def gated(x, gate, up):
    gates = mm(x, gate)
    uppers = mm(x, up)
    return (gates / (1.0 + jnp.exp(-gates)) * uppers).astype(BF16)


def layer_kernel(capacity, head_size, early, *refs):
    (
        r_hbm,
        k_hbm,
        v_hbm,
        d_hbm,
        l_hbm,
        base_hbm,
        shift_hbm,
        gain_hbm,
        project_hbm,
        tokens_hbm,
        scale_hbm,
        routes_hbm,
        weight_hbm,
        gate_hbm,
        up_hbm,
        down_hbm,
        mixer_ref,
        expert_ref,
        r_ref,
        k_ref,
        v_ref,
        d_ref,
        l_ref,
        base_ref,
        shift_in,
        gain_ref,
        project,
        tokens_ref,
        scale_ref,
        routes_ref,
        weight_ref,
        own_gate,
        own_up,
        own_down,
        near_gate,
        near_up,
        near_down,
        far_gate,
        far_up,
        far_down,
        cross_gate,
        cross_up,
        cross_down,
        shift_ref,
        reader,
        local,
        summary,
        state,
        outgoing,
        x_ref,
        total,
        hidden_ref,
        before,
        sending,
        passed,
        mixed,
        theirs,
        part_out,
        part_in,
        staged_early,
        staged_late,
        landed_early,
        landed_late,
        term,
        near_in,
        pair_out,
        far_in,
        combined,
        load_sems,
        post_send,
        post_recv,
        back_send,
        back_recv,
        part_send,
        part_recv,
        round_send,
        round_recv,
        side_send,
        side_recv,
    ) = refs
    here = lax.axis_index("ep")
    count = lax.axis_size("ep")
    place = lax.axis_index("tp")
    low, high = lax.rem(place, 2), place // 2
    beside = place + 1 - 2 * low
    across = place + 2 - 4 * high
    reach_half = count // 2
    local_index, own_half = lax.rem(here, reach_half), here // reach_half
    rounds = passed.shape[0]
    half = LANES // 2
    pairs = before.shape[1]
    rows = x_ref.shape[0]
    units = own_gate.shape[1]
    tokens = expert_ref.shape[0]
    matched = same_head(head_size)
    block = matched.astype(BF16)
    diagonal = grid_index((LANES, LANES), 0) == grid_index((LANES, LANES), 1)

    pieces = [
        (tokens_hbm, tokens_ref),
        (scale_hbm, scale_ref),
        (routes_hbm, routes_ref),
        (weight_hbm, weight_ref),
        (base_hbm, base_ref),
        (shift_hbm, shift_in),
        (gain_hbm, gain_ref),
        (r_hbm, r_ref),
        (k_hbm, k_ref),
        (v_hbm, v_ref),
        (d_hbm, d_ref),
        (l_hbm, l_ref),
        (gate_hbm, own_gate),
        (up_hbm, own_up),
        (down_hbm, own_down),
        (project_hbm, project),
    ]
    loads = [
        pltpu.make_async_copy(src, dst, load_sems.at[i]) for i, (src, dst) in enumerate(pieces)
    ]
    keep_sem = load_sems.at[len(pieces)]
    barrier = pltpu.get_barrier_semaphore()
    greet_all(barrier, here, count, (beside, across))
    for load in loads:
        load.start()

    def side(src, dst, index, target):
        return send_to(src, dst, side_send.at[index], side_recv.at[index], {"tp": target})

    def rows_of(member):
        return pl.ds(pl.multiple_of(member * capacity, capacity), capacity)

    def partner(k, sign):
        crossing, shift = (k + 1) // reach_half, lax.rem(k + 1, reach_half)
        member = lax.rem(local_index + reach_half + sign * shift, reach_half)
        return member + reach_half * (own_half + crossing * (1 - 2 * own_half))

    def post(k, member):
        return send_to(
            outgoing.at[rows_of(member)],
            x_ref.at[rows_of(here)],
            post_send.at[k],
            post_recv.at[k],
            {"ep": member},
        )

    def back(k, member, late):
        staged, landed = (staged_late, landed_late) if late else (staged_early, landed_early)
        return send_to(
            staged.at[rows_of(member)],
            landed.at[rows_of(here)],
            back_send.at[late, k],
            back_recv.at[late, k],
            {"ep": member},
        )

    def part(member):
        return send_to(
            part_out.at[rows_of(member)],
            part_in.at[rows_of(member)],
            part_send.at[member],
            part_recv.at[member],
            {"tp": across},
        )

    def at_half(which):
        return pl.ds(pl.multiple_of(which * (rows // 2), rows // 2), rows // 2)

    halves = (1 - own_half, own_half)
    asks = [
        side(hidden_ref.at[at_half(which)], theirs.at[at_half(which)], 14 + i, across)
        for i, which in enumerate(halves)
    ]

    cut = units // 2
    fars = [side(gate_hbm, far_gate, 0, across), side(up_hbm, far_up, 1, across)] + [
        side(
            down_hbm.at[i * cut : (i + 1) * cut, :early],
            far_down.at[i * cut : (i + 1) * cut],
            2 + i,
            across,
        )
        for i in range(2)
    ]
    nears = [
        side(gate_hbm, near_gate, 4, beside),
        side(up_hbm, near_up, 5, beside),
        side(down_hbm, near_down, 6, beside),
    ]
    forwards = [side(far_gate, cross_gate, 7, beside), side(far_up, cross_up, 8, beside)] + [
        side(
            far_down.at[i * cut : (i + 1) * cut], cross_down.at[i * cut : (i + 1) * cut], 9 + i, beside
        )
        for i in range(2)
    ]

    pl.semaphore_wait(barrier, count + 1)
    for copy in fars + nears:
        copy.start()
    for load in loads[:3]:
        load.wait()
    pack_rows(tokens_ref, scale_ref, routes_ref, outgoing, count, capacity)

    def launch_post(k, nothing):
        post(k, partner(k, 1)).start()
        return nothing

    lax.fori_loop(0, count - 1, launch_post, 0)
    keep = pltpu.make_async_copy(outgoing.at[rows_of(here)], x_ref.at[rows_of(here)], keep_sem)
    keep.start()

    for load in loads[3:12]:
        load.wait()
    shift_ref[...] = shift_in[...].T

    def scan(p, nothing):
        scan_pair(
            p,
            head_size,
            r_ref,
            k_ref,
            v_ref,
            d_ref,
            l_ref,
            base_ref,
            shift_ref,
            reader,
            local,
            summary,
            state,
        )
        return nothing

    lax.fori_loop(0, pairs, scan, 0)

    def transfer(level, distance, target):
        return send_to(
            sending,
            passed.at[level],
            round_send.at[distance - 1],
            round_recv.at[level],
            {"ep": target},
        )

    def transfer_state(level, distance, target):
        return send_to(
            sending.at[1],
            passed.at[level, 1],
            round_send.at[distance - 1],
            round_recv.at[level],
            {"ep": target},
        )

    def sends_all(reach):
        return (lax.rem(here, 2 * reach) == reach - 1) & (here >= 2 * reach)

    def wide(part):
        part = part.astype(F32)
        return jnp.where(matched, jnp.concatenate([part, part], axis=0), 0.0)

    def spot(p):
        return slice(p * half, (p + 1) * half)

    for p in range(pairs):
        before[0, p] = jnp.where(diagonal, 1.0, 0.0)
        before[1, p] = jnp.zeros((LANES, LANES), F32)

    def send_round(level):
        reach = 2**level

        @pl.when(lax.rem(here, 2 * reach) == reach - 1)
        def _():
            for p in range(pairs):
                both = jnp.concatenate([before[0, p], before[1, p]], axis=0)
                upper, lower = split_two(both)
                step = wide(summary[0, spot(p)])
                moved = mm(upper, step) + mm(lower, step)
                after = moved[LANES:] + wide(summary[1, spot(p)])
                sending[0, spot(p)] = (moved[:half] + moved[half:LANES]).astype(BF16)
                sending[1, spot(p)] = (after[:half] + after[half:]).astype(BF16)

        def launch_with(transfer):
            def launch(distance, nothing):
                transfer(level, distance, here + distance).start()
                return nothing

            lax.fori_loop(1, reach + 1, launch, 0)

        pl.when(sends_all(reach))(lambda: launch_with(transfer))
        pl.when(here == reach - 1)(lambda: launch_with(transfer_state))

    def take_round(level):
        reach = 2**level

        @pl.when((lax.rem(here // reach, 2) == 1) & (here >= 2 * reach))
        def _():
            transfer(level, 1, here).wait_recv()
            for p in range(pairs):
                both = jnp.concatenate(
                    [wide(passed[level, 0, spot(p)]), wide(passed[level, 1, spot(p)])], axis=0
                )
                upper, lower = split_two(before[0, p])
                moved = mm(both, upper) + mm(both, lower)
                before[0, p] = moved[:LANES]
                before[1, p] = moved[LANES:] + before[1, p]

        @pl.when((here >= reach) & (here < 2 * reach))
        def _():
            transfer_state(level, 1, here).wait_recv()
            for p in range(pairs):
                entering = wide(passed[level, 1, spot(p)])
                upper, lower = split_two(before[0, p])
                before[1, p] = mm(entering, upper) + mm(entering, lower) + before[1, p]

    def settle_with(transfer, level, reach):
        def settle(distance, nothing):
            transfer(level, distance, here + distance).wait_send()
            return nothing

        lax.fori_loop(1, reach + 1, settle, 0)

    def full_parts(at):
        x = x_ref[at]
        total[at] = mm(gated(x, own_gate[...], own_up[...]), own_down[...])
        total[at] += mm(gated(x, near_gate[...], near_up[...]), near_down[...])

    def far_parts(at):
        x = x_ref[at]
        hidden_ref[at, :units] = gated(x, far_gate[...], far_up[...])
        hidden_ref[at, units:] = gated(x, cross_gate[...], cross_up[...])

    def take_post(k, nothing):
        post(k, partner(k, -1)).wait_recv()
        return nothing

    send_round(0)
    for load in loads[12:15]:
        load.wait()
    keep.wait()
    for copy in nears:
        copy.wait_recv()
    lax.fori_loop(0, reach_half - 1, take_post, 0)
    full_parts(at_half(own_half))
    fars[0].wait_recv()
    forwards[0].start()
    take_round(0)
    if rounds > 1:
        send_round(1)
    fars[1].wait_recv()
    forwards[1].start()
    lax.fori_loop(reach_half - 1, count - 1, take_post, 0)
    full_parts(at_half(1 - own_half))
    for copy in forwards[:2]:
        copy.wait_recv()

    for i in range(2):
        far_parts(at_half(halves[i]))
        asks[i].start()
    for level in range(1, min(rounds, 2)):
        take_round(level)
        if level + 1 < rounds:
            send_round(level + 1)

    for i in range(2):
        fars[2 + i].wait_recv()
        forwards[2 + i].start()
    for copy in forwards[2:]:
        copy.wait_recv()

    def finished(member):
        at = rows_of(member)
        hidden = hidden_ref[at]
        row = total[at, :early] + mm(hidden[:, :units], far_down[...])
        return (row + mm(hidden[:, units:], cross_down[...])).astype(BF16)

    def send_back(k, nothing):
        k = lax.rem(k + reach_half - 1, count - 1)
        member = partner(k, 1)
        staged_early[rows_of(member)] = finished(member)
        back(k, member, 0).start()
        return nothing

    lax.fori_loop(0, count - 1, send_back, 0)
    landed_early[rows_of(here)] = finished(here)

    def answer(i):
        asks[i].wait_recv()
        at = at_half(halves[i])
        asked = theirs[at]
        product = mm(asked[:, :units], own_down[:, early:])
        product += mm(asked[:, units:], near_down[:, early:])
        part_out[at] = product.astype(BF16)

        def launch(j, nothing):
            part(halves[i] * reach_half + lax.rem(local_index + j, reach_half)).start()
            return nothing

        lax.fori_loop(0, reach_half, launch, 0)

    answer(0)
    answer(1)
    for level in range(2, rounds):
        take_round(level)
        if level + 1 < rounds:
            send_round(level + 1)
    loads[15].wait()
    for p in range(pairs):
        lanes = slice(p * LANES, (p + 1) * LANES)
        read = mm_nt(reader[:, lanes], before[1, p]) + local[:, lanes]
        centred = read - head_sums(read, block) * (1.0 / head_size)
        variance = head_sums(centred * centred, block) * (1.0 / head_size)
        scaled = centred * lax.rsqrt(variance + GROUP_EPS) * gain_ref[:, lanes]
        mixed[:, lanes] = scaled.astype(BF16)

    def block_rows(b):
        return pl.ds(pl.multiple_of(b * tokens, tokens), tokens)

    def project_block(b, nothing):
        at = block_rows(b)
        term[at] = mm(mixed[at], project[...]).astype(BF16)
        return nothing

    lax.fori_loop(0, 4, project_block, 0)
    sums = [
        side(term.at[block_rows(2 * y + 1 - low)], near_in.at[y], 11 + y, beside)
        for y in range(2)
    ]
    for copy in sums:
        copy.start()

    picks = routes_ref.shape[0]
    packed = jnp.concatenate(
        [routes_ref[...].astype(F32), weight_ref[...], jnp.zeros((8 - 2 * picks, tokens), F32)],
        axis=0,
    ).T
    lane = grid_index((tokens, LANES), 1)
    routes = [packed[:, i : i + 1].astype(jnp.int32) for i in range(picks)]
    weight = packed[:, picks : 2 * picks]
    named = jnp.zeros((tokens, LANES), F32)
    for route in routes:
        named = jnp.where(route == lane, 1.0, named)
    earlier = grid_index((tokens, tokens), 0) > grid_index((tokens, tokens), 1)
    slots = mm(earlier.astype(F32), named)
    target = jnp.concatenate(
        [
            route * capacity
            + jnp.sum(jnp.where(route == lane, slots, 0.0), axis=1, keepdims=True).astype(
                jnp.int32
            )
            for route in routes
        ],
        axis=1,
    )
    slot = grid_index((tokens, capacity), 1)

    def taken(member, late):
        table = jnp.zeros((tokens, capacity), F32)
        scale = jnp.zeros((tokens, 1), F32)
        for picked in range(target.shape[1]):
            own = target[:, picked : picked + 1] - member * capacity
            table = jnp.where(own == slot, 1.0, table)
            inside = (own >= 0) & (own < capacity)
            scale = jnp.where(inside, weight[:, picked : picked + 1], scale)
        landed = landed_late if late else landed_early
        return mm(table, landed[rows_of(member)]) * scale

    combined[:, :early] = taken(here, 0)

    for copy in sums:
        copy.wait_recv()
    other = 1 - high
    pair_out[...] = (
        term[block_rows(2 * other + low)].astype(F32) + near_in[other].astype(F32)
    ).astype(BF16)
    last_sum = side(pair_out, far_in, 13, across)
    last_sum.start()

    def late_rows(member):
        part(member).wait_recv()
        at = rows_of(member)
        return (total[at, early:] + part_in[at].astype(F32)).astype(BF16)

    def send_late(k, nothing):
        k = lax.rem(k + reach_half - 1, count - 1)
        member = partner(k, 1)
        staged_late[rows_of(member)] = late_rows(member)
        back(k, member, 1).start()
        return nothing

    def gather_early(k, nothing):
        member = partner(k, -1)
        back(k, member, 0).wait_recv()
        combined[:, :early] += taken(member, 0)
        return nothing

    def gather_late(k, nothing):
        member = partner(k, -1)
        back(k, member, 1).wait_recv()
        combined[:, early:] += taken(member, 1)
        return nothing

    lax.fori_loop(0, reach_half, send_late, 0)
    landed_late[rows_of(here)] = late_rows(here)
    combined[:, early:] = taken(here, 1)
    lax.fori_loop(reach_half, count - 1, send_late, 0)
    lax.fori_loop(0, count - 1, gather_early, 0)
    lax.fori_loop(0, reach_half - 1, gather_late, 0)
    last_sum.wait_recv()
    kept = term[block_rows(2 * high + low)].astype(F32) + near_in[high].astype(F32)
    mixer_ref[...] = (kept + far_in[...].astype(F32)).astype(BF16)
    lax.fori_loop(reach_half - 1, count - 1, gather_late, 0)
    expert_ref[...] = combined[...].astype(BF16)

    def settle_rows(k, nothing):
        post(k, partner(k, 1)).wait_send()
        back(k, partner(k, 1), 0).wait_send()
        back(k, partner(k, 1), 1).wait_send()
        return nothing

    def settle_part(member, nothing):
        part(member).wait_send()
        return nothing

    lax.fori_loop(0, count - 1, settle_rows, 0)
    lax.fori_loop(0, count, settle_part, 0)
    for level in range(rounds):
        reach = 2**level
        pl.when(sends_all(reach))(functools.partial(settle_with, transfer, level, reach))
        pl.when(here == reach - 1)(
            functools.partial(settle_with, transfer_state, level, reach)
        )
    for copy in fars + nears + forwards + asks + sums + [last_sum]:
        copy.wait_send()


def whole_layer(streams, base, shift, gain, out_weight, tokens, scale, routes, weights, own, head_size, capacity):
    rows, channels = streams[0].shape
    pairs = channels // LANES
    half = LANES // 2
    count = lax.axis_size("ep")
    rounds = (count - 1).bit_length()
    token_rows, width = tokens.shape
    slots = count * capacity
    units = own[0].shape[1]
    early = width * EARLY // (8 * LANES) * LANES
    late = width - early
    inputs = list(streams) + [
        base.reshape(1, channels),
        shift.T,
        gain.reshape(1, channels),
        out_weight,
        tokens,
        scale.reshape(1, width),
        routes.T,
        weights.T,
    ]
    operands = [in_hbm(array) for array in inputs + list(own)]
    block = (token_rows, width)
    wide, tall = (width, units), (units, width)
    held = [pltpu.VMEM(array.shape, array.dtype) for array in inputs]
    slim = (units, early)
    shapes = (wide, wide, tall) * 2 + (wide, wide, slim) * 2
    shards = [pltpu.VMEM(shape, BF16) for shape in shapes]
    dma = pltpu.SemaphoreType.DMA
    return pl.pallas_call(
        functools.partial(layer_kernel, capacity, head_size, early),
        in_specs=[pl.BlockSpec(memory_space=pl.ANY)] * len(operands),
        out_specs=[pl.BlockSpec(memory_space=pltpu.VMEM)] * 2,
        out_shape=[jax.ShapeDtypeStruct(block, BF16)] * 2,
        scratch_shapes=held
        + shards
        + [
            pltpu.VMEM(shift.shape, F32),
            pltpu.VMEM((rows, channels), BF16),
            pltpu.VMEM((rows, channels), F32),
            pltpu.VMEM((2, pairs * half, LANES), BF16),
            pltpu.VMEM((2 * LANES, LANES), F32),
            pltpu.VMEM((slots, width), BF16),
            pltpu.VMEM((slots, width), BF16),
            pltpu.VMEM((slots, width), F32),
            pltpu.VMEM((slots, 2 * units), BF16),
            pltpu.VMEM((2, pairs, LANES, LANES), F32),
            pltpu.VMEM((2, pairs * half, LANES), BF16),
            pltpu.VMEM((rounds, 2, pairs * half, LANES), BF16),
            pltpu.VMEM((rows, channels), BF16),
            pltpu.VMEM((slots, 2 * units), BF16),
            pltpu.VMEM((slots, late), BF16),
            pltpu.VMEM((slots, late), BF16),
            pltpu.VMEM((slots, early), BF16),
            pltpu.VMEM((slots, late), BF16),
            pltpu.VMEM((slots, early), BF16),
            pltpu.VMEM((slots, late), BF16),
            pltpu.VMEM((rows, width), BF16),
            pltpu.VMEM((2,) + block, BF16),
            pltpu.VMEM(block, BF16),
            pltpu.VMEM(block, BF16),
            pltpu.VMEM(block, F32),
            dma((len(operands) + 1,)),
            dma((count - 1,)),
            dma((count - 1,)),
            dma((2, count - 1)),
            dma((2, count - 1)),
            dma((count,)),
            dma((count,)),
            dma((count // 2,)),
            dma((rounds,)),
            dma((16,)),
            dma((16,)),
        ],
        compiler_params=pltpu.CompilerParams(
            vmem_limit_bytes=52 * 2**20, collective_id=0, has_side_effects=True
        ),
        cost_estimate=pl.CostEstimate(
            flops=40 * 10**9, bytes_accessed=20 * 2**20, transcendentals=2 * 10**6
        ),
        name="whole_layer",
    )(*operands)


def on_device(
    receptance,
    key_rows,
    value_rows,
    decay_input,
    learn_input,
    decay_base,
    decay_shift,
    channel_gain,
    out_weight,
    expert_input,
    expert_gain,
    routes,
    route_weight,
    gate_weight,
    up_weight,
    down_weight,
):
    head_size = receptance.shape[1] // decay_shift.shape[1]
    experts = gate_weight.shape[0] * lax.axis_size("ep")
    capacity = max(2, 2 * expert_input.shape[0] * routes.shape[1] // experts)
    return tuple(
        whole_layer(
            (receptance, key_rows, value_rows, decay_input, learn_input),
            decay_base,
            decay_shift,
            channel_gain,
            out_weight,
            expert_input,
            expert_gain,
            routes,
            route_weight,
            (gate_weight[0], up_weight[0], down_weight[0]),
            head_size,
            capacity,
        )
    )


def solution(mesh):
    return jax.shard_map(
        on_device,
        mesh=mesh,
        in_specs=(
            P("ep", "tp"),
            P("ep", "tp"),
            P("ep", "tp"),
            P("ep", "tp"),
            P("ep", "tp"),
            P("tp"),
            P("ep", "tp"),
            P("tp"),
            P("tp", None),
            P(("ep", "tp"), None),
            P(),
            P(("ep", "tp"), None),
            P(("ep", "tp"), None),
            P("ep", None, "tp"),
            P("ep", None, "tp"),
            P("ep", "tp", None),
        ),
        out_specs=(P(("ep", "tp"), None), P(("ep", "tp"), None)),
        check_vma=False,
    )
```

```python
import functools

import jax
import jax.numpy as jnp
from jax import lax
from jax.experimental import pallas as pl
from jax.experimental.pallas import tpu as pltpu
from jax.sharding import PartitionSpec as P

SPAN = 128
STACK = 2
LANES = 128
EARLY = 6

NORM_EPS = 1e-06
GROUP_EPS = 0.00064
KEY_EPS = 1e-06
F32 = jnp.float32
BF16 = jnp.bfloat16


def mm(a, b):
    return lax.dot_general(
        a.astype(BF16), b.astype(BF16), (((1,), (0,)), ((), ())), preferred_element_type=F32
    )


def mm_nt(a, b):
    return lax.dot_general(
        a.astype(BF16), b.astype(BF16), (((1,), (1,)), ((), ())), preferred_element_type=F32
    )


def mm_tn(a, b):
    return lax.dot_general(
        a.astype(BF16), b.astype(BF16), (((0,), (0,)), ((), ())), preferred_element_type=F32
    )


def split_two(x):
    high = x.astype(BF16)
    return high, (x - high.astype(F32)).astype(BF16)


def grid_index(shape, axis):
    return lax.broadcasted_iota(jnp.int32, shape, axis)


def same_head(head_size):
    rows = grid_index((LANES, LANES), 0) // head_size
    cols = grid_index((LANES, LANES), 1) // head_size
    return rows == cols


def head_sums(x, block):
    high, low = split_two(x)
    return mm(
        jnp.concatenate([high, low], axis=1), jnp.concatenate([block, block], axis=0)
    )


def lower_inverses(strict_parts, rows, cols):
    eye = jnp.where(rows == cols, 1.0, 0.0)
    size = 1
    inverses = None
    while size < SPAN:
        off = (rows // (2 * size) == cols // (2 * size)) & (rows // size != cols // size)
        parts = [jnp.where(off, part, 0.0) for part in strict_parts]
        if inverses is None:
            inverses = [eye - part for part in parts]
        else:
            firsts = [mm(part, inv) for part, inv in zip(parts, inverses)]
            inverses = [inv - mm(inv, first) for inv, first in zip(inverses, firsts)]
        size *= 2
    return inverses


def send_to(src, dst, send_sem, recv_sem, target):
    return pltpu.make_async_remote_copy(
        src_ref=src,
        dst_ref=dst,
        send_sem=send_sem,
        recv_sem=recv_sem,
        device_id=target,
        device_id_type=pl.DeviceIdType.MESH,
    )


def greet_all(barrier, here, count, others):
    def greet(distance, nothing):
        pl.semaphore_signal(
            barrier,
            inc=1,
            device_id={"ep": lax.rem(here + distance, count)},
            device_id_type=pl.DeviceIdType.MESH,
        )
        return nothing

    lax.fori_loop(1, count, greet, 0)
    for target in others:
        pl.semaphore_signal(
            barrier, inc=1, device_id={"tp": target}, device_id_type=pl.DeviceIdType.MESH
        )


def in_hbm(array):
    return pltpu.with_memory_space_constraint(array, pltpu.HBM)


def pack_rows(tokens_ref, scale_ref, routes_ref, outgoing, count, capacity):
    inputs = tokens_ref[...].astype(F32)
    square = jnp.sum(inputs * inputs, axis=1, keepdims=True) * (1.0 / inputs.shape[1])
    normed = (inputs * lax.rsqrt(square + NORM_EPS) * scale_ref[...]).astype(BF16)
    rows = inputs.shape[0]
    members = grid_index((count, rows), 0)
    named = jnp.zeros((count, rows), F32)
    for picked in range(routes_ref.shape[0]):
        named = jnp.where(routes_ref[picked : picked + 1] == members, 1.0, named)
    earlier = grid_index((rows, rows), 0) < grid_index((rows, rows), 1)
    slots = mm(named, earlier.astype(F32))
    slots = jnp.where(named > 0.5, slots, -1.0).astype(jnp.int32)
    wanted = grid_index((capacity, rows), 0)
    group = max(1, min(count, 256 // capacity))
    for begin in range(0, count, group):
        table = jnp.concatenate(
            [
                jnp.where(slots[e : e + 1] == wanted, 1.0, 0.0)
                for e in range(begin, begin + group)
            ],
            axis=0,
        )
        outgoing[begin * capacity : (begin + group) * capacity] = mm(table, normed).astype(BF16)


def scan_pair(
    pair,
    head_size,
    r_ref,
    k_ref,
    v_ref,
    d_ref,
    l_ref,
    base_ref,
    shift_ref,
    reader_ref,
    local_ref,
    summary_ref,
    state,
):
    half = LANES // 2
    lanes = pl.ds(pl.multiple_of(pair * LANES, LANES), LANES)
    spot = pl.ds(pl.multiple_of(pair * half, half), half)

    rows = grid_index((SPAN, SPAN), 0)
    cols = grid_index((SPAN, SPAN), 1)
    strict = rows > cols
    inclusive = rows >= cols
    first = grid_index((SPAN, LANES), 1) < half
    matched = same_head(head_size)
    block = matched.astype(BF16)
    diagonal = grid_index((LANES, LANES), 0) == grid_index((LANES, LANES), 1)
    tri = inclusive.astype(BF16)
    tri_two = jnp.concatenate([tri, tri], axis=1)

    state[:LANES] = jnp.zeros((LANES, LANES), F32)
    state[LANES:] = jnp.where(diagonal, 1.0, 0.0)

    heads = shift_ref.shape[1]
    chosen = grid_index((heads, LANES), 0) == 2 * pair + grid_index((heads, LANES), 1) // half
    def advance(step, nothing):
        start = pl.multiple_of(step * (STACK * SPAN), STACK * SPAN)
        rows_here = pl.ds(start, STACK * SPAN)
        shift = lax.dot_general(
            shift_ref[rows_here],
            chosen.astype(F32),
            (((1,), (0,)), ((), ())),
            precision=lax.Precision.HIGHEST,
            preferred_element_type=F32,
        )
        pre = d_ref[rows_here, lanes].astype(F32) + base_ref[:, lanes] + shift
        log_all = -0.6065306597126334 / (1.0 + jnp.exp(-pre))
        rates = 1.0 / (1.0 + jnp.exp(-l_ref[rows_here, lanes].astype(F32)))
        key_all = k_ref[rows_here, lanes].astype(F32)
        unit_all = key_all * lax.rsqrt(head_sums(key_all * key_all, block) + KEY_EPS)
        removal_all = unit_all * rates

        spans = STACK
        items = []
        strict_parts = []
        for j in range(spans):
            here = slice(j * SPAN, (j + 1) * SPAN)
            log_decay = log_all[here]
            high, low = split_two(log_decay)
            cum = mm(tri_two, jnp.concatenate([high, low], axis=0))
            middle = cum[SPAN // 2 - 1 : SPAN // 2]
            ending = cum[SPAN - 1 :]
            e_cm = jnp.exp(cum - middle)
            e_pm = jnp.exp(cum - log_decay - middle)
            shrink = jnp.exp(middle - cum)
            e_mid = jnp.exp(middle)
            e_tail = jnp.exp(ending - middle)
            unit, key = unit_all[here], key_all[here]
            value = v_ref[pl.ds(start + j * SPAN, SPAN), lanes]
            turned = jnp.concatenate([value[:, half:], value[:, :half]], axis=1)
            recept = r_ref[pl.ds(start + j * SPAN, SPAN), lanes].astype(F32)
            probes = unit * e_pm
            queries = recept * e_cm
            back_removal = removal_all[here] * shrink
            back_keys = key * shrink
            left = jnp.concatenate(
                [
                    jnp.where(first, probes, 0.0),
                    jnp.where(first, 0.0, probes),
                    jnp.where(first, queries, 0.0),
                    jnp.where(first, 0.0, queries),
                ],
                axis=0,
            )
            products = mm_nt(left, jnp.concatenate([back_removal, back_keys], axis=0))
            for h in range(2):
                strict_parts.append(
                    jnp.where(strict, products[h * SPAN : (h + 1) * SPAN, :SPAN], 0.0)
                )
            items.append(
                dict(
                    products=products,
                    turned=turned,
                    carrying=probes * e_mid,
                    reading=queries * e_mid,
                    removal_tail=back_removal * e_tail,
                    key_tail=back_keys * e_tail,
                    fade=jnp.exp(ending),
                )
            )
        inverses = lower_inverses(strict_parts, rows, cols)
        for j in range(spans):
            item = items[j]
            products, turned = item["products"], item["turned"]
            solved, removed, kept = [], [], []
            for h in range(2):
                top = slice(h * SPAN, (h + 1) * SPAN)
                bottom = slice((2 + h) * SPAN, (3 + h) * SPAN)
                pair_keys = jnp.where(strict, products[top, SPAN:], 0.0)
                read_removal = jnp.where(inclusive, products[bottom, :SPAN], 0.0)
                read_keys = jnp.where(inclusive, products[bottom, SPAN:], 0.0)
                both = mm(jnp.concatenate([pair_keys, read_keys], axis=0), turned)
                own = first if h == 0 else jnp.logical_not(first)
                right = jnp.where(own, item["carrying"], both[:SPAN])
                answer = mm(inverses[2 * j + h], right)
                solved.append(answer)
                removed.append(mm(read_removal, answer))
                kept.append(both[SPAN:])
            carried = jnp.where(first, solved[0], solved[1])
            local_turned = jnp.where(first, solved[1], solved[0])
            reader = item["reading"] - jnp.where(first, removed[0], removed[1])
            read_turned = jnp.where(first, kept[1] - removed[1], kept[0] - removed[0])
            local_read = jnp.concatenate([read_turned[:, half:], read_turned[:, :half]], axis=1)
            taken = mm_tn(
                jnp.concatenate([carried, local_turned], axis=1), item["removal_tail"]
            )
            offset_turned = mm_tn(turned, item["key_tail"]) - taken[LANES:]
            offset = jnp.concatenate([offset_turned[half:], offset_turned[:half]], axis=0)
            offset = jnp.where(matched, offset, 0.0)
            transition = jnp.where(diagonal, item["fade"], 0.0) - jnp.where(
                matched, taken[:LANES], 0.0
            )
            now = state[...]
            reads = mm_nt(reader, now)
            here = pl.ds(start + j * SPAN, SPAN)
            local_ref[here, lanes] = local_read + reads[:, :LANES]
            reader_ref[pl.ds(start + j * SPAN, SPAN), lanes] = reads[:, LANES:].astype(BF16)
            now_high, now_low = split_two(now)
            step_high, step_low = split_two(transition)
            moved = mm(now_high, step_high) + mm(now_low, step_high) + mm(now_high, step_low)
            state[:LANES] = moved[:LANES] + offset
            state[LANES:] = moved[LANES:]
        return nothing

    lax.fori_loop(0, r_ref.shape[0] // (STACK * SPAN), advance, 0)
    summary_ref[1, spot] = (state[:half] + state[half:LANES]).astype(BF16)
    summary_ref[0, spot] = (state[LANES : LANES + half] + state[LANES + half :]).astype(BF16)


def gated(x, gate, up):
    gates = mm(x, gate)
    uppers = mm(x, up)
    return (gates / (1.0 + jnp.exp(-gates)) * uppers).astype(BF16)


def layer_kernel(capacity, head_size, early, *refs):
    (
        r_hbm,
        k_hbm,
        v_hbm,
        d_hbm,
        l_hbm,
        base_hbm,
        shift_hbm,
        gain_hbm,
        project_hbm,
        tokens_hbm,
        scale_hbm,
        routes_hbm,
        weight_hbm,
        gate_hbm,
        up_hbm,
        down_hbm,
        mixer_ref,
        expert_ref,
        r_ref,
        k_ref,
        v_ref,
        d_ref,
        l_ref,
        base_ref,
        shift_in,
        gain_ref,
        project,
        tokens_ref,
        scale_ref,
        routes_ref,
        weight_ref,
        own_gate,
        own_up,
        own_down,
        near_gate,
        near_up,
        near_down,
        far_gate,
        far_up,
        far_down,
        cross_gate,
        cross_up,
        cross_down,
        shift_ref,
        reader,
        local,
        summary,
        state,
        outgoing,
        x_ref,
        total,
        hidden_ref,
        before,
        sending,
        passed,
        mixed,
        far_rest_a,
        far_rest_b,
        cross_rest_a,
        cross_rest_b,
        theirs,
        part_out,
        part_in,
        staged_early,
        staged_late,
        landed_early,
        landed_late,
        term,
        near_in,
        pair_out,
        far_in,
        combined,
        load_sems,
        post_send,
        post_recv,
        back_send,
        back_recv,
        part_send,
        part_recv,
        round_send,
        round_recv,
        side_send,
        side_recv,
    ) = refs
    here = lax.axis_index("ep")
    count = lax.axis_size("ep")
    place = lax.axis_index("tp")
    low, high = lax.rem(place, 2), place // 2
    beside = place + 1 - 2 * low
    across = place + 2 - 4 * high
    reach_half = count // 2
    local_index, own_half = lax.rem(here, reach_half), here // reach_half
    rounds = passed.shape[0]
    half = LANES // 2
    pairs = before.shape[1]
    rows = x_ref.shape[0]
    units = own_gate.shape[1]
    tokens = expert_ref.shape[0]
    matched = same_head(head_size)
    block = matched.astype(BF16)
    diagonal = grid_index((LANES, LANES), 0) == grid_index((LANES, LANES), 1)

    pieces = [
        (tokens_hbm, tokens_ref),
        (scale_hbm, scale_ref),
        (routes_hbm, routes_ref),
        (weight_hbm, weight_ref),
        (base_hbm, base_ref),
        (shift_hbm, shift_in),
        (gain_hbm, gain_ref),
        (r_hbm, r_ref),
        (k_hbm, k_ref),
        (v_hbm, v_ref),
        (d_hbm, d_ref),
        (l_hbm, l_ref),
        (gate_hbm, own_gate),
        (up_hbm, own_up),
        (down_hbm, own_down),
        (project_hbm, project),
    ]
    loads = [
        pltpu.make_async_copy(src, dst, load_sems.at[i]) for i, (src, dst) in enumerate(pieces)
    ]
    keep_sem = load_sems.at[len(pieces)]
    barrier = pltpu.get_barrier_semaphore()
    greet_all(barrier, here, count, (beside, across))
    for load in loads:
        load.start()

    def side(src, dst, index, target):
        return send_to(src, dst, side_send.at[index], side_recv.at[index], {"tp": target})

    def rows_of(member):
        return pl.ds(pl.multiple_of(member * capacity, capacity), capacity)

    def partner(k, sign):
        crossing, shift = (k + 1) // reach_half, lax.rem(k + 1, reach_half)
        member = lax.rem(local_index + reach_half + sign * shift, reach_half)
        return member + reach_half * (own_half + crossing * (1 - 2 * own_half))

    def crossing_step(j):
        quarter = reach_half // 2
        side_of = (1 - own_half) + (j // quarter) * (2 * own_half - 1)
        index = side_of * quarter + lax.rem(local_index + j, quarter)
        shift = lax.rem(index - local_index + reach_half, reach_half)
        return reach_half - 1 + shift, (1 - own_half) * reach_half + index

    def post(k, member):
        return send_to(
            outgoing.at[rows_of(member)],
            x_ref.at[rows_of(here)],
            post_send.at[k],
            post_recv.at[k],
            {"ep": member},
        )

    def back(k, member, late):
        staged, landed = (staged_late, landed_late) if late else (staged_early, landed_early)
        return send_to(
            staged.at[rows_of(member)],
            landed.at[rows_of(here)],
            back_send.at[late, k],
            back_recv.at[late, k],
            {"ep": member},
        )

    far_rest = (far_rest_a, far_rest_b)
    cross_rest = (cross_rest_a, cross_rest_b)
    middle = far_rest_a.shape[1]
    spans = ((0, middle), (middle, middle + far_rest_b.shape[1]))

    def back_piece(k, member, i):
        columns = slice(*spans[i])
        return send_to(
            staged_late.at[rows_of(member), columns],
            landed_late.at[rows_of(here), columns],
            back_send.at[1 + i, k],
            back_recv.at[1 + i, k],
            {"ep": member},
        )

    def part(member):
        return send_to(
            part_out.at[rows_of(member)],
            part_in.at[rows_of(member)],
            part_send.at[member],
            part_recv.at[member],
            {"tp": across},
        )

    def at_half(which):
        return pl.ds(pl.multiple_of(which * (rows // 2), rows // 2), rows // 2)

    crossing_rows = at_half(1 - own_half)
    ask = side(hidden_ref.at[crossing_rows], theirs.at[crossing_rows], 14, across)

    cut = units // 2
    fars = [side(gate_hbm, far_gate, 0, across), side(up_hbm, far_up, 1, across)] + [
        side(
            down_hbm.at[i * cut : (i + 1) * cut, :early],
            far_down.at[i * cut : (i + 1) * cut],
            2 + i,
            across,
        )
        for i in range(2)
    ]
    nears = [
        side(gate_hbm, near_gate, 4, beside),
        side(up_hbm, near_up, 5, beside),
        side(down_hbm, near_down, 6, beside),
    ]
    forwards = [side(far_gate, cross_gate, 7, beside), side(far_up, cross_up, 8, beside)] + [
        side(
            far_down.at[i * cut : (i + 1) * cut], cross_down.at[i * cut : (i + 1) * cut], 9 + i, beside
        )
        for i in range(2)
    ]

    rests = [
        side(down_hbm.at[:, early + first : early + last], far_rest[i], 15 + i, across)
        for i, (first, last) in enumerate(spans)
    ]
    onward = [side(far_rest[i], cross_rest[i], 17 + i, beside) for i in range(2)]

    pl.semaphore_wait(barrier, count + 1)
    for copy in fars + nears:
        copy.start()
    for load in loads[:3]:
        load.wait()
    pack_rows(tokens_ref, scale_ref, routes_ref, outgoing, count, capacity)

    def launch_post(k, nothing):
        post(k, partner(k, 1)).start()
        return nothing

    def launch_crossing(j, nothing):
        post(*crossing_step(j)).start()
        return nothing

    lax.fori_loop(0, reach_half - 1, launch_post, 0)
    lax.fori_loop(0, reach_half, launch_crossing, 0)
    keep = pltpu.make_async_copy(outgoing.at[rows_of(here)], x_ref.at[rows_of(here)], keep_sem)
    keep.start()

    for load in loads[3:12]:
        load.wait()
    shift_ref[...] = shift_in[...].T

    def scan(p, nothing):
        scan_pair(
            p,
            head_size,
            r_ref,
            k_ref,
            v_ref,
            d_ref,
            l_ref,
            base_ref,
            shift_ref,
            reader,
            local,
            summary,
            state,
        )
        return nothing

    lax.fori_loop(0, pairs, scan, 0)

    def transfer(level, distance, target):
        return send_to(
            sending,
            passed.at[level],
            round_send.at[distance - 1],
            round_recv.at[level],
            {"ep": target},
        )

    def transfer_state(level, distance, target):
        return send_to(
            sending.at[1],
            passed.at[level, 1],
            round_send.at[distance - 1],
            round_recv.at[level],
            {"ep": target},
        )

    def sends_all(reach):
        return (lax.rem(here, 2 * reach) == reach - 1) & (here >= 2 * reach)

    def wide(part):
        part = part.astype(F32)
        return jnp.where(matched, jnp.concatenate([part, part], axis=0), 0.0)

    def spot(p):
        return slice(p * half, (p + 1) * half)

    for p in range(pairs):
        before[0, p] = jnp.where(diagonal, 1.0, 0.0)
        before[1, p] = jnp.zeros((LANES, LANES), F32)

    def send_round(level):
        reach = 2**level

        @pl.when(lax.rem(here, 2 * reach) == reach - 1)
        def _():
            for p in range(pairs):
                both = jnp.concatenate([before[0, p], before[1, p]], axis=0)
                upper, lower = split_two(both)
                step = wide(summary[0, spot(p)])
                moved = mm(upper, step) + mm(lower, step)
                after = moved[LANES:] + wide(summary[1, spot(p)])
                sending[0, spot(p)] = (moved[:half] + moved[half:LANES]).astype(BF16)
                sending[1, spot(p)] = (after[:half] + after[half:]).astype(BF16)

        def launch_with(transfer):
            def launch(distance, nothing):
                transfer(level, distance, here + distance).start()
                return nothing

            lax.fori_loop(1, reach + 1, launch, 0)

        pl.when(sends_all(reach))(lambda: launch_with(transfer))
        pl.when(here == reach - 1)(lambda: launch_with(transfer_state))

    def take_round(level):
        reach = 2**level

        @pl.when((lax.rem(here // reach, 2) == 1) & (here >= 2 * reach))
        def _():
            transfer(level, 1, here).wait_recv()
            for p in range(pairs):
                both = jnp.concatenate(
                    [wide(passed[level, 0, spot(p)]), wide(passed[level, 1, spot(p)])], axis=0
                )
                upper, lower = split_two(before[0, p])
                moved = mm(both, upper) + mm(both, lower)
                before[0, p] = moved[:LANES]
                before[1, p] = moved[LANES:] + before[1, p]

        @pl.when((here >= reach) & (here < 2 * reach))
        def _():
            transfer_state(level, 1, here).wait_recv()
            for p in range(pairs):
                entering = wide(passed[level, 1, spot(p)])
                upper, lower = split_two(before[0, p])
                before[1, p] = mm(entering, upper) + mm(entering, lower) + before[1, p]

    def settle_with(transfer, level, reach):
        def settle(distance, nothing):
            transfer(level, distance, here + distance).wait_send()
            return nothing

        lax.fori_loop(1, reach + 1, settle, 0)

    def full_parts(at):
        x = x_ref[at]
        total[at] = mm(gated(x, own_gate[...], own_up[...]), own_down[...])
        total[at] += mm(gated(x, near_gate[...], near_up[...]), near_down[...])

    def far_parts(at):
        x = x_ref[at]
        hidden_ref[at, :units] = gated(x, far_gate[...], far_up[...])
        hidden_ref[at, units:] = gated(x, cross_gate[...], cross_up[...])

    def take_post(k, nothing):
        post(k, partner(k, -1)).wait_recv()
        return nothing

    send_round(0)
    for load in loads[12:15]:
        load.wait()
    keep.wait()
    for copy in nears:
        copy.wait_recv()
    lax.fori_loop(0, reach_half - 1, take_post, 0)
    full_parts(at_half(own_half))
    fars[0].wait_recv()
    forwards[0].start()
    take_round(0)
    if rounds > 1:
        send_round(1)
    fars[1].wait_recv()
    forwards[1].start()
    lax.fori_loop(reach_half - 1, count - 1, take_post, 0)
    full_parts(at_half(1 - own_half))
    for copy in forwards[:2]:
        copy.wait_recv()

    far_parts(crossing_rows)
    ask.start()
    far_parts(at_half(own_half))
    for level in range(1, min(rounds, 2)):
        take_round(level)
        if level + 1 < rounds:
            send_round(level + 1)

    for i in range(2):
        fars[2 + i].wait_recv()
        forwards[2 + i].start()
    for copy in forwards[2:]:
        copy.wait_recv()

    def finished(member):
        at = rows_of(member)
        hidden = hidden_ref[at]
        row = total[at, :early] + mm(hidden[:, :units], far_down[...])
        return (row + mm(hidden[:, units:], cross_down[...])).astype(BF16)

    def send_early(k, member):
        staged_early[rows_of(member)] = finished(member)
        back(k, member, 0).start()

    def send_back(j, nothing):
        send_early(*crossing_step(j))
        return nothing

    def send_back_near(k, nothing):
        send_early(k, partner(k, 1))
        return nothing

    lax.fori_loop(0, reach_half, send_back, 0)
    lax.fori_loop(0, reach_half - 1, send_back_near, 0)
    landed_early[rows_of(here)] = finished(here)

    ask.wait_recv()
    asked = theirs[crossing_rows]
    product = mm(asked[:, :units], own_down[:, early:])
    product += mm(asked[:, units:], near_down[:, early:])
    part_out[crossing_rows] = product.astype(BF16)

    def launch_part(j, nothing):
        part(crossing_step(j)[1]).start()
        return nothing

    lax.fori_loop(0, reach_half, launch_part, 0)
    for copy in rests:
        copy.start()
    def send_crossing(j, nothing):
        k, member = crossing_step(j)
        part(member).wait_recv()
        at = rows_of(member)
        staged_late[at] = (total[at, early:] + part_in[at].astype(F32)).astype(BF16)
        back(k, member, 1).start()
        return nothing

    lax.fori_loop(0, reach_half, send_crossing, 0)

    for level in range(2, rounds):
        take_round(level)
        if level + 1 < rounds:
            send_round(level + 1)
    loads[15].wait()
    for p in range(pairs):
        lanes = slice(p * LANES, (p + 1) * LANES)
        read = mm_nt(reader[:, lanes], before[1, p]) + local[:, lanes]
        centred = read - head_sums(read, block) * (1.0 / head_size)
        variance = head_sums(centred * centred, block) * (1.0 / head_size)
        scaled = centred * lax.rsqrt(variance + GROUP_EPS) * gain_ref[:, lanes]
        mixed[:, lanes] = scaled.astype(BF16)

    def block_rows(b):
        return pl.ds(pl.multiple_of(b * tokens, tokens), tokens)

    def project_block(b, nothing):
        at = block_rows(b)
        term[at] = mm(mixed[at], project[...]).astype(BF16)
        return nothing

    lax.fori_loop(0, 4, project_block, 0)
    sums = [
        side(term.at[block_rows(2 * y + 1 - low)], near_in.at[y], 11 + y, beside)
        for y in range(2)
    ]
    for copy in sums:
        copy.start()

    picks = routes_ref.shape[0]
    packed = jnp.concatenate(
        [routes_ref[...].astype(F32), weight_ref[...], jnp.zeros((8 - 2 * picks, tokens), F32)],
        axis=0,
    ).T
    lane = grid_index((tokens, LANES), 1)
    routes = [packed[:, i : i + 1].astype(jnp.int32) for i in range(picks)]
    weight = packed[:, picks : 2 * picks]
    named = jnp.zeros((tokens, LANES), F32)
    for route in routes:
        named = jnp.where(route == lane, 1.0, named)
    earlier = grid_index((tokens, tokens), 0) > grid_index((tokens, tokens), 1)
    slots = mm(earlier.astype(F32), named)
    target = jnp.concatenate(
        [
            route * capacity
            + jnp.sum(jnp.where(route == lane, slots, 0.0), axis=1, keepdims=True).astype(
                jnp.int32
            )
            for route in routes
        ],
        axis=1,
    )
    slot = grid_index((tokens, capacity), 1)

    def taken(member, late):
        table = jnp.zeros((tokens, capacity), F32)
        scale = jnp.zeros((tokens, 1), F32)
        for picked in range(target.shape[1]):
            own = target[:, picked : picked + 1] - member * capacity
            table = jnp.where(own == slot, 1.0, table)
            inside = (own >= 0) & (own < capacity)
            scale = jnp.where(inside, weight[:, picked : picked + 1], scale)
        landed = landed_late if late else landed_early
        return mm(table, landed[rows_of(member)]) * scale

    combined[:, :early] = taken(here, 0)

    for copy in sums:
        copy.wait_recv()
    other = 1 - high
    pair_out[...] = (
        term[block_rows(2 * other + low)].astype(F32) + near_in[other].astype(F32)
    ).astype(BF16)
    last_sum = side(pair_out, far_in, 13, across)
    last_sum.start()

    def late_rows(member, i):
        at = rows_of(member)
        hidden = hidden_ref[at]
        first, last = spans[i]
        row = total[at, early + first : early + last]
        row += mm(hidden[:, :units], far_rest[i][...])
        return (row + mm(hidden[:, units:], cross_rest[i][...])).astype(BF16)

    def send_near(i):
        columns = slice(*spans[i])
        rests[i].wait_recv()
        onward[i].start()
        onward[i].wait_recv()

        def send_piece(k, nothing):
            member = partner(k, 1)
            staged_late[rows_of(member), columns] = late_rows(member, i)
            back_piece(k, member, i).start()
            return nothing

        lax.fori_loop(0, reach_half - 1, send_piece, 0)
        landed_late[rows_of(here), columns] = late_rows(here, i)

    def gather_early(k, nothing):
        member = partner(k, -1)
        back(k, member, 0).wait_recv()
        combined[:, :early] += taken(member, 0)
        return nothing

    def gather_near(k, nothing):
        member = partner(k, -1)
        for i in range(2):
            back_piece(k, member, i).wait_recv()
        combined[:, early:] += taken(member, 1)
        return nothing

    def gather_late(k, nothing):
        member = partner(k, -1)
        back(k, member, 1).wait_recv()
        combined[:, early:] += taken(member, 1)
        return nothing

    lax.fori_loop(0, reach_half - 1, gather_early, 0)
    for i in range(2):
        send_near(i)
    combined[:, early:] = taken(here, 1)
    lax.fori_loop(reach_half - 1, count - 1, gather_early, 0)
    lax.fori_loop(0, reach_half - 1, gather_near, 0)
    lax.fori_loop(reach_half - 1, count - 1, gather_late, 0)
    expert_ref[...] = combined[...].astype(BF16)
    last_sum.wait_recv()
    kept = term[block_rows(2 * high + low)].astype(F32) + near_in[high].astype(F32)
    mixer_ref[...] = (kept + far_in[...].astype(F32)).astype(BF16)

    def settle_rows(k, nothing):
        post(k, partner(k, 1)).wait_send()
        back(k, partner(k, 1), 0).wait_send()
        return nothing

    def settle_near(k, nothing):
        for i in range(2):
            back_piece(k, partner(k, 1), i).wait_send()
        return nothing

    def settle_crossing(k, nothing):
        back(k, partner(k, 1), 1).wait_send()
        return nothing

    def settle_part(j, nothing):
        part(crossing_step(j)[1]).wait_send()
        return nothing

    lax.fori_loop(0, count - 1, settle_rows, 0)
    lax.fori_loop(0, reach_half - 1, settle_near, 0)
    lax.fori_loop(reach_half - 1, count - 1, settle_crossing, 0)
    lax.fori_loop(0, reach_half, settle_part, 0)
    for level in range(rounds):
        reach = 2**level
        pl.when(sends_all(reach))(functools.partial(settle_with, transfer, level, reach))
        pl.when(here == reach - 1)(
            functools.partial(settle_with, transfer_state, level, reach)
        )
    for copy in fars + nears + forwards + [ask] + rests + onward + sums + [last_sum]:
        copy.wait_send()


def whole_layer(streams, base, shift, gain, out_weight, tokens, scale, routes, weights, own, head_size, capacity):
    rows, channels = streams[0].shape
    pairs = channels // LANES
    half = LANES // 2
    count = lax.axis_size("ep")
    rounds = (count - 1).bit_length()
    token_rows, width = tokens.shape
    slots = count * capacity
    units = own[0].shape[1]
    early = width * EARLY // (16 * LANES) * LANES
    late = width - early
    late_end = late // (2 * LANES) * LANES
    inputs = list(streams) + [
        base.reshape(1, channels),
        shift.T,
        gain.reshape(1, channels),
        out_weight,
        tokens,
        scale.reshape(1, width),
        routes.T,
        weights.T,
    ]
    operands = [in_hbm(array) for array in inputs + list(own)]
    block = (token_rows, width)
    wide, tall = (width, units), (units, width)
    held = [pltpu.VMEM(array.shape, array.dtype) for array in inputs]
    slim = (units, early)
    shapes = (wide, wide, tall) * 2 + (wide, wide, slim) * 2
    shards = [pltpu.VMEM(shape, BF16) for shape in shapes]
    dma = pltpu.SemaphoreType.DMA
    return pl.pallas_call(
        functools.partial(layer_kernel, capacity, head_size, early),
        in_specs=[pl.BlockSpec(memory_space=pl.ANY)] * len(operands),
        out_specs=[pl.BlockSpec(memory_space=pltpu.VMEM)] * 2,
        out_shape=[jax.ShapeDtypeStruct(block, BF16)] * 2,
        scratch_shapes=held
        + shards
        + [
            pltpu.VMEM(shift.shape, F32),
            pltpu.VMEM((rows, channels), BF16),
            pltpu.VMEM((rows, channels), F32),
            pltpu.VMEM((2, pairs * half, LANES), BF16),
            pltpu.VMEM((2 * LANES, LANES), F32),
            pltpu.VMEM((slots, width), BF16),
            pltpu.VMEM((slots, width), BF16),
            pltpu.VMEM((slots, width), F32),
            pltpu.VMEM((slots, 2 * units), BF16),
            pltpu.VMEM((2, pairs, LANES, LANES), F32),
            pltpu.VMEM((2, pairs * half, LANES), BF16),
            pltpu.VMEM((rounds, 2, pairs * half, LANES), BF16),
            pltpu.VMEM((rows, channels), BF16),
            pltpu.VMEM((units, late - late_end), BF16),
            pltpu.VMEM((units, late_end), BF16),
            pltpu.VMEM((units, late - late_end), BF16),
            pltpu.VMEM((units, late_end), BF16),
            pltpu.VMEM((slots, 2 * units), BF16),
            pltpu.VMEM((slots, late), BF16),
            pltpu.VMEM((slots, late), BF16),
            pltpu.VMEM((slots, early), BF16),
            pltpu.VMEM((slots, late), BF16),
            pltpu.VMEM((slots, early), BF16),
            pltpu.VMEM((slots, late), BF16),
            pltpu.VMEM((rows, width), BF16),
            pltpu.VMEM((2,) + block, BF16),
            pltpu.VMEM(block, BF16),
            pltpu.VMEM(block, BF16),
            pltpu.VMEM(block, F32),
            dma((len(operands) + 1,)),
            dma((count - 1,)),
            dma((count - 1,)),
            dma((3, count - 1)),
            dma((3, count - 1)),
            dma((count,)),
            dma((count,)),
            dma((count // 2,)),
            dma((rounds,)),
            dma((19,)),
            dma((19,)),
        ],
        compiler_params=pltpu.CompilerParams(
            vmem_limit_bytes=52 * 2**20, collective_id=0, has_side_effects=True
        ),
        cost_estimate=pl.CostEstimate(
            flops=40 * 10**9, bytes_accessed=20 * 2**20, transcendentals=2 * 10**6
        ),
        name="whole_layer",
    )(*operands)


def output_kernel(mixer_ref, expert_ref, mixer_out, expert_out, sems):
    copies = [
        pltpu.make_async_copy(mixer_ref, mixer_out, sems.at[0]),
        pltpu.make_async_copy(expert_ref, expert_out, sems.at[1]),
    ]
    for copy in copies:
        copy.start()
    for copy in copies:
        copy.wait()


def write_outputs(mixer, expert):
    return pl.pallas_call(
        output_kernel,
        in_specs=[pl.BlockSpec(memory_space=pltpu.VMEM)] * 2,
        out_specs=[pl.BlockSpec(memory_space=pl.ANY)] * 2,
        out_shape=[
            jax.ShapeDtypeStruct(mixer.shape, BF16),
            jax.ShapeDtypeStruct(expert.shape, BF16),
        ],
        scratch_shapes=[pltpu.SemaphoreType.DMA((2,))],
        compiler_params=pltpu.CompilerParams(vmem_limit_bytes=4 * 2**20),
        name="write_outputs",
    )(mixer, expert)


def on_device(
    receptance,
    key_rows,
    value_rows,
    decay_input,
    learn_input,
    decay_base,
    decay_shift,
    channel_gain,
    out_weight,
    expert_input,
    expert_gain,
    routes,
    route_weight,
    gate_weight,
    up_weight,
    down_weight,
):
    head_size = receptance.shape[1] // decay_shift.shape[1]
    experts = gate_weight.shape[0] * lax.axis_size("ep")
    capacity = max(2, 2 * expert_input.shape[0] * routes.shape[1] // experts)
    return tuple(
        write_outputs(
            *whole_layer(
                (receptance, key_rows, value_rows, decay_input, learn_input),
                decay_base,
                decay_shift,
                channel_gain,
                out_weight,
                expert_input,
                expert_gain,
                routes,
                route_weight,
                (gate_weight[0], up_weight[0], down_weight[0]),
                head_size,
                capacity,
            )
        )
    )


def solution(mesh):
    return jax.shard_map(
        on_device,
        mesh=mesh,
        in_specs=(
            P("ep", "tp"),
            P("ep", "tp"),
            P("ep", "tp"),
            P("ep", "tp"),
            P("ep", "tp"),
            P("tp"),
            P("ep", "tp"),
            P("tp"),
            P("tp", None),
            P(("ep", "tp"), None),
            P(),
            P(("ep", "tp"), None),
            P(("ep", "tp"), None),
            P("ep", None, "tp"),
            P("ep", None, "tp"),
            P("ep", "tp", None),
        ),
        out_specs=(P(("ep", "tp"), None), P(("ep", "tp"), None)),
        check_vma=False,
    )
```

```python
import functools

import jax
import jax.numpy as jnp
from jax import lax
from jax.experimental import pallas as pl
from jax.experimental.pallas import tpu as pltpu
from jax.sharding import PartitionSpec as P

SPAN = 128
STACK = 2
LANES = 128
EARLY = 6

NORM_EPS = 1e-06
GROUP_EPS = 0.00064
KEY_EPS = 1e-06
F32 = jnp.float32
BF16 = jnp.bfloat16


def mm(a, b):
    return lax.dot_general(
        a.astype(BF16), b.astype(BF16), (((1,), (0,)), ((), ())), preferred_element_type=F32
    )


def mm_nt(a, b):
    return lax.dot_general(
        a.astype(BF16), b.astype(BF16), (((1,), (1,)), ((), ())), preferred_element_type=F32
    )


def mm_tn(a, b):
    return lax.dot_general(
        a.astype(BF16), b.astype(BF16), (((0,), (0,)), ((), ())), preferred_element_type=F32
    )


def split_two(x):
    high = x.astype(BF16)
    return high, (x - high.astype(F32)).astype(BF16)


def grid_index(shape, axis):
    return lax.broadcasted_iota(jnp.int32, shape, axis)


def same_head(head_size):
    rows = grid_index((LANES, LANES), 0) // head_size
    cols = grid_index((LANES, LANES), 1) // head_size
    return rows == cols


def head_sums(x, block):
    high, low = split_two(x)
    return mm(
        jnp.concatenate([high, low], axis=1), jnp.concatenate([block, block], axis=0)
    )


def lower_inverses(strict_parts, rows, cols):
    eye = jnp.where(rows == cols, 1.0, 0.0)
    size = 1
    inverses = None
    while size < SPAN:
        off = (rows // (2 * size) == cols // (2 * size)) & (rows // size != cols // size)
        parts = [jnp.where(off, part, 0.0) for part in strict_parts]
        if inverses is None:
            inverses = [eye - part for part in parts]
        else:
            firsts = [mm(part, inv) for part, inv in zip(parts, inverses)]
            inverses = [inv - mm(inv, first) for inv, first in zip(inverses, firsts)]
        size *= 2
    return inverses


def send_to(src, dst, send_sem, recv_sem, target):
    return pltpu.make_async_remote_copy(
        src_ref=src,
        dst_ref=dst,
        send_sem=send_sem,
        recv_sem=recv_sem,
        device_id=target,
        device_id_type=pl.DeviceIdType.MESH,
    )


def greet_all(barrier, here, count, others):
    def greet(distance, nothing):
        pl.semaphore_signal(
            barrier,
            inc=1,
            device_id={"ep": lax.rem(here + distance, count)},
            device_id_type=pl.DeviceIdType.MESH,
        )
        return nothing

    lax.fori_loop(1, count, greet, 0)
    for target in others:
        pl.semaphore_signal(
            barrier, inc=1, device_id={"tp": target}, device_id_type=pl.DeviceIdType.MESH
        )


def in_hbm(array):
    return pltpu.with_memory_space_constraint(array, pltpu.HBM)


def pack_rows(tokens_ref, scale_ref, routes_ref, outgoing, count, capacity):
    inputs = tokens_ref[...].astype(F32)
    square = jnp.sum(inputs * inputs, axis=1, keepdims=True) * (1.0 / inputs.shape[1])
    normed = (inputs * lax.rsqrt(square + NORM_EPS) * scale_ref[...]).astype(BF16)
    rows = inputs.shape[0]
    members = grid_index((count, rows), 0)
    named = jnp.zeros((count, rows), F32)
    for picked in range(routes_ref.shape[0]):
        named = jnp.where(routes_ref[picked : picked + 1] == members, 1.0, named)
    earlier = grid_index((rows, rows), 0) < grid_index((rows, rows), 1)
    slots = mm(named, earlier.astype(F32))
    slots = jnp.where(named > 0.5, slots, -1.0).astype(jnp.int32)
    wanted = grid_index((capacity, rows), 0)
    group = max(1, min(count, 256 // capacity))
    for begin in range(0, count, group):
        table = jnp.concatenate(
            [
                jnp.where(slots[e : e + 1] == wanted, 1.0, 0.0)
                for e in range(begin, begin + group)
            ],
            axis=0,
        )
        outgoing[begin * capacity : (begin + group) * capacity] = mm(table, normed).astype(BF16)


def scan_pair(
    pair,
    head_size,
    r_ref,
    k_ref,
    v_ref,
    d_ref,
    l_ref,
    base_ref,
    shift_ref,
    reader_ref,
    local_ref,
    summary_ref,
    state,
):
    half = LANES // 2
    lanes = pl.ds(pl.multiple_of(pair * LANES, LANES), LANES)
    spot = pl.ds(pl.multiple_of(pair * half, half), half)

    rows = grid_index((SPAN, SPAN), 0)
    cols = grid_index((SPAN, SPAN), 1)
    strict = rows > cols
    inclusive = rows >= cols
    first = grid_index((SPAN, LANES), 1) < half
    matched = same_head(head_size)
    block = matched.astype(BF16)
    diagonal = grid_index((LANES, LANES), 0) == grid_index((LANES, LANES), 1)
    tri = inclusive.astype(BF16)
    tri_two = jnp.concatenate([tri, tri], axis=1)

    state[:LANES] = jnp.zeros((LANES, LANES), F32)
    state[LANES:] = jnp.where(diagonal, 1.0, 0.0)

    heads = shift_ref.shape[1]
    chosen = grid_index((heads, LANES), 0) == 2 * pair + grid_index((heads, LANES), 1) // half
    def advance(step, nothing):
        start = pl.multiple_of(step * (STACK * SPAN), STACK * SPAN)
        rows_here = pl.ds(start, STACK * SPAN)
        shift = lax.dot_general(
            shift_ref[rows_here],
            chosen.astype(F32),
            (((1,), (0,)), ((), ())),
            precision=lax.Precision.HIGHEST,
            preferred_element_type=F32,
        )
        pre = d_ref[rows_here, lanes].astype(F32) + base_ref[:, lanes] + shift
        log_all = -0.6065306597126334 / (1.0 + jnp.exp(-pre))
        rates = 1.0 / (1.0 + jnp.exp(-l_ref[rows_here, lanes].astype(F32)))
        key_all = k_ref[rows_here, lanes].astype(F32)
        unit_all = key_all * lax.rsqrt(head_sums(key_all * key_all, block) + KEY_EPS)
        removal_all = unit_all * rates

        spans = STACK
        items = []
        strict_parts = []
        for j in range(spans):
            here = slice(j * SPAN, (j + 1) * SPAN)
            log_decay = log_all[here]
            high, low = split_two(log_decay)
            cum = mm(tri_two, jnp.concatenate([high, low], axis=0))
            middle = cum[SPAN // 2 - 1 : SPAN // 2]
            ending = cum[SPAN - 1 :]
            e_cm = jnp.exp(cum - middle)
            e_pm = jnp.exp(cum - log_decay - middle)
            shrink = jnp.exp(middle - cum)
            e_mid = jnp.exp(middle)
            e_tail = jnp.exp(ending - middle)
            unit, key = unit_all[here], key_all[here]
            value = v_ref[pl.ds(start + j * SPAN, SPAN), lanes]
            turned = jnp.concatenate([value[:, half:], value[:, :half]], axis=1)
            recept = r_ref[pl.ds(start + j * SPAN, SPAN), lanes].astype(F32)
            probes = unit * e_pm
            queries = recept * e_cm
            back_removal = removal_all[here] * shrink
            back_keys = key * shrink
            left = jnp.concatenate(
                [
                    jnp.where(first, probes, 0.0),
                    jnp.where(first, 0.0, probes),
                    jnp.where(first, queries, 0.0),
                    jnp.where(first, 0.0, queries),
                ],
                axis=0,
            )
            products = mm_nt(left, jnp.concatenate([back_removal, back_keys], axis=0))
            for h in range(2):
                strict_parts.append(
                    jnp.where(strict, products[h * SPAN : (h + 1) * SPAN, :SPAN], 0.0)
                )
            items.append(
                dict(
                    products=products,
                    turned=turned,
                    carrying=probes * e_mid,
                    reading=queries * e_mid,
                    removal_tail=back_removal * e_tail,
                    key_tail=back_keys * e_tail,
                    fade=jnp.exp(ending),
                )
            )
        inverses = lower_inverses(strict_parts, rows, cols)
        for j in range(spans):
            item = items[j]
            products, turned = item["products"], item["turned"]
            solved, removed, kept = [], [], []
            for h in range(2):
                top = slice(h * SPAN, (h + 1) * SPAN)
                bottom = slice((2 + h) * SPAN, (3 + h) * SPAN)
                pair_keys = jnp.where(strict, products[top, SPAN:], 0.0)
                read_removal = jnp.where(inclusive, products[bottom, :SPAN], 0.0)
                read_keys = jnp.where(inclusive, products[bottom, SPAN:], 0.0)
                both = mm(jnp.concatenate([pair_keys, read_keys], axis=0), turned)
                own = first if h == 0 else jnp.logical_not(first)
                right = jnp.where(own, item["carrying"], both[:SPAN])
                answer = mm(inverses[2 * j + h], right)
                solved.append(answer)
                removed.append(mm(read_removal, answer))
                kept.append(both[SPAN:])
            carried = jnp.where(first, solved[0], solved[1])
            local_turned = jnp.where(first, solved[1], solved[0])
            reader = item["reading"] - jnp.where(first, removed[0], removed[1])
            read_turned = jnp.where(first, kept[1] - removed[1], kept[0] - removed[0])
            local_read = jnp.concatenate([read_turned[:, half:], read_turned[:, :half]], axis=1)
            taken = mm_tn(
                jnp.concatenate([carried, local_turned], axis=1), item["removal_tail"]
            )
            offset_turned = mm_tn(turned, item["key_tail"]) - taken[LANES:]
            offset = jnp.concatenate([offset_turned[half:], offset_turned[:half]], axis=0)
            offset = jnp.where(matched, offset, 0.0)
            transition = jnp.where(diagonal, item["fade"], 0.0) - jnp.where(
                matched, taken[:LANES], 0.0
            )
            now = state[...]
            reads = mm_nt(reader, now)
            here = pl.ds(start + j * SPAN, SPAN)
            local_ref[here, lanes] = local_read + reads[:, :LANES]
            reader_ref[pl.ds(start + j * SPAN, SPAN), lanes] = reads[:, LANES:].astype(BF16)
            now_high, now_low = split_two(now)
            step_high, step_low = split_two(transition)
            moved = mm(now_high, step_high) + mm(now_low, step_high) + mm(now_high, step_low)
            state[:LANES] = moved[:LANES] + offset
            state[LANES:] = moved[LANES:]
        return nothing

    lax.fori_loop(0, r_ref.shape[0] // (STACK * SPAN), advance, 0)
    summary_ref[1, spot] = (state[:half] + state[half:LANES]).astype(BF16)
    summary_ref[0, spot] = (state[LANES : LANES + half] + state[LANES + half :]).astype(BF16)


def gated(x, gate, up):
    gates = mm(x, gate)
    uppers = mm(x, up)
    return (gates / (1.0 + jnp.exp(-gates)) * uppers).astype(BF16)


def layer_kernel(capacity, head_size, early, *refs):
    (
        r_hbm,
        k_hbm,
        v_hbm,
        d_hbm,
        l_hbm,
        base_hbm,
        shift_hbm,
        gain_hbm,
        project_hbm,
        tokens_hbm,
        scale_hbm,
        routes_hbm,
        weight_hbm,
        gate_hbm,
        up_hbm,
        down_hbm,
        mixer_ref,
        expert_ref,
        r_ref,
        k_ref,
        v_ref,
        d_ref,
        l_ref,
        base_ref,
        shift_in,
        gain_ref,
        project,
        tokens_ref,
        scale_ref,
        routes_ref,
        weight_ref,
        own_gate,
        own_up,
        own_down,
        near_gate,
        near_up,
        near_down,
        far_gate,
        far_up,
        far_down,
        cross_gate,
        cross_up,
        cross_down,
        shift_ref,
        reader,
        local,
        summary,
        state,
        outgoing,
        x_ref,
        total,
        hidden_ref,
        before,
        sending,
        passed,
        mixed,
        far_rest_a,
        far_rest_b,
        cross_rest_a,
        cross_rest_b,
        theirs,
        part_out,
        part_in,
        staged_early,
        staged_late,
        landed_early,
        landed_late,
        term,
        near_in,
        pair_out,
        far_in,
        combined,
        load_sems,
        post_send,
        post_recv,
        back_send,
        back_recv,
        part_send,
        part_recv,
        round_send,
        round_recv,
        side_send,
        side_recv,
    ) = refs
    here = lax.axis_index("ep")
    count = lax.axis_size("ep")
    place = lax.axis_index("tp")
    low, high = lax.rem(place, 2), place // 2
    beside = place + 1 - 2 * low
    across = place + 2 - 4 * high
    reach_half = count // 2
    local_index, own_half = lax.rem(here, reach_half), here // reach_half
    rounds = passed.shape[0]
    half = LANES // 2
    pairs = before.shape[1]
    rows = x_ref.shape[0]
    units = own_gate.shape[1]
    tokens = expert_ref.shape[0]
    matched = same_head(head_size)
    block = matched.astype(BF16)
    diagonal = grid_index((LANES, LANES), 0) == grid_index((LANES, LANES), 1)

    pieces = [
        (tokens_hbm, tokens_ref),
        (scale_hbm, scale_ref),
        (routes_hbm, routes_ref),
        (weight_hbm, weight_ref),
        (base_hbm, base_ref),
        (shift_hbm, shift_in),
        (gain_hbm, gain_ref),
        (r_hbm, r_ref),
        (k_hbm, k_ref),
        (v_hbm, v_ref),
        (d_hbm, d_ref),
        (l_hbm, l_ref),
        (gate_hbm, own_gate),
        (up_hbm, own_up),
        (down_hbm, own_down),
        (project_hbm, project),
    ]
    loads = [
        pltpu.make_async_copy(src, dst, load_sems.at[i]) for i, (src, dst) in enumerate(pieces)
    ]
    keep_sem = load_sems.at[len(pieces)]
    barrier = pltpu.get_barrier_semaphore()
    greet_all(barrier, here, count, (beside, across))
    for load in loads:
        load.start()

    def side(src, dst, index, target):
        return send_to(src, dst, side_send.at[index], side_recv.at[index], {"tp": target})

    def rows_of(member):
        return pl.ds(pl.multiple_of(member * capacity, capacity), capacity)

    def partner(k, sign):
        crossing, shift = (k + 1) // reach_half, lax.rem(k + 1, reach_half)
        member = lax.rem(local_index + reach_half + sign * shift, reach_half)
        return member + reach_half * (own_half + crossing * (1 - 2 * own_half))

    def crossing_step(j):
        quarter = reach_half // 2
        side_of = (1 - own_half) + (j // quarter) * (2 * own_half - 1)
        index = side_of * quarter + lax.rem(local_index + j, quarter)
        shift = lax.rem(index - local_index + reach_half, reach_half)
        return reach_half - 1 + shift, (1 - own_half) * reach_half + index

    def post(k, member):
        return send_to(
            outgoing.at[rows_of(member)],
            x_ref.at[rows_of(here)],
            post_send.at[k],
            post_recv.at[k],
            {"ep": member},
        )

    def back(k, member, late):
        staged, landed = (staged_late, landed_late) if late else (staged_early, landed_early)
        return send_to(
            staged.at[rows_of(member)],
            landed.at[rows_of(here)],
            back_send.at[late, k],
            back_recv.at[late, k],
            {"ep": member},
        )

    far_rest = (far_rest_a, far_rest_b)
    cross_rest = (cross_rest_a, cross_rest_b)
    middle = far_rest_a.shape[1]
    spans = ((0, middle), (middle, middle + far_rest_b.shape[1]))

    def back_piece(k, member, i):
        columns = slice(*spans[i])
        return send_to(
            staged_late.at[rows_of(member), columns],
            landed_late.at[rows_of(here), columns],
            back_send.at[1 + i, k],
            back_recv.at[1 + i, k],
            {"ep": member},
        )

    def part(member):
        return send_to(
            part_out.at[rows_of(member)],
            part_in.at[rows_of(member)],
            part_send.at[member],
            part_recv.at[member],
            {"tp": across},
        )

    def at_half(which):
        return pl.ds(pl.multiple_of(which * (rows // 2), rows // 2), rows // 2)

    crossing_rows = at_half(1 - own_half)
    ask = side(hidden_ref.at[crossing_rows], theirs.at[crossing_rows], 14, across)

    cut = units // 2
    fars = [side(gate_hbm, far_gate, 0, across), side(up_hbm, far_up, 1, across)] + [
        side(
            down_hbm.at[i * cut : (i + 1) * cut, :early],
            far_down.at[i * cut : (i + 1) * cut],
            2 + i,
            across,
        )
        for i in range(2)
    ]
    nears = [
        side(gate_hbm, near_gate, 4, beside),
        side(up_hbm, near_up, 5, beside),
        side(down_hbm, near_down, 6, beside),
    ]
    forwards = [side(far_gate, cross_gate, 7, beside), side(far_up, cross_up, 8, beside)] + [
        side(
            far_down.at[i * cut : (i + 1) * cut], cross_down.at[i * cut : (i + 1) * cut], 9 + i, beside
        )
        for i in range(2)
    ]

    rests = [
        side(down_hbm.at[:, early + first : early + last], far_rest[i], 15 + i, across)
        for i, (first, last) in enumerate(spans)
    ]
    onward = [side(far_rest[i], cross_rest[i], 17 + i, beside) for i in range(2)]

    pl.semaphore_wait(barrier, count + 1)
    for copy in fars + nears:
        copy.start()
    for load in loads[:3]:
        load.wait()
    pack_rows(tokens_ref, scale_ref, routes_ref, outgoing, count, capacity)

    def launch_post(k, nothing):
        post(k, partner(k, 1)).start()
        return nothing

    def launch_crossing(j, nothing):
        post(*crossing_step(j)).start()
        return nothing

    lax.fori_loop(0, reach_half - 1, launch_post, 0)
    lax.fori_loop(0, reach_half, launch_crossing, 0)
    keep = pltpu.make_async_copy(outgoing.at[rows_of(here)], x_ref.at[rows_of(here)], keep_sem)
    keep.start()

    for load in loads[3:12]:
        load.wait()
    shift_ref[...] = shift_in[...].T

    def scan(p, nothing):
        scan_pair(
            p,
            head_size,
            r_ref,
            k_ref,
            v_ref,
            d_ref,
            l_ref,
            base_ref,
            shift_ref,
            reader,
            local,
            summary,
            state,
        )
        return nothing

    lax.fori_loop(0, pairs, scan, 0)

    def transfer(level, distance, target):
        return send_to(
            sending,
            passed.at[level],
            round_send.at[distance - 1],
            round_recv.at[level],
            {"ep": target},
        )

    def transfer_state(level, distance, target):
        return send_to(
            sending.at[1],
            passed.at[level, 1],
            round_send.at[distance - 1],
            round_recv.at[level],
            {"ep": target},
        )

    def sends_all(reach):
        return (lax.rem(here, 2 * reach) == reach - 1) & (here >= 2 * reach)

    def wide(part):
        part = part.astype(F32)
        return jnp.where(matched, jnp.concatenate([part, part], axis=0), 0.0)

    def spot(p):
        return slice(p * half, (p + 1) * half)

    for p in range(pairs):
        before[0, p] = jnp.where(diagonal, 1.0, 0.0)
        before[1, p] = jnp.zeros((LANES, LANES), F32)

    def send_round(level):
        reach = 2**level

        @pl.when(lax.rem(here, 2 * reach) == reach - 1)
        def _():
            for p in range(pairs):
                both = jnp.concatenate([before[0, p], before[1, p]], axis=0)
                upper, lower = split_two(both)
                step = wide(summary[0, spot(p)])
                moved = mm(upper, step) + mm(lower, step)
                after = moved[LANES:] + wide(summary[1, spot(p)])
                sending[0, spot(p)] = (moved[:half] + moved[half:LANES]).astype(BF16)
                sending[1, spot(p)] = (after[:half] + after[half:]).astype(BF16)

        def launch_with(transfer):
            def launch(distance, nothing):
                transfer(level, distance, here + distance).start()
                return nothing

            lax.fori_loop(1, reach + 1, launch, 0)

        pl.when(sends_all(reach))(lambda: launch_with(transfer))
        pl.when(here == reach - 1)(lambda: launch_with(transfer_state))

    def take_round(level):
        reach = 2**level

        @pl.when((lax.rem(here // reach, 2) == 1) & (here >= 2 * reach))
        def _():
            transfer(level, 1, here).wait_recv()
            for p in range(pairs):
                both = jnp.concatenate(
                    [wide(passed[level, 0, spot(p)]), wide(passed[level, 1, spot(p)])], axis=0
                )
                upper, lower = split_two(before[0, p])
                moved = mm(both, upper) + mm(both, lower)
                before[0, p] = moved[:LANES]
                before[1, p] = moved[LANES:] + before[1, p]

        @pl.when((here >= reach) & (here < 2 * reach))
        def _():
            transfer_state(level, 1, here).wait_recv()
            for p in range(pairs):
                entering = wide(passed[level, 1, spot(p)])
                upper, lower = split_two(before[0, p])
                before[1, p] = mm(entering, upper) + mm(entering, lower) + before[1, p]

    def settle_with(transfer, level, reach):
        def settle(distance, nothing):
            transfer(level, distance, here + distance).wait_send()
            return nothing

        lax.fori_loop(1, reach + 1, settle, 0)

    def full_parts(at):
        x = x_ref[at]
        total[at] = mm(gated(x, own_gate[...], own_up[...]), own_down[...])
        total[at] += mm(gated(x, near_gate[...], near_up[...]), near_down[...])

    def far_parts(at):
        x = x_ref[at]
        hidden_ref[at, :units] = gated(x, far_gate[...], far_up[...])
        hidden_ref[at, units:] = gated(x, cross_gate[...], cross_up[...])

    def take_post(k, nothing):
        post(k, partner(k, -1)).wait_recv()
        return nothing

    send_round(0)
    for load in loads[12:15]:
        load.wait()
    keep.wait()
    for copy in nears:
        copy.wait_recv()
    lax.fori_loop(0, reach_half - 1, take_post, 0)
    full_parts(at_half(own_half))
    fars[0].wait_recv()
    forwards[0].start()
    take_round(0)
    if rounds > 1:
        send_round(1)
    fars[1].wait_recv()
    forwards[1].start()
    lax.fori_loop(reach_half - 1, count - 1, take_post, 0)
    for level in range(1, min(rounds, 2)):
        take_round(level)
        if level + 1 < rounds:
            send_round(level + 1)
    full_parts(at_half(1 - own_half))
    for copy in forwards[:2]:
        copy.wait_recv()

    far_parts(crossing_rows)
    ask.start()
    far_parts(at_half(own_half))

    for i in range(2):
        fars[2 + i].wait_recv()
        forwards[2 + i].start()
    for copy in forwards[2:]:
        copy.wait_recv()

    def finished(member):
        at = rows_of(member)
        hidden = hidden_ref[at]
        row = total[at, :early] + mm(hidden[:, :units], far_down[...])
        return (row + mm(hidden[:, units:], cross_down[...])).astype(BF16)

    def send_early(k, member):
        staged_early[rows_of(member)] = finished(member)
        back(k, member, 0).start()

    def send_back(j, nothing):
        send_early(*crossing_step(j))
        return nothing

    def send_back_near(k, nothing):
        send_early(k, partner(k, 1))
        return nothing

    lax.fori_loop(0, reach_half, send_back, 0)
    lax.fori_loop(0, reach_half - 1, send_back_near, 0)
    landed_early[rows_of(here)] = finished(here)

    ask.wait_recv()
    asked = theirs[crossing_rows]
    product = mm(asked[:, :units], own_down[:, early:])
    product += mm(asked[:, units:], near_down[:, early:])
    part_out[crossing_rows] = product.astype(BF16)

    def launch_part(j, nothing):
        part(crossing_step(j)[1]).start()
        return nothing

    lax.fori_loop(0, reach_half, launch_part, 0)
    for copy in rests:
        copy.start()
    def send_crossing(j, nothing):
        k, member = crossing_step(j)
        part(member).wait_recv()
        at = rows_of(member)
        staged_late[at] = (total[at, early:] + part_in[at].astype(F32)).astype(BF16)
        back(k, member, 1).start()
        return nothing

    lax.fori_loop(0, reach_half, send_crossing, 0)

    for level in range(2, rounds):
        take_round(level)
        if level + 1 < rounds:
            send_round(level + 1)
    loads[15].wait()
    for p in range(pairs):
        lanes = slice(p * LANES, (p + 1) * LANES)
        read = mm_nt(reader[:, lanes], before[1, p]) + local[:, lanes]
        centred = read - head_sums(read, block) * (1.0 / head_size)
        variance = head_sums(centred * centred, block) * (1.0 / head_size)
        scaled = centred * lax.rsqrt(variance + GROUP_EPS) * gain_ref[:, lanes]
        mixed[:, lanes] = scaled.astype(BF16)

    def block_rows(b):
        return pl.ds(pl.multiple_of(b * tokens, tokens), tokens)

    def project_block(b, nothing):
        at = block_rows(b)
        term[at] = mm(mixed[at], project[...]).astype(BF16)
        return nothing

    lax.fori_loop(0, 4, project_block, 0)
    sums = [
        side(term.at[block_rows(2 * y + 1 - low)], near_in.at[y], 11 + y, beside)
        for y in range(2)
    ]
    for copy in sums:
        copy.start()

    picks = routes_ref.shape[0]
    packed = jnp.concatenate(
        [routes_ref[...].astype(F32), weight_ref[...], jnp.zeros((8 - 2 * picks, tokens), F32)],
        axis=0,
    ).T
    lane = grid_index((tokens, LANES), 1)
    routes = [packed[:, i : i + 1].astype(jnp.int32) for i in range(picks)]
    weight = packed[:, picks : 2 * picks]
    named = jnp.zeros((tokens, LANES), F32)
    for route in routes:
        named = jnp.where(route == lane, 1.0, named)
    earlier = grid_index((tokens, tokens), 0) > grid_index((tokens, tokens), 1)
    slots = mm(earlier.astype(F32), named)
    target = jnp.concatenate(
        [
            route * capacity
            + jnp.sum(jnp.where(route == lane, slots, 0.0), axis=1, keepdims=True).astype(
                jnp.int32
            )
            for route in routes
        ],
        axis=1,
    )
    slot = grid_index((tokens, capacity), 1)

    def taken(member, late):
        table = jnp.zeros((tokens, capacity), F32)
        scale = jnp.zeros((tokens, 1), F32)
        for picked in range(target.shape[1]):
            own = target[:, picked : picked + 1] - member * capacity
            table = jnp.where(own == slot, 1.0, table)
            inside = (own >= 0) & (own < capacity)
            scale = jnp.where(inside, weight[:, picked : picked + 1], scale)
        landed = landed_late if late else landed_early
        return mm(table, landed[rows_of(member)]) * scale

    combined[:, :early] = taken(here, 0)

    for copy in sums:
        copy.wait_recv()
    other = 1 - high
    pair_out[...] = (
        term[block_rows(2 * other + low)].astype(F32) + near_in[other].astype(F32)
    ).astype(BF16)
    last_sum = side(pair_out, far_in, 13, across)
    last_sum.start()

    def late_rows(member, i):
        at = rows_of(member)
        hidden = hidden_ref[at]
        first, last = spans[i]
        row = total[at, early + first : early + last]
        row += mm(hidden[:, :units], far_rest[i][...])
        return (row + mm(hidden[:, units:], cross_rest[i][...])).astype(BF16)

    def send_near(i):
        columns = slice(*spans[i])
        rests[i].wait_recv()
        onward[i].start()
        onward[i].wait_recv()

        def send_piece(k, nothing):
            member = partner(k, 1)
            staged_late[rows_of(member), columns] = late_rows(member, i)
            back_piece(k, member, i).start()
            return nothing

        lax.fori_loop(0, reach_half - 1, send_piece, 0)
        landed_late[rows_of(here), columns] = late_rows(here, i)

    def gather_early(k, nothing):
        member = partner(k, -1)
        back(k, member, 0).wait_recv()
        combined[:, :early] += taken(member, 0)
        return nothing

    def gather_near(k, nothing):
        member = partner(k, -1)
        for i in range(2):
            back_piece(k, member, i).wait_recv()
        combined[:, early:] += taken(member, 1)
        return nothing

    def gather_late(k, nothing):
        member = partner(k, -1)
        back(k, member, 1).wait_recv()
        combined[:, early:] += taken(member, 1)
        return nothing

    lax.fori_loop(0, reach_half - 1, gather_early, 0)
    for i in range(2):
        send_near(i)
    combined[:, early:] = taken(here, 1)
    lax.fori_loop(reach_half - 1, count - 1, gather_early, 0)
    lax.fori_loop(0, reach_half - 1, gather_near, 0)
    lax.fori_loop(reach_half - 1, count - 1, gather_late, 0)
    expert_ref[...] = combined[...].astype(BF16)
    last_sum.wait_recv()
    kept = term[block_rows(2 * high + low)].astype(F32) + near_in[high].astype(F32)
    mixer_ref[...] = (kept + far_in[...].astype(F32)).astype(BF16)

    def settle_rows(k, nothing):
        post(k, partner(k, 1)).wait_send()
        back(k, partner(k, 1), 0).wait_send()
        return nothing

    def settle_near(k, nothing):
        for i in range(2):
            back_piece(k, partner(k, 1), i).wait_send()
        return nothing

    def settle_crossing(k, nothing):
        back(k, partner(k, 1), 1).wait_send()
        return nothing

    def settle_part(j, nothing):
        part(crossing_step(j)[1]).wait_send()
        return nothing

    lax.fori_loop(0, count - 1, settle_rows, 0)
    lax.fori_loop(0, reach_half - 1, settle_near, 0)
    lax.fori_loop(reach_half - 1, count - 1, settle_crossing, 0)
    lax.fori_loop(0, reach_half, settle_part, 0)
    for level in range(rounds):
        reach = 2**level
        pl.when(sends_all(reach))(functools.partial(settle_with, transfer, level, reach))
        pl.when(here == reach - 1)(
            functools.partial(settle_with, transfer_state, level, reach)
        )
    for copy in fars + nears + forwards + [ask] + rests + onward + sums + [last_sum]:
        copy.wait_send()


def whole_layer(streams, base, shift, gain, out_weight, tokens, scale, routes, weights, own, head_size, capacity):
    rows, channels = streams[0].shape
    pairs = channels // LANES
    half = LANES // 2
    count = lax.axis_size("ep")
    rounds = (count - 1).bit_length()
    token_rows, width = tokens.shape
    slots = count * capacity
    units = own[0].shape[1]
    early = width * EARLY // (16 * LANES) * LANES
    late = width - early
    late_end = late // (2 * LANES) * LANES
    inputs = list(streams) + [
        base.reshape(1, channels),
        shift.T,
        gain.reshape(1, channels),
        out_weight,
        tokens,
        scale.reshape(1, width),
        routes.T,
        weights.T,
    ]
    operands = [in_hbm(array) for array in inputs + list(own)]
    block = (token_rows, width)
    wide, tall = (width, units), (units, width)
    held = [pltpu.VMEM(array.shape, array.dtype) for array in inputs]
    slim = (units, early)
    shapes = (wide, wide, tall) * 2 + (wide, wide, slim) * 2
    shards = [pltpu.VMEM(shape, BF16) for shape in shapes]
    dma = pltpu.SemaphoreType.DMA
    return pl.pallas_call(
        functools.partial(layer_kernel, capacity, head_size, early),
        in_specs=[pl.BlockSpec(memory_space=pl.ANY)] * len(operands),
        out_specs=[pl.BlockSpec(memory_space=pltpu.VMEM)] * 2,
        out_shape=[jax.ShapeDtypeStruct(block, BF16)] * 2,
        scratch_shapes=held
        + shards
        + [
            pltpu.VMEM(shift.shape, F32),
            pltpu.VMEM((rows, channels), BF16),
            pltpu.VMEM((rows, channels), F32),
            pltpu.VMEM((2, pairs * half, LANES), BF16),
            pltpu.VMEM((2 * LANES, LANES), F32),
            pltpu.VMEM((slots, width), BF16),
            pltpu.VMEM((slots, width), BF16),
            pltpu.VMEM((slots, width), F32),
            pltpu.VMEM((slots, 2 * units), BF16),
            pltpu.VMEM((2, pairs, LANES, LANES), F32),
            pltpu.VMEM((2, pairs * half, LANES), BF16),
            pltpu.VMEM((rounds, 2, pairs * half, LANES), BF16),
            pltpu.VMEM((rows, channels), BF16),
            pltpu.VMEM((units, late - late_end), BF16),
            pltpu.VMEM((units, late_end), BF16),
            pltpu.VMEM((units, late - late_end), BF16),
            pltpu.VMEM((units, late_end), BF16),
            pltpu.VMEM((slots, 2 * units), BF16),
            pltpu.VMEM((slots, late), BF16),
            pltpu.VMEM((slots, late), BF16),
            pltpu.VMEM((slots, early), BF16),
            pltpu.VMEM((slots, late), BF16),
            pltpu.VMEM((slots, early), BF16),
            pltpu.VMEM((slots, late), BF16),
            pltpu.VMEM((rows, width), BF16),
            pltpu.VMEM((2,) + block, BF16),
            pltpu.VMEM(block, BF16),
            pltpu.VMEM(block, BF16),
            pltpu.VMEM(block, F32),
            dma((len(operands) + 1,)),
            dma((count - 1,)),
            dma((count - 1,)),
            dma((3, count - 1)),
            dma((3, count - 1)),
            dma((count,)),
            dma((count,)),
            dma((count // 2,)),
            dma((rounds,)),
            dma((19,)),
            dma((19,)),
        ],
        compiler_params=pltpu.CompilerParams(
            vmem_limit_bytes=52 * 2**20, collective_id=0, has_side_effects=True
        ),
        cost_estimate=pl.CostEstimate(
            flops=40 * 10**9, bytes_accessed=20 * 2**20, transcendentals=2 * 10**6
        ),
        name="whole_layer",
    )(*operands)


def output_kernel(mixer_ref, expert_ref, mixer_out, expert_out, sems):
    copies = [
        pltpu.make_async_copy(mixer_ref, mixer_out, sems.at[0]),
        pltpu.make_async_copy(expert_ref, expert_out, sems.at[1]),
    ]
    for copy in copies:
        copy.start()
    for copy in copies:
        copy.wait()


def write_outputs(mixer, expert):
    return pl.pallas_call(
        output_kernel,
        in_specs=[pl.BlockSpec(memory_space=pltpu.VMEM)] * 2,
        out_specs=[pl.BlockSpec(memory_space=pl.ANY)] * 2,
        out_shape=[
            jax.ShapeDtypeStruct(mixer.shape, BF16),
            jax.ShapeDtypeStruct(expert.shape, BF16),
        ],
        scratch_shapes=[pltpu.SemaphoreType.DMA((2,))],
        compiler_params=pltpu.CompilerParams(vmem_limit_bytes=4 * 2**20),
        name="write_outputs",
    )(mixer, expert)


def on_device(
    receptance,
    key_rows,
    value_rows,
    decay_input,
    learn_input,
    decay_base,
    decay_shift,
    channel_gain,
    out_weight,
    expert_input,
    expert_gain,
    routes,
    route_weight,
    gate_weight,
    up_weight,
    down_weight,
):
    head_size = receptance.shape[1] // decay_shift.shape[1]
    experts = gate_weight.shape[0] * lax.axis_size("ep")
    capacity = max(2, 2 * expert_input.shape[0] * routes.shape[1] // experts)
    return tuple(
        write_outputs(
            *whole_layer(
                (receptance, key_rows, value_rows, decay_input, learn_input),
                decay_base,
                decay_shift,
                channel_gain,
                out_weight,
                expert_input,
                expert_gain,
                routes,
                route_weight,
                (gate_weight[0], up_weight[0], down_weight[0]),
                head_size,
                capacity,
            )
        )
    )


def solution(mesh):
    return jax.shard_map(
        on_device,
        mesh=mesh,
        in_specs=(
            P("ep", "tp"),
            P("ep", "tp"),
            P("ep", "tp"),
            P("ep", "tp"),
            P("ep", "tp"),
            P("tp"),
            P("ep", "tp"),
            P("tp"),
            P("tp", None),
            P(("ep", "tp"), None),
            P(),
            P(("ep", "tp"), None),
            P(("ep", "tp"), None),
            P("ep", None, "tp"),
            P("ep", None, "tp"),
            P("ep", "tp", None),
        ),
        out_specs=(P(("ep", "tp"), None), P(("ep", "tp"), None)),
        check_vma=False,
    )
```

```python
import functools

import jax
import jax.numpy as jnp
from jax import lax
from jax.experimental import pallas as pl
from jax.experimental.pallas import tpu as pltpu
from jax.sharding import PartitionSpec as P

SPAN = 128
STACK = 2
LANES = 128
EARLY = 6

NORM_EPS = 1e-06
GROUP_EPS = 0.00064
KEY_EPS = 1e-06
F32 = jnp.float32
BF16 = jnp.bfloat16


def mm(a, b):
    return lax.dot_general(
        a.astype(BF16), b.astype(BF16), (((1,), (0,)), ((), ())), preferred_element_type=F32
    )


def mm_nt(a, b):
    return lax.dot_general(
        a.astype(BF16), b.astype(BF16), (((1,), (1,)), ((), ())), preferred_element_type=F32
    )


def mm_tn(a, b):
    return lax.dot_general(
        a.astype(BF16), b.astype(BF16), (((0,), (0,)), ((), ())), preferred_element_type=F32
    )


def split_two(x):
    high = x.astype(BF16)
    return high, (x - high.astype(F32)).astype(BF16)


def grid_index(shape, axis):
    return lax.broadcasted_iota(jnp.int32, shape, axis)


def same_head(head_size):
    rows = grid_index((LANES, LANES), 0) // head_size
    cols = grid_index((LANES, LANES), 1) // head_size
    return rows == cols


def head_sums(x, block):
    high, low = split_two(x)
    return mm(
        jnp.concatenate([high, low], axis=1), jnp.concatenate([block, block], axis=0)
    )


def lower_inverses(strict_parts, rows, cols):
    eye = jnp.where(rows == cols, 1.0, 0.0)
    size = 1
    inverses = None
    while size < SPAN:
        off = (rows // (2 * size) == cols // (2 * size)) & (rows // size != cols // size)
        parts = [jnp.where(off, part, 0.0) for part in strict_parts]
        if inverses is None:
            inverses = [eye - part for part in parts]
        else:
            firsts = [mm(part, inv) for part, inv in zip(parts, inverses)]
            inverses = [inv - mm(inv, first) for inv, first in zip(inverses, firsts)]
        size *= 2
    return inverses


def send_to(src, dst, send_sem, recv_sem, target):
    return pltpu.make_async_remote_copy(
        src_ref=src,
        dst_ref=dst,
        send_sem=send_sem,
        recv_sem=recv_sem,
        device_id=target,
        device_id_type=pl.DeviceIdType.MESH,
    )


def greet_all(barrier, here, count, others):
    def greet(distance, nothing):
        pl.semaphore_signal(
            barrier,
            inc=1,
            device_id={"ep": lax.rem(here + distance, count)},
            device_id_type=pl.DeviceIdType.MESH,
        )
        return nothing

    lax.fori_loop(1, count, greet, 0)
    for target in others:
        pl.semaphore_signal(
            barrier, inc=1, device_id={"tp": target}, device_id_type=pl.DeviceIdType.MESH
        )


def in_hbm(array):
    return pltpu.with_memory_space_constraint(array, pltpu.HBM)


def pack_rows(tokens_ref, scale_ref, routes_ref, outgoing, count, capacity):
    inputs = tokens_ref[...].astype(F32)
    square = jnp.sum(inputs * inputs, axis=1, keepdims=True) * (1.0 / inputs.shape[1])
    normed = (inputs * lax.rsqrt(square + NORM_EPS) * scale_ref[...]).astype(BF16)
    rows = inputs.shape[0]
    members = grid_index((count, rows), 0)
    named = jnp.zeros((count, rows), F32)
    for picked in range(routes_ref.shape[0]):
        named = jnp.where(routes_ref[picked : picked + 1] == members, 1.0, named)
    earlier = grid_index((rows, rows), 0) < grid_index((rows, rows), 1)
    slots = mm(named, earlier.astype(F32))
    slots = jnp.where(named > 0.5, slots, -1.0).astype(jnp.int32)
    wanted = grid_index((capacity, rows), 0)
    group = max(1, min(count, 256 // capacity))
    for begin in range(0, count, group):
        table = jnp.concatenate(
            [
                jnp.where(slots[e : e + 1] == wanted, 1.0, 0.0)
                for e in range(begin, begin + group)
            ],
            axis=0,
        )
        outgoing[begin * capacity : (begin + group) * capacity] = mm(table, normed).astype(BF16)


def scan_pair(
    pair,
    head_size,
    r_ref,
    k_ref,
    v_ref,
    d_ref,
    l_ref,
    base_ref,
    shift_ref,
    reader_ref,
    local_ref,
    summary_ref,
    state,
):
    half = LANES // 2
    lanes = pl.ds(pl.multiple_of(pair * LANES, LANES), LANES)
    spot = pl.ds(pl.multiple_of(pair * half, half), half)

    rows = grid_index((SPAN, SPAN), 0)
    cols = grid_index((SPAN, SPAN), 1)
    strict = rows > cols
    inclusive = rows >= cols
    first = grid_index((SPAN, LANES), 1) < half
    matched = same_head(head_size)
    block = matched.astype(BF16)
    diagonal = grid_index((LANES, LANES), 0) == grid_index((LANES, LANES), 1)
    tri = inclusive.astype(BF16)
    tri_two = jnp.concatenate([tri, tri], axis=1)

    state[:LANES] = jnp.zeros((LANES, LANES), F32)
    state[LANES:] = jnp.where(diagonal, 1.0, 0.0)

    heads = shift_ref.shape[1]
    chosen = grid_index((heads, LANES), 0) == 2 * pair + grid_index((heads, LANES), 1) // half
    def advance(step, nothing):
        start = pl.multiple_of(step * (STACK * SPAN), STACK * SPAN)
        rows_here = pl.ds(start, STACK * SPAN)
        shift = lax.dot_general(
            shift_ref[rows_here],
            chosen.astype(F32),
            (((1,), (0,)), ((), ())),
            precision=lax.Precision.HIGHEST,
            preferred_element_type=F32,
        )
        pre = d_ref[rows_here, lanes].astype(F32) + base_ref[:, lanes] + shift
        log_all = -0.6065306597126334 / (1.0 + jnp.exp(-pre))
        rates = 1.0 / (1.0 + jnp.exp(-l_ref[rows_here, lanes].astype(F32)))
        key_all = k_ref[rows_here, lanes].astype(F32)
        unit_all = key_all * lax.rsqrt(head_sums(key_all * key_all, block) + KEY_EPS)
        removal_all = unit_all * rates

        spans = STACK
        items = []
        strict_parts = []
        for j in range(spans):
            here = slice(j * SPAN, (j + 1) * SPAN)
            log_decay = log_all[here]
            high, low = split_two(log_decay)
            cum = mm(tri_two, jnp.concatenate([high, low], axis=0))
            middle = cum[SPAN // 2 - 1 : SPAN // 2]
            ending = cum[SPAN - 1 :]
            e_cm = jnp.exp(cum - middle)
            e_pm = jnp.exp(cum - log_decay - middle)
            shrink = jnp.exp(middle - cum)
            e_mid = jnp.exp(middle)
            e_tail = jnp.exp(ending - middle)
            unit, key = unit_all[here], key_all[here]
            value = v_ref[pl.ds(start + j * SPAN, SPAN), lanes]
            turned = jnp.concatenate([value[:, half:], value[:, :half]], axis=1)
            recept = r_ref[pl.ds(start + j * SPAN, SPAN), lanes].astype(F32)
            probes = unit * e_pm
            queries = recept * e_cm
            back_removal = removal_all[here] * shrink
            back_keys = key * shrink
            left = jnp.concatenate(
                [
                    jnp.where(first, probes, 0.0),
                    jnp.where(first, 0.0, probes),
                    jnp.where(first, queries, 0.0),
                    jnp.where(first, 0.0, queries),
                ],
                axis=0,
            )
            products = mm_nt(left, jnp.concatenate([back_removal, back_keys], axis=0))
            for h in range(2):
                strict_parts.append(
                    jnp.where(strict, products[h * SPAN : (h + 1) * SPAN, :SPAN], 0.0)
                )
            items.append(
                dict(
                    products=products,
                    turned=turned,
                    carrying=probes * e_mid,
                    reading=queries * e_mid,
                    removal_tail=back_removal * e_tail,
                    key_tail=back_keys * e_tail,
                    fade=jnp.exp(ending),
                )
            )
        inverses = lower_inverses(strict_parts, rows, cols)
        for j in range(spans):
            item = items[j]
            products, turned = item["products"], item["turned"]
            solved, removed, kept = [], [], []
            for h in range(2):
                top = slice(h * SPAN, (h + 1) * SPAN)
                bottom = slice((2 + h) * SPAN, (3 + h) * SPAN)
                pair_keys = jnp.where(strict, products[top, SPAN:], 0.0)
                read_removal = jnp.where(inclusive, products[bottom, :SPAN], 0.0)
                read_keys = jnp.where(inclusive, products[bottom, SPAN:], 0.0)
                both = mm(jnp.concatenate([pair_keys, read_keys], axis=0), turned)
                own = first if h == 0 else jnp.logical_not(first)
                right = jnp.where(own, item["carrying"], both[:SPAN])
                answer = mm(inverses[2 * j + h], right)
                solved.append(answer)
                removed.append(mm(read_removal, answer))
                kept.append(both[SPAN:])
            carried = jnp.where(first, solved[0], solved[1])
            local_turned = jnp.where(first, solved[1], solved[0])
            reader = item["reading"] - jnp.where(first, removed[0], removed[1])
            read_turned = jnp.where(first, kept[1] - removed[1], kept[0] - removed[0])
            local_read = jnp.concatenate([read_turned[:, half:], read_turned[:, :half]], axis=1)
            taken = mm_tn(
                jnp.concatenate([carried, local_turned], axis=1), item["removal_tail"]
            )
            offset_turned = mm_tn(turned, item["key_tail"]) - taken[LANES:]
            offset = jnp.concatenate([offset_turned[half:], offset_turned[:half]], axis=0)
            offset = jnp.where(matched, offset, 0.0)
            transition = jnp.where(diagonal, item["fade"], 0.0) - jnp.where(
                matched, taken[:LANES], 0.0
            )
            now = state[...]
            reads = mm_nt(reader, now)
            here = pl.ds(start + j * SPAN, SPAN)
            local_ref[here, lanes] = local_read + reads[:, :LANES]
            reader_ref[pl.ds(start + j * SPAN, SPAN), lanes] = reads[:, LANES:].astype(BF16)
            now_high, now_low = split_two(now)
            step_high, step_low = split_two(transition)
            moved = mm(now_high, step_high) + mm(now_low, step_high) + mm(now_high, step_low)
            state[:LANES] = moved[:LANES] + offset
            state[LANES:] = moved[LANES:]
        return nothing

    lax.fori_loop(0, r_ref.shape[0] // (STACK * SPAN), advance, 0)
    summary_ref[1, spot] = (state[:half] + state[half:LANES]).astype(BF16)
    summary_ref[0, spot] = (state[LANES : LANES + half] + state[LANES + half :]).astype(BF16)


def gated(x, gate, up):
    gates = mm(x, gate)
    uppers = mm(x, up)
    return (gates / (1.0 + jnp.exp(-gates)) * uppers).astype(BF16)


def layer_kernel(capacity, head_size, early, *refs):
    (
        r_hbm,
        k_hbm,
        v_hbm,
        d_hbm,
        l_hbm,
        base_hbm,
        shift_hbm,
        gain_hbm,
        project_hbm,
        tokens_hbm,
        scale_hbm,
        routes_hbm,
        weight_hbm,
        gate_hbm,
        up_hbm,
        down_hbm,
        mixer_ref,
        expert_ref,
        r_ref,
        k_ref,
        v_ref,
        d_ref,
        l_ref,
        base_ref,
        shift_in,
        gain_ref,
        project,
        tokens_ref,
        scale_ref,
        routes_ref,
        weight_ref,
        own_gate,
        own_up,
        own_down,
        near_gate,
        near_up,
        near_down,
        far_gate,
        far_up,
        far_down,
        cross_gate,
        cross_up,
        cross_down,
        shift_ref,
        reader,
        local,
        summary,
        state,
        outgoing,
        x_ref,
        total,
        hidden_ref,
        before,
        sending,
        passed,
        mixed,
        far_rest_a,
        far_rest_b,
        cross_rest_a,
        cross_rest_b,
        theirs,
        part_out,
        part_in,
        staged_early,
        staged_late,
        landed_early,
        landed_late,
        term,
        near_in,
        pair_out,
        far_in,
        combined,
        load_sems,
        post_send,
        post_recv,
        back_send,
        back_recv,
        part_send,
        part_recv,
        round_send,
        round_recv,
        side_send,
        side_recv,
    ) = refs
    here = lax.axis_index("ep")
    count = lax.axis_size("ep")
    place = lax.axis_index("tp")
    low, high = lax.rem(place, 2), place // 2
    beside = place + 1 - 2 * low
    across = place + 2 - 4 * high
    reach_half = count // 2
    local_index, own_half = lax.rem(here, reach_half), here // reach_half
    rounds = passed.shape[0]
    half = LANES // 2
    pairs = before.shape[1]
    rows = x_ref.shape[0]
    units = own_gate.shape[1]
    tokens = expert_ref.shape[0]
    matched = same_head(head_size)
    block = matched.astype(BF16)
    diagonal = grid_index((LANES, LANES), 0) == grid_index((LANES, LANES), 1)

    pieces = [
        (tokens_hbm, tokens_ref),
        (scale_hbm, scale_ref),
        (routes_hbm, routes_ref),
        (weight_hbm, weight_ref),
        (base_hbm, base_ref),
        (shift_hbm, shift_in),
        (gain_hbm, gain_ref),
        (r_hbm, r_ref),
        (k_hbm, k_ref),
        (v_hbm, v_ref),
        (d_hbm, d_ref),
        (l_hbm, l_ref),
        (gate_hbm, own_gate),
        (up_hbm, own_up),
        (down_hbm, own_down),
        (project_hbm, project),
    ]
    loads = [
        pltpu.make_async_copy(src, dst, load_sems.at[i]) for i, (src, dst) in enumerate(pieces)
    ]
    keep_sem = load_sems.at[len(pieces)]
    barrier = pltpu.get_barrier_semaphore()
    greet_all(barrier, here, count, (beside, across))
    for load in loads:
        load.start()

    def side(src, dst, index, target):
        return send_to(src, dst, side_send.at[index], side_recv.at[index], {"tp": target})

    def rows_of(member):
        return pl.ds(pl.multiple_of(member * capacity, capacity), capacity)

    def partner(k, sign):
        crossing, shift = (k + 1) // reach_half, lax.rem(k + 1, reach_half)
        member = lax.rem(local_index + reach_half + sign * shift, reach_half)
        return member + reach_half * (own_half + crossing * (1 - 2 * own_half))

    def crossing_step(j):
        quarter = reach_half // 2
        side_of = (1 - own_half) + (j // quarter) * (2 * own_half - 1)
        index = side_of * quarter + lax.rem(local_index + j, quarter)
        shift = lax.rem(index - local_index + reach_half, reach_half)
        return reach_half - 1 + shift, (1 - own_half) * reach_half + index

    def post(k, member):
        return send_to(
            outgoing.at[rows_of(member)],
            x_ref.at[rows_of(here)],
            post_send.at[k],
            post_recv.at[k],
            {"ep": member},
        )

    def back(k, member, late):
        staged, landed = (staged_late, landed_late) if late else (staged_early, landed_early)
        return send_to(
            staged.at[rows_of(member)],
            landed.at[rows_of(here)],
            back_send.at[late, k],
            back_recv.at[late, k],
            {"ep": member},
        )

    far_rest = (far_rest_a, far_rest_b)
    cross_rest = (cross_rest_a, cross_rest_b)
    middle = far_rest_a.shape[1]
    spans = ((0, middle), (middle, middle + far_rest_b.shape[1]))

    def back_piece(k, member, i):
        columns = slice(*spans[i])
        return send_to(
            staged_late.at[rows_of(member), columns],
            landed_late.at[rows_of(here), columns],
            back_send.at[1 + i, k],
            back_recv.at[1 + i, k],
            {"ep": member},
        )

    def part(member):
        return send_to(
            part_out.at[rows_of(member)],
            part_in.at[rows_of(member)],
            part_send.at[member],
            part_recv.at[member],
            {"tp": across},
        )

    def at_half(which):
        return pl.ds(pl.multiple_of(which * (rows // 2), rows // 2), rows // 2)

    crossing_rows = at_half(1 - own_half)
    ask = side(hidden_ref.at[crossing_rows], theirs.at[crossing_rows], 14, across)

    cut = units // 2
    fars = [side(gate_hbm, far_gate, 0, across), side(up_hbm, far_up, 1, across)] + [
        side(
            down_hbm.at[i * cut : (i + 1) * cut, :early],
            far_down.at[i * cut : (i + 1) * cut],
            2 + i,
            across,
        )
        for i in range(2)
    ]
    nears = [
        side(gate_hbm, near_gate, 4, beside),
        side(up_hbm, near_up, 5, beside),
        side(down_hbm, near_down, 6, beside),
    ]
    forwards = [side(far_gate, cross_gate, 7, beside), side(far_up, cross_up, 8, beside)] + [
        side(
            far_down.at[i * cut : (i + 1) * cut], cross_down.at[i * cut : (i + 1) * cut], 9 + i, beside
        )
        for i in range(2)
    ]

    rests = [
        side(down_hbm.at[:, early + first : early + last], far_rest[i], 15 + i, across)
        for i, (first, last) in enumerate(spans)
    ]
    onward = [side(far_rest[i], cross_rest[i], 17 + i, beside) for i in range(2)]

    pl.semaphore_wait(barrier, count + 1)
    for copy in fars + nears:
        copy.start()
    for load in loads[:3]:
        load.wait()
    pack_rows(tokens_ref, scale_ref, routes_ref, outgoing, count, capacity)

    def launch_post(k, nothing):
        post(k, partner(k, 1)).start()
        return nothing

    def launch_crossing(j, nothing):
        post(*crossing_step(j)).start()
        return nothing

    lax.fori_loop(0, reach_half - 1, launch_post, 0)
    lax.fori_loop(0, reach_half, launch_crossing, 0)
    keep = pltpu.make_async_copy(outgoing.at[rows_of(here)], x_ref.at[rows_of(here)], keep_sem)
    keep.start()

    for load in loads[3:12]:
        load.wait()
    shift_ref[...] = shift_in[...].T

    def scan(p, nothing):
        scan_pair(
            p,
            head_size,
            r_ref,
            k_ref,
            v_ref,
            d_ref,
            l_ref,
            base_ref,
            shift_ref,
            reader,
            local,
            summary,
            state,
        )
        return nothing

    lax.fori_loop(0, pairs, scan, 0)

    def transfer(level, distance, target):
        return send_to(
            sending,
            passed.at[level],
            round_send.at[distance - 1],
            round_recv.at[level],
            {"ep": target},
        )

    def transfer_state(level, distance, target):
        return send_to(
            sending.at[1],
            passed.at[level, 1],
            round_send.at[distance - 1],
            round_recv.at[level],
            {"ep": target},
        )

    def sends_all(reach):
        return (lax.rem(here, 2 * reach) == reach - 1) & (here >= 2 * reach)

    def wide(part):
        part = part.astype(F32)
        return jnp.where(matched, jnp.concatenate([part, part], axis=0), 0.0)

    def spot(p):
        return slice(p * half, (p + 1) * half)

    for p in range(pairs):
        before[0, p] = jnp.where(diagonal, 1.0, 0.0)
        before[1, p] = jnp.zeros((LANES, LANES), F32)

    def send_round(level):
        reach = 2**level

        @pl.when(lax.rem(here, 2 * reach) == reach - 1)
        def _():
            for p in range(pairs):
                both = jnp.concatenate([before[0, p], before[1, p]], axis=0)
                upper, lower = split_two(both)
                step = wide(summary[0, spot(p)])
                moved = mm(upper, step) + mm(lower, step)
                after = moved[LANES:] + wide(summary[1, spot(p)])
                sending[0, spot(p)] = (moved[:half] + moved[half:LANES]).astype(BF16)
                sending[1, spot(p)] = (after[:half] + after[half:]).astype(BF16)

        def launch_with(transfer):
            def launch(distance, nothing):
                transfer(level, distance, here + distance).start()
                return nothing

            lax.fori_loop(1, reach + 1, launch, 0)

        pl.when(sends_all(reach))(lambda: launch_with(transfer))
        pl.when(here == reach - 1)(lambda: launch_with(transfer_state))

    def take_round(level):
        reach = 2**level

        @pl.when((lax.rem(here // reach, 2) == 1) & (here >= 2 * reach))
        def _():
            transfer(level, 1, here).wait_recv()
            for p in range(pairs):
                both = jnp.concatenate(
                    [wide(passed[level, 0, spot(p)]), wide(passed[level, 1, spot(p)])], axis=0
                )
                upper, lower = split_two(before[0, p])
                moved = mm(both, upper) + mm(both, lower)
                before[0, p] = moved[:LANES]
                before[1, p] = moved[LANES:] + before[1, p]

        @pl.when((here >= reach) & (here < 2 * reach))
        def _():
            transfer_state(level, 1, here).wait_recv()
            for p in range(pairs):
                entering = wide(passed[level, 1, spot(p)])
                upper, lower = split_two(before[0, p])
                before[1, p] = mm(entering, upper) + mm(entering, lower) + before[1, p]

    def settle_with(transfer, level, reach):
        def settle(distance, nothing):
            transfer(level, distance, here + distance).wait_send()
            return nothing

        lax.fori_loop(1, reach + 1, settle, 0)

    def full_parts(at):
        x = x_ref[at]
        total[at] = mm(gated(x, own_gate[...], own_up[...]), own_down[...])
        total[at] += mm(gated(x, near_gate[...], near_up[...]), near_down[...])

    def far_parts(at):
        x = x_ref[at]
        hidden_ref[at, :units] = gated(x, far_gate[...], far_up[...])
        hidden_ref[at, units:] = gated(x, cross_gate[...], cross_up[...])

    def take_post(k, nothing):
        post(k, partner(k, -1)).wait_recv()
        return nothing

    send_round(0)
    for load in loads[12:15]:
        load.wait()
    keep.wait()
    for copy in nears:
        copy.wait_recv()
    lax.fori_loop(0, reach_half - 1, take_post, 0)
    full_parts(at_half(own_half))
    fars[0].wait_recv()
    forwards[0].start()
    take_round(0)
    if rounds > 1:
        send_round(1)
    fars[1].wait_recv()
    forwards[1].start()
    lax.fori_loop(reach_half - 1, count - 1, take_post, 0)
    for level in range(1, min(rounds, 2)):
        take_round(level)
        if level + 1 < rounds:
            send_round(level + 1)
    full_parts(at_half(1 - own_half))
    for copy in forwards[:2]:
        copy.wait_recv()

    far_parts(crossing_rows)
    ask.start()
    far_parts(at_half(own_half))

    for i in range(2):
        fars[2 + i].wait_recv()
        forwards[2 + i].start()
    for copy in forwards[2:]:
        copy.wait_recv()

    def finished(member):
        at = rows_of(member)
        hidden = hidden_ref[at]
        row = total[at, :early] + mm(hidden[:, :units], far_down[...])
        return (row + mm(hidden[:, units:], cross_down[...])).astype(BF16)

    def send_early(k, member):
        staged_early[rows_of(member)] = finished(member)
        back(k, member, 0).start()

    def send_back(j, nothing):
        send_early(*crossing_step(j))
        return nothing

    def send_back_near(k, nothing):
        send_early(k, partner(k, 1))
        return nothing

    lax.fori_loop(0, reach_half, send_back, 0)
    lax.fori_loop(0, reach_half - 1, send_back_near, 0)
    landed_early[rows_of(here)] = finished(here)

    ask.wait_recv()
    asked = theirs[crossing_rows]
    product = mm(asked[:, :units], own_down[:, early:])
    product += mm(asked[:, units:], near_down[:, early:])
    part_out[crossing_rows] = product.astype(BF16)

    def launch_part(j, nothing):
        part(crossing_step(j)[1]).start()
        return nothing

    lax.fori_loop(0, reach_half, launch_part, 0)
    for copy in rests:
        copy.start()
    def send_crossing(j, nothing):
        k, member = crossing_step(j)
        part(member).wait_recv()
        at = rows_of(member)
        staged_late[at] = (total[at, early:] + part_in[at].astype(F32)).astype(BF16)
        back(k, member, 1).start()
        return nothing

    lax.fori_loop(0, reach_half, send_crossing, 0)

    for level in range(2, rounds):
        take_round(level)
        if level + 1 < rounds:
            send_round(level + 1)
    loads[15].wait()
    for p in range(pairs):
        lanes = slice(p * LANES, (p + 1) * LANES)
        read = mm_nt(reader[:, lanes], before[1, p]) + local[:, lanes]
        centred = read - head_sums(read, block) * (1.0 / head_size)
        variance = head_sums(centred * centred, block) * (1.0 / head_size)
        scaled = centred * lax.rsqrt(variance + GROUP_EPS) * gain_ref[:, lanes]
        mixed[:, lanes] = scaled.astype(BF16)

    def block_rows(b):
        return pl.ds(pl.multiple_of(b * tokens, tokens), tokens)

    def project_block(b, nothing):
        at = block_rows(b)
        term[at] = mm(mixed[at], project[...]).astype(BF16)
        return nothing

    lax.fori_loop(0, 4, project_block, 0)
    sums = [
        side(term.at[block_rows(2 * y + 1 - low)], near_in.at[y], 11 + y, beside)
        for y in range(2)
    ]
    for copy in sums:
        copy.start()

    picks = routes_ref.shape[0]
    packed = jnp.concatenate(
        [routes_ref[...].astype(F32), weight_ref[...], jnp.zeros((8 - 2 * picks, tokens), F32)],
        axis=0,
    ).T
    lane = grid_index((tokens, LANES), 1)
    routes = [packed[:, i : i + 1].astype(jnp.int32) for i in range(picks)]
    weight = packed[:, picks : 2 * picks]
    named = jnp.zeros((tokens, LANES), F32)
    for route in routes:
        named = jnp.where(route == lane, 1.0, named)
    earlier = grid_index((tokens, tokens), 0) > grid_index((tokens, tokens), 1)
    slots = mm(earlier.astype(F32), named)
    target = jnp.concatenate(
        [
            route * capacity
            + jnp.sum(jnp.where(route == lane, slots, 0.0), axis=1, keepdims=True).astype(
                jnp.int32
            )
            for route in routes
        ],
        axis=1,
    )
    slot = grid_index((tokens, capacity), 1)

    def taken(member, late):
        table = jnp.zeros((tokens, capacity), F32)
        scale = jnp.zeros((tokens, 1), F32)
        for picked in range(target.shape[1]):
            own = target[:, picked : picked + 1] - member * capacity
            table = jnp.where(own == slot, 1.0, table)
            inside = (own >= 0) & (own < capacity)
            scale = jnp.where(inside, weight[:, picked : picked + 1], scale)
        landed = landed_late if late else landed_early
        return mm(table, landed[rows_of(member)]) * scale

    combined[:, :early] = taken(here, 0)

    for copy in sums:
        copy.wait_recv()
    other = 1 - high
    pair_out[...] = (
        term[block_rows(2 * other + low)].astype(F32) + near_in[other].astype(F32)
    ).astype(BF16)
    last_sum = side(pair_out, far_in, 13, across)
    last_sum.start()

    def late_rows(member, i):
        at = rows_of(member)
        hidden = hidden_ref[at]
        first, last = spans[i]
        row = total[at, early + first : early + last]
        row += mm(hidden[:, :units], far_rest[i][...])
        return (row + mm(hidden[:, units:], cross_rest[i][...])).astype(BF16)

    def send_near(i):
        columns = slice(*spans[i])
        rests[i].wait_recv()
        onward[i].start()
        onward[i].wait_recv()

        def send_piece(k, nothing):
            member = partner(k, 1)
            staged_late[rows_of(member), columns] = late_rows(member, i)
            back_piece(k, member, i).start()
            return nothing

        lax.fori_loop(0, reach_half - 1, send_piece, 0)
        landed_late[rows_of(here), columns] = late_rows(here, i)

    def gather_early(k, nothing):
        member = partner(k, -1)
        back(k, member, 0).wait_recv()
        combined[:, :early] += taken(member, 0)
        return nothing

    def gather_near(k, nothing):
        member = partner(k, -1)
        for i in range(2):
            back_piece(k, member, i).wait_recv()
        combined[:, early:] += taken(member, 1)
        return nothing

    def gather_late(k, nothing):
        member = partner(k, -1)
        back(k, member, 1).wait_recv()
        combined[:, early:] += taken(member, 1)
        return nothing

    lax.fori_loop(0, reach_half - 1, gather_early, 0)
    for i in range(2):
        send_near(i)
    combined[:, early:] = taken(here, 1)
    lax.fori_loop(reach_half - 1, count - 1, gather_early, 0)
    lax.fori_loop(0, reach_half - 1, gather_near, 0)
    lax.fori_loop(reach_half - 1, count - 1, gather_late, 0)
    expert_ref[...] = combined[...].astype(BF16)
    last_sum.wait_recv()
    kept = term[block_rows(2 * high + low)].astype(F32) + near_in[high].astype(F32)
    mixer_ref[...] = (kept + far_in[...].astype(F32)).astype(BF16)

    def settle_rows(k, nothing):
        post(k, partner(k, 1)).wait_send()
        back(k, partner(k, 1), 0).wait_send()
        return nothing

    def settle_near(k, nothing):
        for i in range(2):
            back_piece(k, partner(k, 1), i).wait_send()
        return nothing

    def settle_crossing(k, nothing):
        back(k, partner(k, 1), 1).wait_send()
        return nothing

    def settle_part(j, nothing):
        part(crossing_step(j)[1]).wait_send()
        return nothing

    lax.fori_loop(0, count - 1, settle_rows, 0)
    lax.fori_loop(0, reach_half - 1, settle_near, 0)
    lax.fori_loop(reach_half - 1, count - 1, settle_crossing, 0)
    lax.fori_loop(0, reach_half, settle_part, 0)
    for level in range(rounds):
        reach = 2**level
        pl.when(sends_all(reach))(functools.partial(settle_with, transfer, level, reach))
        pl.when(here == reach - 1)(
            functools.partial(settle_with, transfer_state, level, reach)
        )
    for copy in fars + nears + forwards + [ask] + rests + onward + sums + [last_sum]:
        copy.wait_send()


def whole_layer(streams, base, shift, gain, out_weight, tokens, scale, routes, weights, own, head_size, capacity):
    rows, channels = streams[0].shape
    pairs = channels // LANES
    half = LANES // 2
    count = lax.axis_size("ep")
    rounds = (count - 1).bit_length()
    token_rows, width = tokens.shape
    slots = count * capacity
    units = own[0].shape[1]
    early = width * EARLY // (16 * LANES) * LANES
    late = width - early
    late_end = late // (3 * LANES) * LANES
    inputs = list(streams) + [
        base.reshape(1, channels),
        shift.T,
        gain.reshape(1, channels),
        out_weight,
        tokens,
        scale.reshape(1, width),
        routes.T,
        weights.T,
    ]
    operands = [in_hbm(array) for array in inputs + list(own)]
    block = (token_rows, width)
    wide, tall = (width, units), (units, width)
    held = [pltpu.VMEM(array.shape, array.dtype) for array in inputs]
    slim = (units, early)
    shapes = (wide, wide, tall) * 2 + (wide, wide, slim) * 2
    shards = [pltpu.VMEM(shape, BF16) for shape in shapes]
    dma = pltpu.SemaphoreType.DMA
    return pl.pallas_call(
        functools.partial(layer_kernel, capacity, head_size, early),
        in_specs=[pl.BlockSpec(memory_space=pl.ANY)] * len(operands),
        out_specs=[pl.BlockSpec(memory_space=pltpu.VMEM)] * 2,
        out_shape=[jax.ShapeDtypeStruct(block, BF16)] * 2,
        scratch_shapes=held
        + shards
        + [
            pltpu.VMEM(shift.shape, F32),
            pltpu.VMEM((rows, channels), BF16),
            pltpu.VMEM((rows, channels), F32),
            pltpu.VMEM((2, pairs * half, LANES), BF16),
            pltpu.VMEM((2 * LANES, LANES), F32),
            pltpu.VMEM((slots, width), BF16),
            pltpu.VMEM((slots, width), BF16),
            pltpu.VMEM((slots, width), F32),
            pltpu.VMEM((slots, 2 * units), BF16),
            pltpu.VMEM((2, pairs, LANES, LANES), F32),
            pltpu.VMEM((2, pairs * half, LANES), BF16),
            pltpu.VMEM((rounds, 2, pairs * half, LANES), BF16),
            pltpu.VMEM((rows, channels), BF16),
            pltpu.VMEM((units, late - late_end), BF16),
            pltpu.VMEM((units, late_end), BF16),
            pltpu.VMEM((units, late - late_end), BF16),
            pltpu.VMEM((units, late_end), BF16),
            pltpu.VMEM((slots, 2 * units), BF16),
            pltpu.VMEM((slots, late), BF16),
            pltpu.VMEM((slots, late), BF16),
            pltpu.VMEM((slots, early), BF16),
            pltpu.VMEM((slots, late), BF16),
            pltpu.VMEM((slots, early), BF16),
            pltpu.VMEM((slots, late), BF16),
            pltpu.VMEM((rows, width), BF16),
            pltpu.VMEM((2,) + block, BF16),
            pltpu.VMEM(block, BF16),
            pltpu.VMEM(block, BF16),
            pltpu.VMEM(block, F32),
            dma((len(operands) + 1,)),
            dma((count - 1,)),
            dma((count - 1,)),
            dma((3, count - 1)),
            dma((3, count - 1)),
            dma((count,)),
            dma((count,)),
            dma((count // 2,)),
            dma((rounds,)),
            dma((19,)),
            dma((19,)),
        ],
        compiler_params=pltpu.CompilerParams(
            vmem_limit_bytes=52 * 2**20, collective_id=0, has_side_effects=True
        ),
        cost_estimate=pl.CostEstimate(
            flops=40 * 10**9, bytes_accessed=20 * 2**20, transcendentals=2 * 10**6
        ),
        name="whole_layer",
    )(*operands)


def output_kernel(mixer_ref, expert_ref, mixer_out, expert_out, sems):
    copies = [
        pltpu.make_async_copy(mixer_ref, mixer_out, sems.at[0]),
        pltpu.make_async_copy(expert_ref, expert_out, sems.at[1]),
    ]
    for copy in copies:
        copy.start()
    for copy in copies:
        copy.wait()


def write_outputs(mixer, expert):
    return pl.pallas_call(
        output_kernel,
        in_specs=[pl.BlockSpec(memory_space=pltpu.VMEM)] * 2,
        out_specs=[pl.BlockSpec(memory_space=pl.ANY)] * 2,
        out_shape=[
            jax.ShapeDtypeStruct(mixer.shape, BF16),
            jax.ShapeDtypeStruct(expert.shape, BF16),
        ],
        scratch_shapes=[pltpu.SemaphoreType.DMA((2,))],
        compiler_params=pltpu.CompilerParams(vmem_limit_bytes=4 * 2**20),
        name="write_outputs",
    )(mixer, expert)


def on_device(
    receptance,
    key_rows,
    value_rows,
    decay_input,
    learn_input,
    decay_base,
    decay_shift,
    channel_gain,
    out_weight,
    expert_input,
    expert_gain,
    routes,
    route_weight,
    gate_weight,
    up_weight,
    down_weight,
):
    head_size = receptance.shape[1] // decay_shift.shape[1]
    experts = gate_weight.shape[0] * lax.axis_size("ep")
    capacity = max(2, 2 * expert_input.shape[0] * routes.shape[1] // experts)
    return tuple(
        write_outputs(
            *whole_layer(
                (receptance, key_rows, value_rows, decay_input, learn_input),
                decay_base,
                decay_shift,
                channel_gain,
                out_weight,
                expert_input,
                expert_gain,
                routes,
                route_weight,
                (gate_weight[0], up_weight[0], down_weight[0]),
                head_size,
                capacity,
            )
        )
    )


def solution(mesh):
    return jax.shard_map(
        on_device,
        mesh=mesh,
        in_specs=(
            P("ep", "tp"),
            P("ep", "tp"),
            P("ep", "tp"),
            P("ep", "tp"),
            P("ep", "tp"),
            P("tp"),
            P("ep", "tp"),
            P("tp"),
            P("tp", None),
            P(("ep", "tp"), None),
            P(),
            P(("ep", "tp"), None),
            P(("ep", "tp"), None),
            P("ep", None, "tp"),
            P("ep", None, "tp"),
            P("ep", "tp", None),
        ),
        out_specs=(P(("ep", "tp"), None), P(("ep", "tp"), None)),
        check_vma=False,
    )
```
